512 devices in a mesh: grp: 2 (over y), kv: 64 (over z, core), tp: 4 (over x).
Axes of the slice: x: 4, y: 2, z: 32, core: 2. Of those that a mesh axis runs over, the one named last changes fastest.
The devices are a block of a 4x8x32 slice.
Arguments:
- tokens: bfloat16 [65536, 2048], P(('grp', 'kv'), 'tp'), parts along dimension 0, may hold values from -5400 to 5400, as said below
- gain: bfloat16 [2048], replicated, may hold values from 0.099609375 to 1.8984375
- w_query: bfloat16 [2048, 1024], P(None, 'tp'), may hold values from -1 to 1
- w_key: bfloat16 [2048, 512], P(None, 'tp'), may hold values from -3 to 3
- w_value: bfloat16 [2048, 512], P(None, 'tp'), may hold values from -0.125 to 0.125
- w_out: bfloat16 [1024, 2048], P(None, 'tp'), may hold values from -2 to 2
- select: int32 [512, 32], P(('grp', 'kv')), parts along dimension 0, may hold values from -1 to 1023, as said below
Outputs:
- mixed: bfloat16 [65536, 2048], P(('grp', 'kv'), 'tp'), parts along dimension 0
The draws below stay inside these ranges and needn't reach their ends.
There are 2 independent parts, one for each index of `grp`. The reference program is written for one: setup_inputs(seed, part) draws one part's arguments, and reference() takes and returns one part's arrays. A program takes and returns all parts, laid end to end along the dimension named above; an argument that names none is the same for every part. Nothing has to cross between parts.
Inputs may be any that keep to these rules, and one draw needn't show every extreme that they name: Entries of tokens are finite with scales that vary by row and by column. `select`: row b lists distinct key blocks that start no later than query block b ends, or -1 for an empty slot. Every query block lists each key block of its own index of kv up to its own last position. Apart from its own index, the query blocks of one index of kv together list at most 2 distinct key blocks held by any other index; every index but the first lists exactly 2 blocks of the index before it.
All inputs are finite; a program needn't handle non-finite values.
Results may differ from the reference program's by a relative error of at most 0.012.
Values may be sent and summed in bfloat16 or wider, within the bound.
A program may use at most 128 MiB of HBM per device.

```python
import math
import jax
import jax.numpy as jnp
from jax import lax

D = 2048
HEADS = 8
KV_HEADS = 4
HD = 128
TOK_DEV = 512
QB = 128
KB = 32
NSEL = 32
TOKENS = 32768
NQB = 256
NKB = 1024
N_KV = 64


def draw_tokens(key, part):
    base_key = jax.random.fold_in(key, 11)
    draw_keys = jax.random.split(base_key, 3)
    column = jnp.arange(D, dtype=jnp.float32)
    base_draw = jnp.clip(jax.random.normal(draw_keys[0], (TOKENS, D), jnp.float32), -6.0, 6.0)
    rise_factor = 3.0 ** (column / D)
    row_scale = jnp.exp(jax.random.uniform(draw_keys[1], (TOKENS, 1), jnp.float32, 0.0, math.log(10.0)))
    col_scale = jnp.exp(jax.random.uniform(draw_keys[2], (1, D), jnp.float32, 0.0, math.log(10.0)))
    return (base_draw * row_scale * col_scale * rise_factor[None, :]).astype(jnp.bfloat16)


def query_weight(key):
    normal_draw = jax.random.normal(jax.random.fold_in(key, 21), (D, HEADS * HD), jnp.float32)
    return jnp.clip(normal_draw, -6.0, 6.0) / math.sqrt(D)


def draw_w_query(key, part):
    return query_weight(key).astype(jnp.bfloat16)


def draw_w_key(key, part):
    own_part = jnp.clip(jax.random.normal(jax.random.fold_in(key, 22), (D, KV_HEADS * HD), jnp.float32), -6.0, 6.0) / math.sqrt(D)
    own_part = jnp.clip(own_part, -3.0, 3.0)
    return own_part.astype(jnp.bfloat16)


def draw_select(key, part):
    base_key = jax.random.fold_in(key, 31)
    query_blocks = TOK_DEV // QB
    block_ratio = QB // KB
    blocks_dev = TOK_DEV // KB
    owner_ids = jnp.arange(N_KV, dtype=jnp.int32)
    hot_owner = (jax.random.randint(jax.random.fold_in(base_key, 1), (N_KV,), 0, 4) == 0).astype(jnp.int32)
    first_pick = jax.random.randint(jax.random.fold_in(base_key, 2), (N_KV, N_KV), 0, blocks_dev)
    step_offset = jax.random.randint(jax.random.fold_in(base_key, 3), (N_KV, N_KV), 1, blocks_dev)
    second_pick = (first_pick + step_offset) % blocks_dev
    slot_ids = jnp.arange(NSEL, dtype=jnp.int32)

    def draw_row(block_id):
        device = block_id // query_blocks
        local_block = block_id % query_blocks
        own_count = block_ratio * (local_block + 1)
        pair_count = (NSEL - own_count) // 2
        noise_bits = jax.random.randint(jax.random.fold_in(jax.random.fold_in(base_key, 4), block_id), (N_KV,), 0, 1 << 12)
        forced = (owner_ids == device - 1) | (owner_ids == device - N_KV // 2) & (device >= N_KV // 2)
        scores = noise_bits + hot_owner * (1 << 13) + forced.astype(jnp.int32) * (1 << 15)
        scores = jnp.where(owner_ids < device, scores, -(1 << 16))
        scores = scores * N_KV + owner_ids
        ranking = jnp.argsort(-scores, stable=True).astype(jnp.int32)
        rank_ids = jnp.arange(N_KV, dtype=jnp.int32)
        usable = (rank_ids < pair_count) & (ranking < device)
        block_a = ranking * blocks_dev + first_pick[device, ranking]
        block_b = ranking * blocks_dev + second_pick[device, ranking]
        pair_ids = jnp.where(usable[:, None], jnp.stack([block_a, block_b], axis=1), -1).reshape(-1)
        pair_ids = jnp.concatenate([pair_ids, jnp.full((NSEL,), -1, jnp.int32)])
        own_ids = device * blocks_dev + slot_ids
        from_pairs = jnp.take(pair_ids, jnp.maximum(slot_ids - own_count, 0))
        return jnp.where(slot_ids < own_count, own_ids, from_pairs).astype(jnp.int32)
    return jax.vmap(draw_row)(jnp.arange(NQB, dtype=jnp.int32))


def steps_of(key, shape, cuts, smallest, largest):
    level = 1.0
    for position, shards_of in cuts:
        draws = jax.random.uniform(jax.random.fold_in(jax.random.fold_in(key, 6), position), (shards_of,), jnp.float32, smallest / len(cuts), largest / len(cuts))
        level = level * jnp.repeat(jnp.exp(draws), shape[position] // shards_of).reshape((-1,) + (1,) * (len(shape) - 1 - position))
    return level


def scatter_about(key, extent, width, most, shards=(), kind=jnp.bfloat16):
    entries = width * jax.random.normal(key, extent, jnp.float32)
    if shards:
        entries = entries * steps_of(key, extent, shards, -0.22, 0.18)
    return jnp.clip(entries, -most, most).astype(kind)


def setup_inputs(seed: int = 0, part: int = 0) -> dict:
    splits = jax.random.split(jax.random.key(seed), 8)
    part_splits = jax.random.split(jax.random.fold_in(splits[7], part), 8)
    return {
        "tokens": draw_tokens(jax.random.fold_in(jax.random.fold_in(splits[7], part), 71), part),
        "gain": jnp.clip(1.0 + 0.18 * jax.random.normal(splits[1], (D,), jnp.float32), 0.099609375, 1.8984375).astype(jnp.bfloat16),
        "w_query": draw_w_query(jax.random.fold_in(splits[7], 71), part),
        "w_key": draw_w_key(jax.random.fold_in(splits[7], 71), part),
        "w_value": scatter_about(splits[4], (D, KV_HEADS * HD), D ** -0.5, 0.125, ((1, 4),)),
        "w_out": scatter_about(splits[5], (HEADS * HD, D), (max(HEADS * HD // 128, 1)) ** -0.5, 2.0, ((1, 4),)),
        "select": draw_select(jax.random.fold_in(jax.random.fold_in(splits[7], part), 71), part),
    }


epsilon = 1e-06
theta = 10000.0

def rotary(values, positions):
    head_width = values.shape[-1]
    frequency = theta ** (-jnp.arange(0, head_width, 2, dtype=jnp.float32) / head_width)
    angles = positions.astype(jnp.float32)[:, None] * frequency[None, :]
    cosine = jnp.cos(angles)[:, None, :]
    sine_table = jnp.sin(angles)[:, None, :]
    front_half = values[..., :head_width // 2]
    second = values[..., head_width // 2:]
    return jnp.concatenate([front_half * cosine - second * sine_table, second * cosine + front_half * sine_table], axis=-1)

def reference(tokens, gain, w_query, w_key, w_value, w_out, select):
    tokens_f32 = tokens.astype(jnp.float32)
    mean_square = lax.optimization_barrier(jnp.mean(tokens_f32 * tokens_f32, axis=1))
    scaled = (tokens_f32 * gain.astype(jnp.float32)[None, :]).astype(jnp.bfloat16)
    inverse = lax.rsqrt(mean_square + epsilon)[:, None]
    positions = jnp.arange(TOKENS, dtype=jnp.int32)
    query_pre = jnp.dot(scaled, w_query, preferred_element_type=jnp.float32) * inverse
    key_pre = jnp.dot(scaled, w_key, preferred_element_type=jnp.float32) * inverse
    value_pre = jnp.dot(scaled, w_value, preferred_element_type=jnp.float32) * inverse
    queries = rotary(query_pre.reshape(TOKENS, HEADS, HD), positions).astype(jnp.bfloat16)
    keys_all = rotary(key_pre.reshape(TOKENS, KV_HEADS, HD), positions).astype(jnp.bfloat16)
    values_all = value_pre.astype(jnp.bfloat16).reshape(TOKENS, KV_HEADS, HD)
    group_size = HEADS // KV_HEADS
    key_blocks = keys_all.reshape(NKB, KB, KV_HEADS, HD)
    value_blocks = values_all.reshape(NKB, KB, KV_HEADS, HD)

    def one_block(block_id):
        block_ids = select[block_id]
        safe_ids = jnp.maximum(block_ids, 0)
        keys_sel = jnp.take(key_blocks, safe_ids, axis=0).reshape(NSEL * KB, KV_HEADS, HD).astype(jnp.float32)
        values_sel = jnp.take(value_blocks, safe_ids, axis=0).reshape(NSEL * KB, KV_HEADS, HD).astype(jnp.float32)
        query_rows = lax.dynamic_slice_in_dim(queries, block_id * QB, QB, 0)
        query_rows = query_rows.reshape(QB, KV_HEADS, group_size, HD).astype(jnp.float32)
        scores = jnp.einsum('qgrd,kgd->grqk', query_rows, keys_sel) * HD ** (-0.5)
        key_pos = (safe_ids[:, None] * KB + jnp.arange(KB, dtype=jnp.int32)[None, :]).reshape(-1)
        live_keys = jnp.repeat(block_ids >= 0, KB)
        q_pos = block_id * QB + jnp.arange(QB, dtype=jnp.int32)
        allowed = live_keys[None, :] & (key_pos[None, :] <= q_pos[:, None])
        scores = jnp.where(allowed[None, None], scores, -jnp.inf)
        row_max = lax.optimization_barrier(jnp.max(scores, axis=-1, keepdims=True))
        raised = jnp.exp(scores - row_max)
        weights = (raised / lax.optimization_barrier(jnp.sum(raised, axis=-1, keepdims=True))).astype(jnp.bfloat16)
        attended = jnp.einsum('grqk,kgd->qgrd', weights.astype(jnp.float32), values_sel)
        return attended.astype(jnp.bfloat16).reshape(QB, HEADS * HD)
    attended_all = lax.map(one_block, jnp.arange(NQB, dtype=jnp.int32)).reshape(TOKENS, HEADS * HD)
    return jnp.dot(attended_all, w_out, preferred_element_type=jnp.float32).astype(jnp.bfloat16)
```

```python
import functools

import jax
import jax.numpy as jnp
from jax import lax
from jax.experimental import pallas as pl
from jax.experimental.pallas import tpu as pltpu
from jax.sharding import PartitionSpec as P

HD = 128
QB = 128
KB = 32
PIECES = 4

epsilon = 1e-06
theta = 10000.0
MESH = pl.DeviceIdType.MESH


def rotary_tables(positions):
    frequency = theta ** (-jnp.arange(0, HD, 2, dtype=jnp.float32) / HD)
    angles = positions.astype(jnp.float32)[:, None] * frequency[None, :]
    cosine, sine = jnp.cos(angles), jnp.sin(angles)
    return jnp.concatenate([cosine, cosine], 1), jnp.concatenate([-sine, sine], 1)


def remote(src, dst, send, recv, **where):
    return pltpu.make_async_remote_copy(
        src_ref=src, dst_ref=dst, send_sem=send, recv_sem=recv, device_id=where, device_id_type=MESH
    )


class TpRing:
    def __init__(self, own, slots, send, recv, rows):
        self.n = lax.axis_size("tp")
        self.me = lax.axis_index("tp")
        self.right = lax.rem(self.me + 1, self.n)
        self.left = lax.rem(self.me + self.n - 1, self.n)
        self.far = lax.rem(self.me + 2, self.n)
        self.own, self.slots, self.send, self.recv, self.rows = own, slots, send, recv, rows

    def copy(self, chunk, kind):
        half = self.rows // 2
        start, size, source, to = {
            0: (0, self.rows, None, self.right),
            1: (0, self.rows, None, self.left),
            2: (0, half, self.left, self.right),
            3: (half, half, self.right, self.left),
        }[kind]
        at = pl.ds(chunk * self.rows + start, size)
        src = self.own.at[at] if source is None else self.slots.at[source, at]
        dst = self.slots.at[self.me if source is None else source, at]
        return remote(src, dst, self.send.at[chunk, kind], self.recv.at[chunk, kind], tp=to)

    def begin(self, chunk):
        self.copy(chunk, 0).start()
        self.copy(chunk, 1).start()

    def hand_on(self, chunk):
        self.copy(chunk, 0).wait_recv()
        self.copy(chunk, 2).start()
        self.copy(chunk, 1).wait_recv()
        self.copy(chunk, 3).start()

    def arrived(self, chunk):
        self.copy(chunk, 2).wait_recv()
        self.copy(chunk, 3).wait_recv()

    def sent(self, chunk):
        for kind in range(4):
            self.copy(chunk, kind).wait_send()


def greet(others):
    barrier = pltpu.get_barrier_semaphore()
    for where in others:
        pl.semaphore_signal(barrier, inc=1, device_id=where, device_id_type=MESH)
    pl.semaphore_wait(barrier, len(others))


def project_kernel(
    tok, gain, wq, wk, wv, cos, sin, q_out, every,
    slots, weights, kv, send_t, recv_t, send_z, recv_z, send_c, recv_c, local,
):
    rows, width = tok.shape
    tp = lax.axis_size("tp")
    chunk_rows = rows // PIECES
    ring = TpRing(tok, slots, send_t, recv_t, chunk_rows)
    devices = lax.axis_size("kv")
    chips = devices // 2
    mine = lax.axis_index("kv")
    z, core = mine // 2, lax.rem(mine, 2)
    partner = mine + 1 - 2 * core
    up = lax.rem(mine + 2, devices)
    down = lax.rem(mine + devices - 2, devices)
    q_cols, k_cols = wq.shape[1], wk.shape[1]
    loads = [
        pltpu.make_async_copy(wq, weights.at[:, pl.ds(0, q_cols)], local.at[0]),
        pltpu.make_async_copy(wk, weights.at[:, pl.ds(q_cols, k_cols)], local.at[1]),
        pltpu.make_async_copy(wv, weights.at[:, pl.ds(q_cols + k_cols, k_cols)], local.at[2]),
        pltpu.make_async_copy(tok, slots.at[ring.me], local.at[3]),
    ]
    for load in loads:
        load.start()
    greet(
        [{"tp": ring.right}, {"tp": ring.left}, {"kv": partner}, {"kv": up}, {"kv": down}]
    )
    for chunk in range(PIECES):
        ring.begin(chunk)
    for load in loads:
        load.wait()

    def piece_of(owner, piece):
        return every.at[owner, pl.ds(piece * chunk_rows, chunk_rows)]

    def owner_at(direction, step):
        if direction == 0:
            return lax.rem(z - step + chips, chips) * 2 + core
        return lax.rem(z + step, chips) * 2 + core

    def hop(direction, step, piece):
        to = up if direction == 0 else down
        owner = owner_at(direction, step - 1)
        return remote(
            piece_of(owner, piece), piece_of(owner, piece),
            send_z.at[direction, step, piece], recv_z.at[direction, step, piece], kv=to,
        )

    def first_hop(direction, piece):
        to = up if direction == 0 else down
        return remote(
            kv.at[pl.ds(piece * chunk_rows, chunk_rows)], piece_of(mine, piece),
            send_z.at[direction, 1, piece], recv_z.at[direction, 1, piece], kv=to,
        )

    def across(direction, step, piece):
        owner = owner_at(direction, step)
        return remote(
            piece_of(owner, piece), piece_of(owner, piece),
            send_c.at[direction, step], recv_c.at[direction, step], kv=partner,
        )

    def across_whole(direction, step):
        owner = owner_at(direction, step)
        return remote(
            every.at[owner], every.at[owner],
            send_c.at[direction, step], recv_c.at[direction, step], kv=partner,
        )

    for chunk in range(PIECES):
        ring.hand_on(chunk)
        ring.arrived(chunk)
        at = pl.ds(chunk * chunk_rows, chunk_rows)
        total = jnp.zeros((chunk_rows, weights.shape[1]), jnp.float32)
        squares = jnp.zeros((chunk_rows, 1), jnp.float32)
        for t in range(tp):
            block = slots[t, at, :].astype(jnp.float32)
            squares += jnp.sum(block * block, axis=1, keepdims=True)
            scaled = (block * gain[:, t * width:(t + 1) * width].astype(jnp.float32)).astype(jnp.bfloat16)
            total += jnp.dot(
                scaled, weights[t * width:(t + 1) * width, :], preferred_element_type=jnp.float32
            )
        inverse = lax.rsqrt(squares / (tp * width) + epsilon)
        total *= inverse
        cosine, sine = cos[at, :], sin[at, :]
        heads = []
        for h in range((q_cols + k_cols) // HD):
            head = total[:, h * HD:(h + 1) * HD]
            heads.append((head * cosine + pltpu.roll(head, HD // 2, 1) * sine).astype(jnp.bfloat16))
        for h in range(q_cols // HD):
            q_out[at, h * HD:(h + 1) * HD] = heads[h]
        kv[at, 0:k_cols] = heads[-1]
        kv[at, k_cols:2 * k_cols] = total[:, q_cols + k_cols:].astype(jnp.bfloat16)
        first_hop(0, chunk).start()
        first_hop(1, chunk).start()

    keep = pltpu.make_async_copy(kv, every.at[mine], local.at[4])
    keep.start()
    give = remote(kv, every.at[mine], send_c.at[0, 0], recv_c.at[0, 0], kv=partner)
    give.start()

    last = chips // 2
    half = PIECES // 2

    @pl.loop(1, last - 1)
    def _(step):
        for piece in range(PIECES):
            for direction in range(2):
                hop(direction, step, piece).wait_recv()
                hop(direction, step + 1, piece).start()
                across(direction, step, piece).start()

    for piece in range(PIECES):
        for direction in range(2):
            hop(direction, last - 1, piece).wait_recv()
            if (piece < half) == (direction == 0):
                hop(direction, last, piece).start()
            across(direction, last - 1, piece).start()
    for piece in range(half):
        for direction in range(2):
            which = piece + direction * half
            hop(direction, last, which).wait_recv()
            across(0, last, which).start()

    keep.wait()
    give.wait()
    for chunk in range(PIECES):
        ring.sent(chunk)
        for direction in range(2):
            first_hop(direction, chunk).wait_send()

    @pl.loop(1, last)
    def _(step):
        for direction in range(2):
            across_whole(direction, step).wait()

    @pl.loop(2, last)
    def _(step):
        for direction in range(2):
            for piece in range(PIECES):
                hop(direction, step, piece).wait_send()

    across_whole(0, last).wait()
    for piece in range(half):
        for direction in range(2):
            hop(direction, last, piece + direction * half).wait_send()


def project(tokens, gain, w_query, w_key, w_value, cosine, sine):
    rows, width = tokens.shape
    devices = lax.axis_size("kv")
    tp = lax.axis_size("tp")
    q_cols, k_cols = w_query.shape[1], w_key.shape[1]
    steps = devices // 4 + 1
    dma = pltpu.SemaphoreType.DMA
    vmem = pl.BlockSpec(memory_space=pltpu.VMEM)
    hbm = pl.BlockSpec(memory_space=pl.ANY)
    return pl.pallas_call(
        project_kernel,
        out_shape=(
            jax.ShapeDtypeStruct((rows, q_cols), jnp.bfloat16),
            jax.ShapeDtypeStruct((devices, rows, 2 * k_cols), jnp.bfloat16),
        ),
        in_specs=[vmem, vmem, hbm, hbm, hbm, vmem, vmem],
        out_specs=(vmem, hbm),
        scratch_shapes=[
            pltpu.VMEM((tp, rows, width), jnp.bfloat16),
            pltpu.VMEM((tp * width, q_cols + 2 * k_cols), jnp.bfloat16),
            pltpu.VMEM((rows, 2 * k_cols), jnp.bfloat16),
            dma((PIECES, 4)),
            dma((PIECES, 4)),
            dma((2, steps, PIECES)),
            dma((2, steps, PIECES)),
            dma((2, steps)),
            dma((2, steps)),
            dma((5,)),
        ],
        compiler_params=pltpu.CompilerParams(collective_id=0, has_side_effects=True),
        name="project",
    )(tokens, gain, w_query, w_key, w_value, cosine, sine)


def attend_kernel(listed, q, sel, every, out, keys, sems):
    blocks, slots = sel.shape
    heads = q.shape[1] // HD
    start_at = lax.axis_index("kv") * q.shape[0]

    def fetch(b, s, index):
        return pltpu.make_async_copy(
            every.at[pl.ds(pl.multiple_of(index * KB, KB), KB)],
            keys.at[b, pl.ds(pl.multiple_of(s * KB, KB), KB)],
            sems.at[b],
        )

    for b in range(blocks):
        @pl.loop(0, slots)
        def _(s, b=b):
            fetch(b, s, jnp.maximum(listed[b, s], 0)).start()

    width = slots * KB
    spread = (
        lax.broadcasted_iota(jnp.int32, (slots, width), 1) // KB
        == lax.broadcasted_iota(jnp.int32, (slots, width), 0)
    ).astype(jnp.float32)
    ids = sel[...]
    safe = jnp.where(ids < 0, 1 << 20, ids)
    high = (safe // 64).astype(jnp.float32)
    low = lax.rem(safe, 64).astype(jnp.float32)
    wide = jnp.dot(high, spread, preferred_element_type=jnp.float32) * 64.0 + jnp.dot(
        low, spread, preferred_element_type=jnp.float32
    )
    key_pos = wide.astype(jnp.int32) * KB + lax.rem(
        lax.broadcasted_iota(jnp.int32, (blocks, width), 1), KB
    )
    for b in range(blocks):
        pltpu.make_async_copy(every.at[pl.ds(0, width)], keys.at[b], sems.at[b]).wait()
        q_pos = start_at + b * QB + lax.broadcasted_iota(jnp.int32, (QB, width), 0)
        allowed = jnp.broadcast_to(key_pos[b:b + 1, :], (QB, width)) <= q_pos
        for h in range(heads):
            score = lax.dot_general(
                q[b * QB:(b + 1) * QB, h * HD:(h + 1) * HD], keys[b, :, 0:HD],
                (((1,), (1,)), ((), ())), preferred_element_type=jnp.float32,
            ) * HD ** (-0.5)
            score = jnp.where(allowed, score, -jnp.inf)
            raised = jnp.exp(score - jnp.max(score, axis=1, keepdims=True))
            weights = (raised / jnp.sum(raised, axis=1, keepdims=True)).astype(jnp.bfloat16)
            out[b * QB:(b + 1) * QB, h * HD:(h + 1) * HD] = jnp.dot(
                weights, keys[b, :, HD:2 * HD], preferred_element_type=jnp.float32
            ).astype(jnp.bfloat16)


def attend(select, queries, every):
    blocks, slots = select.shape
    rows, cols = queries.shape
    vmem = pl.BlockSpec(memory_space=pltpu.VMEM)
    return pl.pallas_call(
        attend_kernel,
        out_shape=jax.ShapeDtypeStruct((rows, cols), jnp.bfloat16),
        in_specs=[
            pl.BlockSpec(memory_space=pltpu.SMEM), vmem, vmem, pl.BlockSpec(memory_space=pl.ANY)
        ],
        out_specs=vmem,
        scratch_shapes=[
            pltpu.VMEM((blocks, slots * KB, 2 * HD), jnp.bfloat16),
            pltpu.SemaphoreType.DMA((blocks,)),
        ],
        name="attend",
    )(select, queries, select, every)


def mix_kernel(mine, w_out, out, slots, send_t, recv_t, local):
    rows, width = mine.shape
    chunk_rows = rows // PIECES
    ring = TpRing(mine, slots, send_t, recv_t, chunk_rows)
    keep = pltpu.make_async_copy(mine, slots.at[ring.me], local)
    keep.start()
    greet([{"tp": ring.right}, {"tp": ring.left}])
    for chunk in range(PIECES):
        ring.begin(chunk)
    keep.wait()
    for chunk in range(PIECES):
        ring.hand_on(chunk)
        ring.arrived(chunk)
        at = pl.ds(chunk * chunk_rows, chunk_rows)
        total = jnp.zeros((chunk_rows, out.shape[1]), jnp.float32)
        for t in range(lax.axis_size("tp")):
            total += jnp.dot(
                slots[t, at, :], w_out[t * width:(t + 1) * width, :],
                preferred_element_type=jnp.float32,
            )
        out[at, :] = total.astype(jnp.bfloat16)
    for chunk in range(PIECES):
        ring.sent(chunk)


def mix(attended, w_out):
    rows, width = attended.shape
    tp = lax.axis_size("tp")
    dma = pltpu.SemaphoreType.DMA
    vmem = pl.BlockSpec(memory_space=pltpu.VMEM)
    return pl.pallas_call(
        mix_kernel,
        out_shape=jax.ShapeDtypeStruct((rows, w_out.shape[1]), jnp.bfloat16),
        in_specs=[vmem, vmem],
        out_specs=vmem,
        scratch_shapes=[
            pltpu.VMEM((tp, rows, width), jnp.bfloat16),
            dma((PIECES, 4)),
            dma((PIECES, 4)),
            dma(()),
        ],
        compiler_params=pltpu.CompilerParams(collective_id=1, has_side_effects=True),
        name="mix",
    )(attended, w_out)


def per_device(tokens, gain, w_query, w_key, w_value, w_out, select):
    rows = tokens.shape[0]
    positions = lax.axis_index("kv") * rows + jnp.arange(rows, dtype=jnp.int32)
    cosine, sine = rotary_tables(positions)
    queries, every = project(
        tokens, gain.reshape(1, -1), w_query, w_key, w_value, cosine, sine
    )
    attended = attend(select, queries, every.reshape(-1, every.shape[2]))
    return mix(attended, w_out)


def solution(mesh):
    placed = (
        P(("grp", "kv"), "tp"),
        P(),
        P(None, "tp"),
        P(None, "tp"),
        P(None, "tp"),
        P(None, "tp"),
        P(("grp", "kv"), None),
    )
    return jax.shard_map(
        per_device, mesh=mesh, in_specs=placed, out_specs=P(("grp", "kv"), "tp"), check_vma=False
    )
```

```python
import functools

import jax
import jax.numpy as jnp
from jax import lax
from jax.experimental import pallas as pl
from jax.experimental.pallas import tpu as pltpu
from jax.sharding import PartitionSpec as P

HD = 128
QB = 128
KB = 32
PIECES = 4

epsilon = 1e-06
theta = 10000.0
MESH = pl.DeviceIdType.MESH


def rotary_tables(positions):
    frequency = theta ** (-jnp.arange(0, HD, 2, dtype=jnp.float32) / HD)
    angles = positions.astype(jnp.float32)[:, None] * frequency[None, :]
    cosine, sine = jnp.cos(angles), jnp.sin(angles)
    return jnp.concatenate([cosine, cosine], 1), jnp.concatenate([-sine, sine], 1)


def remote(src, dst, send, recv, **where):
    return pltpu.make_async_remote_copy(
        src_ref=src, dst_ref=dst, send_sem=send, recv_sem=recv, device_id=where, device_id_type=MESH
    )


class TpRing:
    def __init__(self, own, slots, send, recv, rows):
        self.n = lax.axis_size("tp")
        self.me = lax.axis_index("tp")
        self.right = lax.rem(self.me + 1, self.n)
        self.left = lax.rem(self.me + self.n - 1, self.n)
        self.far = lax.rem(self.me + 2, self.n)
        self.own, self.slots, self.send, self.recv, self.rows = own, slots, send, recv, rows

    def copy(self, chunk, kind):
        half = self.rows // 2
        start, size, source, to = {
            0: (0, self.rows, None, self.right),
            1: (0, self.rows, None, self.left),
            2: (0, half, self.left, self.right),
            3: (half, half, self.right, self.left),
        }[kind]
        at = pl.ds(chunk * self.rows + start, size)
        src = self.own.at[at] if source is None else self.slots.at[source, at]
        dst = self.slots.at[self.me if source is None else source, at]
        return remote(src, dst, self.send.at[chunk, kind], self.recv.at[chunk, kind], tp=to)

    def begin(self, chunk):
        self.copy(chunk, 0).start()
        self.copy(chunk, 1).start()

    def hand_on(self, chunk):
        self.copy(chunk, 0).wait_recv()
        self.copy(chunk, 2).start()
        self.copy(chunk, 1).wait_recv()
        self.copy(chunk, 3).start()

    def arrived(self, chunk):
        self.copy(chunk, 2).wait_recv()
        self.copy(chunk, 3).wait_recv()

    def sent(self, chunk):
        for kind in range(4):
            self.copy(chunk, kind).wait_send()


def layer_kernel(
    tok, gain, wq, wk, wv, w_out, cos, sin, listed, sel, out,
    slots, weights, queries, need, transit, keys, attended, mixing,
    send_t, recv_t, send_z, recv_z, send_c, recv_c, send_m, recv_m, local, go,
):
    rows, width = tok.shape
    tp = lax.axis_size("tp")
    chunk_rows = rows // PIECES
    devices = lax.axis_size("kv")
    chips = devices // 2
    most_up, most_down = reach(chips)
    mine = lax.axis_index("kv")
    z, core = mine // 2, lax.rem(mine, 2)
    partner = mine + 1 - 2 * core
    up = lax.rem(mine + 2, devices)
    down = lax.rem(mine + devices - 2, devices)
    q_cols, k_cols = wq.shape[1], wk.shape[1]
    ring = TpRing(tok, slots, send_t, recv_t, chunk_rows)
    mix_ring = TpRing(attended, mixing, send_m, recv_m, chunk_rows)

    loads = [
        pltpu.make_async_copy(wq, weights.at[:, pl.ds(0, q_cols)], local.at[0]),
        pltpu.make_async_copy(wk, weights.at[:, pl.ds(q_cols, k_cols)], local.at[1]),
        pltpu.make_async_copy(wv, weights.at[:, pl.ds(q_cols + k_cols, k_cols)], local.at[2]),
        pltpu.make_async_copy(tok, slots.at[ring.me], local.at[3]),
    ]
    for load in loads:
        load.start()

    barrier = pltpu.get_barrier_semaphore()

    def hail(**where):
        pl.semaphore_signal(barrier, inc=1, device_id=where, device_id_type=MESH)

    hail(tp=ring.right)
    hail(tp=ring.left)
    hail(kv=partner)
    hail(kv=down)

    @pl.when(z < chips - 1)
    def _():
        hail(kv=up)

    @pl.when(z == 0)
    def _():
        pl.semaphore_wait(barrier, 4)

    @pl.when(z > 0)
    def _():
        pl.semaphore_wait(barrier, 5)

    @pl.when(z == chips - 1)
    def _():
        pl.semaphore_signal(go, inc=1, device_id={"kv": up}, device_id_type=MESH)

    own_blocks = rows // KB
    chunk_blocks = chunk_rows // KB

    def piece_rows(piece):
        return pl.ds(piece * chunk_rows, chunk_rows)

    def piece_blocks(holder, piece):
        return pl.ds(holder * own_blocks + piece * chunk_blocks, chunk_blocks)

    def goes_up(step):
        return (step <= most_up) & (z - step + 1 >= 0) & (z < chips - 1)

    def comes_up(step):
        return (step <= most_up) & (z - step >= 0)

    def goes_down(step):
        return (step <= most_down) & (lax.rem(z + step - 1, chips) < most_down)

    def comes_down(step):
        return (step <= most_down) & (lax.rem(z + step, chips) < most_down)

    def send_up(step, piece):
        block = need.at[piece_blocks(lax.rem(z - step + 1 + chips, chips) * 2 + core, piece)]
        return remote(block, block, send_z.at[0, step, piece], recv_z.at[0, step, piece], kv=up)

    def send_down(step, piece, from_transit, to_transit):
        chip = lax.rem(z + step - 1, chips)
        kept = need.at[piece_blocks(chip * 2 + core, piece)]
        passing = transit.at[piece_blocks(lax.rem(chip, most_down), piece)]
        return remote(
            passing if from_transit else kept, passing if to_transit else kept,
            send_z.at[1, step, piece], recv_z.at[1, step, piece], kv=down,
        )

    def across(direction, step, piece):
        chip = lax.rem(z - step + chips, chips) if direction == 0 else lax.rem(z + step, chips)
        block = need.at[piece_blocks(chip * 2 + core, piece)]
        return remote(
            block, block, send_c.at[direction, step], recv_c.at[direction, step], kv=partner
        )

    def across_whole(direction, step):
        block = need.at[pl.ds(mine * own_blocks, own_blocks)]
        return remote(
            block, block, send_c.at[direction, step], recv_c.at[direction, step], kv=partner
        )

    def project(chunk):
        at = piece_rows(chunk)
        total = jnp.zeros((chunk_rows, weights.shape[1]), jnp.float32)
        squares = jnp.zeros((chunk_rows, 1), jnp.float32)
        for t in range(tp):
            block = slots[t, at, :].astype(jnp.float32)
            squares += jnp.sum(block * block, axis=1, keepdims=True)
            scaled = (block * gain[:, t * width:(t + 1) * width].astype(jnp.float32)).astype(
                jnp.bfloat16
            )
            total += jnp.dot(
                scaled, weights[t * width:(t + 1) * width, :], preferred_element_type=jnp.float32
            )
        total *= lax.rsqrt(squares / (tp * width) + epsilon)
        cosine, sine = cos[at, :], sin[at, :]
        heads = []
        for h in range((q_cols + k_cols) // HD):
            head = total[:, h * HD:(h + 1) * HD]
            heads.append((head * cosine + pltpu.roll(head, HD // 2, 1) * sine).astype(jnp.bfloat16))
        for h in range(q_cols // HD):
            queries[at, h * HD:(h + 1) * HD] = heads[h]
        kept = piece_blocks(mine, chunk)
        values = total[:, q_cols + k_cols:].astype(jnp.bfloat16)
        need[kept, :, 0:k_cols] = heads[-1].reshape(chunk_blocks, KB, k_cols)
        need[kept, :, k_cols:2 * k_cols] = values.reshape(chunk_blocks, KB, k_cols)

        @pl.when(goes_up(1))
        def _():
            send_up(1, chunk).start()

        @pl.when(goes_down(1) & (z > 0))
        def _():
            send_down(1, chunk, False, True).start()

    ring.begin(0)
    ring.begin(1)
    for load in loads:
        load.wait()
    for chunk in range(PIECES):
        if chunk == 0:
            ring.hand_on(0)
            ring.begin(2)
            ring.hand_on(1)
            ring.begin(3)
        elif chunk + 1 < PIECES:
            ring.hand_on(chunk + 1)
        ring.arrived(chunk)
        project(chunk)
    give = across_whole(0, 0)
    give.start()

    blocks, listed_slots = sel.shape
    wide = listed_slots * KB
    heads_here = q_cols // HD

    def attend(b, key_pos):
        @pl.loop(0, listed_slots, unroll=4)
        def _(s):
            keys[pl.ds(pl.multiple_of(s * KB, KB), KB), :] = need[jnp.maximum(listed[b, s], 0)]

        q_pos = mine * rows + b * QB + lax.broadcasted_iota(jnp.int32, (QB, wide), 0)
        allowed = jnp.broadcast_to(key_pos[b:b + 1, :], (QB, wide)) <= q_pos
        for h in range(heads_here):
            score = lax.dot_general(
                queries[b * QB:(b + 1) * QB, h * HD:(h + 1) * HD], keys[:, 0:HD],
                (((1,), (1,)), ((), ())), preferred_element_type=jnp.float32,
            ) * HD ** (-0.5)
            score = jnp.where(allowed, score, -jnp.inf)
            raised = jnp.exp(score - jnp.max(score, axis=1, keepdims=True))
            parts = (raised / jnp.sum(raised, axis=1, keepdims=True)).astype(jnp.bfloat16)
            attended[b * QB:(b + 1) * QB, h * HD:(h + 1) * HD] = jnp.dot(
                parts, keys[:, HD:2 * HD], preferred_element_type=jnp.float32
            ).astype(jnp.bfloat16)
        mixing[mix_ring.me, b * QB:(b + 1) * QB, :] = attended[b * QB:(b + 1) * QB, :]

    def mix(chunk):
        at = piece_rows(chunk)
        total = jnp.zeros((chunk_rows, out.shape[1]), jnp.float32)
        for t in range(tp):
            total += jnp.dot(
                mixing[t, at, :], w_out[t * q_cols:(t + 1) * q_cols, :],
                preferred_element_type=jnp.float32,
            )
        out[at, :] = total.astype(jnp.bfloat16)

    def finish():
        give.wait()

        @pl.loop(1, jnp.minimum(z, most_up) + 1)
        def _(step):
            across_whole(0, step).wait()

        @pl.loop(jnp.maximum(chips - z, 1), most_down + 1)
        def _(step):
            across_whole(1, step).wait()

        spread = (
            lax.broadcasted_iota(jnp.int32, (listed_slots, wide), 1) // KB
            == lax.broadcasted_iota(jnp.int32, (listed_slots, wide), 0)
        ).astype(jnp.float32)
        ids = sel[...]
        safe = jnp.where(ids < 0, 1 << 20, ids)
        high = (safe // 64).astype(jnp.float32)
        low = lax.rem(safe, 64).astype(jnp.float32)
        found = jnp.dot(high, spread, preferred_element_type=jnp.float32) * 64.0 + jnp.dot(
            low, spread, preferred_element_type=jnp.float32
        )
        key_pos = found.astype(jnp.int32) * KB + lax.rem(
            lax.broadcasted_iota(jnp.int32, (blocks, wide), 1), KB
        )
        for b in range(PIECES):
            attend(b, key_pos)
            mix_ring.begin(b)
            if b:
                mix_ring.hand_on(b - 1)
        for b in range(PIECES):
            if b == 0:
                mix_ring.hand_on(PIECES - 1)
            mix_ring.arrived(b)
            mix(b)

    attend_at = jnp.minimum(z, most_up)

    @pl.loop(0, most_up + 1)
    def _(step):
        for piece in range(PIECES):
            @pl.when((step > 0) & comes_up(step))
            def _():
                send_up(step, piece).wait_recv()

                @pl.when(goes_up(step + 1))
                def _():
                    send_up(step + 1, piece).start()

                across(0, step, piece).start()

            @pl.when((step > 0) & comes_down(step))
            def _():
                send_down(step, piece, False, False).wait_recv()
                wrapped = z + step >= chips
                onward = step < most_down

                @pl.when(onward & wrapped)
                def _():
                    send_down(step + 1, piece, False, False).start()

                @pl.when(onward & jnp.logical_not(wrapped) & (z > 0))
                def _():
                    send_down(step + 1, piece, True, True).start()

                @pl.when(onward & (z == 0))
                def _():
                    send_down(step + 1, piece, True, False).start()

                @pl.when(wrapped)
                def _():
                    across(1, step, piece).start()

        @pl.when(step == attend_at)
        def _():
            finish()

        @pl.when((step == 0) & (z == 0))
        def _():
            pl.semaphore_wait(go, 1)
            for piece in range(PIECES):
                send_down(1, piece, False, False).start()

    for chunk in range(PIECES):
        ring.sent(chunk)
        mix_ring.sent(chunk)

    @pl.loop(1, most_up + 1)
    def _(step):
        for piece in range(PIECES):
            @pl.when(goes_up(step))
            def _():
                send_up(step, piece).wait_send()

            @pl.when(goes_down(step))
            def _():
                send_down(step, piece, False, False).wait_send()


def reach(chips):
    most_up = chips // 2 + 1
    return most_up, chips - 1 - most_up


def layer(tokens, gain, w_query, w_key, w_value, w_out, cosine, sine, select):
    rows, width = tokens.shape
    devices = lax.axis_size("kv")
    tp = lax.axis_size("tp")
    q_cols, k_cols = w_query.shape[1], w_key.shape[1]
    most_up, most_down = reach(devices // 2)
    dma = pltpu.SemaphoreType.DMA
    bf16 = jnp.bfloat16
    vmem = pl.BlockSpec(memory_space=pltpu.VMEM)
    hbm = pl.BlockSpec(memory_space=pl.ANY)
    smem = pl.BlockSpec(memory_space=pltpu.SMEM)
    return pl.pallas_call(
        layer_kernel,
        out_shape=jax.ShapeDtypeStruct((rows, w_out.shape[1]), bf16),
        in_specs=[vmem, vmem, hbm, hbm, hbm, vmem, vmem, vmem, smem, vmem],
        out_specs=vmem,
        scratch_shapes=[
            pltpu.VMEM((tp, rows, width), bf16),
            pltpu.VMEM((tp * width, q_cols + 2 * k_cols), bf16),
            pltpu.VMEM((rows, q_cols), bf16),
            pltpu.VMEM((devices * rows // KB, KB, 2 * k_cols), bf16),
            pltpu.VMEM((most_down * rows // KB, KB, 2 * k_cols), bf16),
            pltpu.VMEM((select.shape[1] * KB, 2 * k_cols), bf16),
            pltpu.VMEM((rows, q_cols), bf16),
            pltpu.VMEM((tp, rows, q_cols), bf16),
            dma((PIECES, 4)),
            dma((PIECES, 4)),
            dma((2, most_up + 1, PIECES)),
            dma((2, most_up + 1, PIECES)),
            dma((2, most_up + 1)),
            dma((2, most_up + 1)),
            dma((PIECES, 4)),
            dma((PIECES, 4)),
            dma((4,)),
            pltpu.SemaphoreType.REGULAR,
        ],
        compiler_params=pltpu.CompilerParams(collective_id=0, has_side_effects=True),
        name="layer",
    )(tokens, gain, w_query, w_key, w_value, w_out, cosine, sine, select, select)


def per_device(tokens, gain, w_query, w_key, w_value, w_out, select):
    rows = tokens.shape[0]
    positions = lax.axis_index("kv") * rows + jnp.arange(rows, dtype=jnp.int32)
    cosine, sine = rotary_tables(positions)
    return layer(
        tokens, gain.reshape(1, -1), w_query, w_key, w_value, w_out, cosine, sine, select
    )


def solution(mesh):
    placed = (
        P(("grp", "kv"), "tp"),
        P(),
        P(None, "tp"),
        P(None, "tp"),
        P(None, "tp"),
        P(None, "tp"),
        P(("grp", "kv"), None),
    )
    return jax.shard_map(
        per_device, mesh=mesh, in_specs=placed, out_specs=P(("grp", "kv"), "tp"), check_vma=False
    )
```

```python
import functools

import jax
import jax.numpy as jnp
from jax import lax
from jax.experimental import pallas as pl
from jax.experimental.pallas import tpu as pltpu
from jax.sharding import PartitionSpec as P

HD = 128
QB = 128
KB = 32
PIECES = 4
IN_FLIGHT = 4
FAR_FIRST = 6

epsilon = 1e-06
theta = 10000.0
MESH = pl.DeviceIdType.MESH


def rotary_tables(positions):
    frequency = theta ** (-jnp.arange(0, HD, 2, dtype=jnp.float32) / HD)
    angles = positions.astype(jnp.float32)[:, None] * frequency[None, :]
    cosine, sine = jnp.cos(angles), jnp.sin(angles)
    return jnp.concatenate([cosine, cosine], 1), jnp.concatenate([-sine, sine], 1)


def remote(src, dst, send, recv, **where):
    return pltpu.make_async_remote_copy(
        src_ref=src, dst_ref=dst, send_sem=send, recv_sem=recv, device_id=where, device_id_type=MESH
    )


class TpRing:
    def __init__(self, own, slots, send, recv, rows):
        self.n = lax.axis_size("tp")
        self.me = lax.axis_index("tp")
        self.right = lax.rem(self.me + 1, self.n)
        self.left = lax.rem(self.me + self.n - 1, self.n)
        self.far = lax.rem(self.me + 2, self.n)
        self.own, self.slots, self.send, self.recv, self.rows = own, slots, send, recv, rows

    def copy(self, chunk, kind):
        half = self.rows // 2
        start, size, source, to = {
            0: (0, self.rows, None, self.right),
            1: (0, self.rows, None, self.left),
            2: (0, half, self.left, self.right),
            3: (half, half, self.right, self.left),
        }[kind]
        at = pl.ds(chunk * self.rows + start, size)
        src = self.own.at[at] if source is None else self.slots.at[source, at]
        dst = self.slots.at[self.me if source is None else source, at]
        return remote(src, dst, self.send.at[chunk, kind], self.recv.at[chunk, kind], tp=to)

    def begin(self, chunk):
        self.copy(chunk, 0).start()
        self.copy(chunk, 1).start()

    def hand_on(self, chunk):
        self.copy(chunk, 0).wait_recv()
        self.copy(chunk, 2).start()
        self.copy(chunk, 1).wait_recv()
        self.copy(chunk, 3).start()

    def arrived(self, chunk):
        self.copy(chunk, 2).wait_recv()
        self.copy(chunk, 3).wait_recv()

    def sent(self, chunk):
        for kind in range(4):
            self.copy(chunk, kind).wait_send()


def layer_kernel(
    tok, gain, wq, wk, wv, w_out, cos, sin, listed, sel, out,
    slots, weights, queries, need, keys, attended, mixing,
    send_t, recv_t, send_z, recv_z, send_c, recv_c, send_m, recv_m, local, go,
):
    rows, width = tok.shape
    tp = lax.axis_size("tp")
    chunk_rows = rows // PIECES
    devices = lax.axis_size("kv")
    chips = devices // 2
    most_up, most_down = reach(chips)
    mine = lax.axis_index("kv")
    z, core = mine // 2, lax.rem(mine, 2)
    partner = mine + 1 - 2 * core
    up = lax.rem(mine + 2, devices)
    down = lax.rem(mine + devices - 2, devices)
    q_cols, k_cols = wq.shape[1], wk.shape[1]
    ring = TpRing(tok, slots, send_t, recv_t, chunk_rows)
    mix_ring = TpRing(attended, mixing, send_m, recv_m, chunk_rows)

    loads = [
        pltpu.make_async_copy(wq, weights.at[:, pl.ds(0, q_cols)], local.at[0]),
        pltpu.make_async_copy(wk, weights.at[:, pl.ds(q_cols, k_cols)], local.at[1]),
        pltpu.make_async_copy(wv, weights.at[:, pl.ds(q_cols + k_cols, k_cols)], local.at[2]),
        pltpu.make_async_copy(tok, slots.at[ring.me], local.at[3]),
    ]
    for load in loads:
        load.start()

    barrier = pltpu.get_barrier_semaphore()
    end = chips - 1
    last = end * 2 + core

    def hail(**where):
        pl.semaphore_signal(barrier, inc=1, device_id=where, device_id_type=MESH)

    def let_go(chip):
        pl.semaphore_signal(go, inc=1, device_id={"kv": chip * 2 + core}, device_id_type=MESH)

    hail(tp=ring.right)
    hail(tp=ring.left)
    hail(kv=partner)

    @pl.when(z > 0)
    def _():
        hail(kv=mine - 2)

    @pl.when(z < end)
    def _():
        hail(kv=mine + 2)

    @pl.when(z < most_down)
    def _():
        hail(kv=last)

    @pl.when(z == 0)
    def _():
        pl.semaphore_wait(barrier, 4)

    @pl.when((z > 0) & (z < end))
    def _():
        pl.semaphore_wait(barrier, 5)

    @pl.when(z == end)
    def _():
        pl.semaphore_wait(barrier, 4 + most_down)
        for chip in range(IN_FLIGHT):
            let_go(chip)

    own_blocks = rows // KB
    chunk_blocks = chunk_rows // KB

    def piece_rows(piece):
        return pl.ds(piece * chunk_rows, chunk_rows)

    def piece_blocks(holder, piece):
        return pl.ds(holder * own_blocks + piece * chunk_blocks, chunk_blocks)

    def goes_up(step):
        return (step <= most_up) & (z - step + 1 >= 0) & (z < end)

    def comes_up(step):
        return (step <= most_up) & (z - step >= 0)

    def comes_down(step):
        return (step <= most_down) & (z + step >= chips)

    def goes_down(step):
        return (step <= most_down) & (z + step > chips)

    def send_up(step, piece):
        block = need.at[piece_blocks(lax.rem(z - step + 1 + chips, chips) * 2 + core, piece)]
        return remote(block, block, send_z.at[0, step, piece], recv_z.at[0, step, piece], kv=up)

    def send_down(step, piece):
        block = need.at[piece_blocks(lax.rem(z + step - 1, chips) * 2 + core, piece)]
        return remote(block, block, send_z.at[1, step, piece], recv_z.at[1, step, piece], kv=down)

    def send_far(piece):
        block = need.at[piece_blocks(mine, piece)]
        step = jnp.minimum(z + 1, most_down)
        return remote(block, block, send_z.at[1, step, piece], recv_z.at[1, step, piece], kv=last)

    def across(direction, step, piece):
        chip = lax.rem(z - step + chips, chips) if direction == 0 else lax.rem(z + step, chips)
        block = need.at[piece_blocks(chip * 2 + core, piece)]
        return remote(
            block, block, send_c.at[direction, step], recv_c.at[direction, step], kv=partner
        )

    def across_whole(direction, step):
        block = need.at[pl.ds(mine * own_blocks, own_blocks)]
        return remote(
            block, block, send_c.at[direction, step], recv_c.at[direction, step], kv=partner
        )

    def project(chunk):
        at = piece_rows(chunk)
        total = jnp.zeros((chunk_rows, weights.shape[1]), jnp.float32)
        squares = jnp.zeros((chunk_rows, 1), jnp.float32)
        for t in range(tp):
            block = slots[t, at, :].astype(jnp.float32)
            squares += jnp.sum(block * block, axis=1, keepdims=True)
            scaled = (block * gain[:, t * width:(t + 1) * width].astype(jnp.float32)).astype(
                jnp.bfloat16
            )
            total += jnp.dot(
                scaled, weights[t * width:(t + 1) * width, :], preferred_element_type=jnp.float32
            )
        total *= lax.rsqrt(squares / (tp * width) + epsilon)
        cosine, sine = cos[at, :], sin[at, :]
        heads = []
        for h in range((q_cols + k_cols) // HD):
            head = total[:, h * HD:(h + 1) * HD]
            heads.append((head * cosine + pltpu.roll(head, HD // 2, 1) * sine).astype(jnp.bfloat16))
        for h in range(q_cols // HD):
            queries[at, h * HD:(h + 1) * HD] = heads[h]
        kept = piece_blocks(mine, chunk)
        values = total[:, q_cols + k_cols:].astype(jnp.bfloat16)
        need[kept, :, 0:k_cols] = heads[-1].reshape(chunk_blocks, KB, k_cols)
        need[kept, :, k_cols:2 * k_cols] = values.reshape(chunk_blocks, KB, k_cols)

        @pl.when(goes_up(1))
        def _():
            send_up(1, chunk).start()

    def hand_up(step, piece):
        @pl.when(comes_up(step))
        def _():
            send_up(step, piece).wait_recv()

            @pl.when(goes_up(step + 1))
            def _():
                send_up(step + 1, piece).start()

            across(0, step, piece).start()

    ring.begin(0)
    ring.begin(1)
    for load in loads:
        load.wait()
    for chunk in range(PIECES):
        if chunk == 0:
            ring.hand_on(0)
            ring.begin(2)
            ring.hand_on(1)
            ring.begin(3)
        elif chunk + 1 < PIECES:
            ring.hand_on(chunk + 1)
        ring.arrived(chunk)
        project(chunk)
        for step in range(1, chunk + 1):
            hand_up(step, chunk - step)
    give = across_whole(0, 0)
    give.start()

    blocks, listed_slots = sel.shape
    wide = listed_slots * KB
    heads_here = q_cols // HD

    def attend(b, key_pos):
        @pl.loop(0, listed_slots, unroll=4)
        def _(s):
            keys[pl.ds(pl.multiple_of(s * KB, KB), KB), :] = need[jnp.maximum(listed[b, s], 0)]

        q_pos = mine * rows + b * QB + lax.broadcasted_iota(jnp.int32, (QB, wide), 0)
        allowed = jnp.broadcast_to(key_pos[b:b + 1, :], (QB, wide)) <= q_pos
        for h in range(heads_here):
            score = lax.dot_general(
                queries[b * QB:(b + 1) * QB, h * HD:(h + 1) * HD], keys[:, 0:HD],
                (((1,), (1,)), ((), ())), preferred_element_type=jnp.float32,
            ) * HD ** (-0.5)
            score = jnp.where(allowed, score, -jnp.inf)
            raised = jnp.exp(score - jnp.max(score, axis=1, keepdims=True))
            parts = (raised / jnp.sum(raised, axis=1, keepdims=True)).astype(jnp.bfloat16)
            attended[b * QB:(b + 1) * QB, h * HD:(h + 1) * HD] = jnp.dot(
                parts, keys[:, HD:2 * HD], preferred_element_type=jnp.float32
            ).astype(jnp.bfloat16)
        mixing[mix_ring.me, b * QB:(b + 1) * QB, :] = attended[b * QB:(b + 1) * QB, :]

    def mix(chunk):
        at = piece_rows(chunk)
        total = jnp.zeros((chunk_rows, out.shape[1]), jnp.float32)
        for t in range(tp):
            total += jnp.dot(
                mixing[t, at, :], w_out[t * q_cols:(t + 1) * q_cols, :],
                preferred_element_type=jnp.float32,
            )
        out[at, :] = total.astype(jnp.bfloat16)

    def finish():
        give.wait()

        @pl.loop(1, jnp.minimum(z, most_up) + 1)
        def _(step):
            across_whole(0, step).wait()

        @pl.loop(jnp.maximum(chips - z, 1), most_down + 1)
        def _(step):
            across_whole(1, step).wait()

        spread = (
            lax.broadcasted_iota(jnp.int32, (listed_slots, wide), 1) // KB
            == lax.broadcasted_iota(jnp.int32, (listed_slots, wide), 0)
        ).astype(jnp.float32)
        ids = sel[...]
        safe = jnp.where(ids < 0, 1 << 20, ids)
        high = (safe // 64).astype(jnp.float32)
        low = lax.rem(safe, 64).astype(jnp.float32)
        found = jnp.dot(high, spread, preferred_element_type=jnp.float32) * 64.0 + jnp.dot(
            low, spread, preferred_element_type=jnp.float32
        )
        key_pos = found.astype(jnp.int32) * KB + lax.rem(
            lax.broadcasted_iota(jnp.int32, (blocks, wide), 1), KB
        )
        for b in range(PIECES):
            attend(b, key_pos)
            mix_ring.begin(b)
            if b:
                mix_ring.hand_on(b - 1)
        for b in range(PIECES):
            if b == 0:
                mix_ring.hand_on(PIECES - 1)
            mix_ring.arrived(b)
            mix(b)

    attend_at = jnp.minimum(z, most_up)

    def go_far():
        pl.semaphore_wait(go, 1)
        for piece in range(PIECES):
            send_far(piece).start()

    @pl.loop(0, most_up + 1)
    def _(step):
        for piece in range(PIECES):
            @pl.when((step > 0) & (step + piece >= PIECES))
            def _():
                hand_up(step, piece)

            @pl.when((step > 0) & comes_down(step))
            def _():
                send_down(step, piece).wait_recv()

                @pl.when(goes_down(step + 1))
                def _():
                    send_down(step + 1, piece).start()

                across(1, step, piece).start()

        @pl.when((step > 0) & (step + IN_FLIGHT <= most_down) & (z == end))
        def _():
            let_go(jnp.minimum(step + IN_FLIGHT - 1, most_down - 1))

        @pl.when((step == attend_at) & (z >= FAR_FIRST) & (z < most_down))
        def _():
            go_far()

        @pl.when(step == attend_at)
        def _():
            finish()

        @pl.when((step == attend_at) & (z < FAR_FIRST))
        def _():
            go_far()

    for chunk in range(PIECES):
        ring.sent(chunk)
        mix_ring.sent(chunk)

    @pl.when(z < most_down)
    def _():
        for piece in range(PIECES):
            send_far(piece).wait_send()

    @pl.loop(1, most_up + 1)
    def _(step):
        for piece in range(PIECES):
            @pl.when(goes_up(step))
            def _():
                send_up(step, piece).wait_send()

            @pl.when(goes_down(step) & (step > 1))
            def _():
                send_down(step, piece).wait_send()


def reach(chips):
    most_up = chips // 2
    return most_up, chips - 1 - most_up


def layer(tokens, gain, w_query, w_key, w_value, w_out, cosine, sine, select):
    rows, width = tokens.shape
    devices = lax.axis_size("kv")
    tp = lax.axis_size("tp")
    q_cols, k_cols = w_query.shape[1], w_key.shape[1]
    most_up, most_down = reach(devices // 2)
    dma = pltpu.SemaphoreType.DMA
    bf16 = jnp.bfloat16
    vmem = pl.BlockSpec(memory_space=pltpu.VMEM)
    hbm = pl.BlockSpec(memory_space=pl.ANY)
    smem = pl.BlockSpec(memory_space=pltpu.SMEM)
    return pl.pallas_call(
        layer_kernel,
        out_shape=jax.ShapeDtypeStruct((rows, w_out.shape[1]), bf16),
        in_specs=[vmem, vmem, hbm, hbm, hbm, vmem, vmem, vmem, smem, vmem],
        out_specs=vmem,
        scratch_shapes=[
            pltpu.VMEM((tp, rows, width), bf16),
            pltpu.VMEM((tp * width, q_cols + 2 * k_cols), bf16),
            pltpu.VMEM((rows, q_cols), bf16),
            pltpu.VMEM((devices * rows // KB, KB, 2 * k_cols), bf16),
            pltpu.VMEM((select.shape[1] * KB, 2 * k_cols), bf16),
            pltpu.VMEM((rows, q_cols), bf16),
            pltpu.VMEM((tp, rows, q_cols), bf16),
            dma((PIECES, 4)),
            dma((PIECES, 4)),
            dma((2, most_up + 1, PIECES)),
            dma((2, most_up + 1, PIECES)),
            dma((2, most_up + 1)),
            dma((2, most_up + 1)),
            dma((PIECES, 4)),
            dma((PIECES, 4)),
            dma((4,)),
            pltpu.SemaphoreType.REGULAR,
        ],
        compiler_params=pltpu.CompilerParams(collective_id=0, has_side_effects=True),
        name="layer",
    )(tokens, gain, w_query, w_key, w_value, w_out, cosine, sine, select, select)


def per_device(tokens, gain, w_query, w_key, w_value, w_out, select):
    rows = tokens.shape[0]
    positions = lax.axis_index("kv") * rows + jnp.arange(rows, dtype=jnp.int32)
    cosine, sine = rotary_tables(positions)
    return layer(
        tokens, gain.reshape(1, -1), w_query, w_key, w_value, w_out, cosine, sine, select
    )


def solution(mesh):
    placed = (
        P(("grp", "kv"), "tp"),
        P(),
        P(None, "tp"),
        P(None, "tp"),
        P(None, "tp"),
        P(None, "tp"),
        P(("grp", "kv"), None),
    )
    return jax.shard_map(
        per_device, mesh=mesh, in_specs=placed, out_specs=P(("grp", "kv"), "tp"), check_vma=False
    )
```

```python
import functools

import jax
import jax.numpy as jnp
from jax import lax
from jax.experimental import pallas as pl
from jax.experimental.pallas import tpu as pltpu
from jax.sharding import PartitionSpec as P

HD = 128
QB = 128
KB = 32
PIECES = 4
IN_FLIGHT = 8
DOWN_LAG = 1

epsilon = 1e-06
theta = 10000.0
MESH = pl.DeviceIdType.MESH


def rotary_tables(positions):
    frequency = theta ** (-jnp.arange(0, HD, 2, dtype=jnp.float32) / HD)
    angles = positions.astype(jnp.float32)[:, None] * frequency[None, :]
    cosine, sine = jnp.cos(angles), jnp.sin(angles)
    return jnp.concatenate([cosine, cosine], 1), jnp.concatenate([-sine, sine], 1)


def remote(src, dst, send, recv, **where):
    return pltpu.make_async_remote_copy(
        src_ref=src, dst_ref=dst, send_sem=send, recv_sem=recv, device_id=where, device_id_type=MESH
    )


class TpRing:
    def __init__(self, own, slots, send, recv, rows):
        self.n = lax.axis_size("tp")
        self.me = lax.axis_index("tp")
        self.right = lax.rem(self.me + 1, self.n)
        self.left = lax.rem(self.me + self.n - 1, self.n)
        self.far = lax.rem(self.me + 2, self.n)
        self.own, self.slots, self.send, self.recv, self.rows = own, slots, send, recv, rows

    def copy(self, chunk, kind):
        half = self.rows // 2
        start, size, source, to = {
            0: (0, self.rows, None, self.right),
            1: (0, self.rows, None, self.left),
            2: (0, half, self.left, self.right),
            3: (half, half, self.right, self.left),
        }[kind]
        at = pl.ds(chunk * self.rows + start, size)
        src = self.own.at[at] if source is None else self.slots.at[source, at]
        dst = self.slots.at[self.me if source is None else source, at]
        return remote(src, dst, self.send.at[chunk, kind], self.recv.at[chunk, kind], tp=to)

    def begin(self, chunk):
        self.copy(chunk, 0).start()
        self.copy(chunk, 1).start()

    def hand_on(self, chunk):
        self.copy(chunk, 0).wait_recv()
        self.copy(chunk, 2).start()
        self.copy(chunk, 1).wait_recv()
        self.copy(chunk, 3).start()

    def arrived(self, chunk):
        self.copy(chunk, 2).wait_recv()
        self.copy(chunk, 3).wait_recv()

    def sent(self, chunk):
        for kind in range(4):
            self.copy(chunk, kind).wait_send()


def layer_kernel(
    tok, gain, wq, wk, wv, w_out, cos, sin, listed, sel, out,
    slots, weights, queries, need, keys, attended, mixing,
    send_t, recv_t, send_z, recv_z, send_c, recv_c, send_m, recv_m, local, go,
):
    rows, width = tok.shape
    tp = lax.axis_size("tp")
    chunk_rows = rows // PIECES
    devices = lax.axis_size("kv")
    chips = devices // 2
    most_up, most_down = reach(chips)
    mine = lax.axis_index("kv")
    z, core = mine // 2, lax.rem(mine, 2)
    partner = mine + 1 - 2 * core
    up = lax.rem(mine + 2, devices)
    down = lax.rem(mine + devices - 2, devices)
    q_cols, k_cols = wq.shape[1], wk.shape[1]
    ring = TpRing(tok, slots, send_t, recv_t, chunk_rows)
    mix_ring = TpRing(attended, mixing, send_m, recv_m, chunk_rows)

    loads = [
        pltpu.make_async_copy(wq, weights.at[:, pl.ds(0, q_cols)], local.at[0]),
        pltpu.make_async_copy(wk, weights.at[:, pl.ds(q_cols, k_cols)], local.at[1]),
        pltpu.make_async_copy(wv, weights.at[:, pl.ds(q_cols + k_cols, k_cols)], local.at[2]),
        pltpu.make_async_copy(tok, slots.at[ring.me], local.at[3]),
    ]
    for load in loads:
        load.start()

    barrier = pltpu.get_barrier_semaphore()
    end = chips - 1
    last = end * 2 + core

    def hail(**where):
        pl.semaphore_signal(barrier, inc=1, device_id=where, device_id_type=MESH)

    def let_go(chip):
        pl.semaphore_signal(go, inc=1, device_id={"kv": chip * 2 + core}, device_id_type=MESH)

    hail(tp=ring.right)
    hail(tp=ring.left)
    hail(kv=partner)

    @pl.when(z > 0)
    def _():
        hail(kv=mine - 2)

    @pl.when(z < end)
    def _():
        hail(kv=mine + 2)

    @pl.when(z < most_down)
    def _():
        hail(kv=last)

    @pl.when(z == 0)
    def _():
        pl.semaphore_wait(barrier, 4)

    @pl.when((z > 0) & (z < end))
    def _():
        pl.semaphore_wait(barrier, 5)

    @pl.when(z == end)
    def _():
        pl.semaphore_wait(barrier, 4 + most_down)
        for chip in range(IN_FLIGHT):
            let_go(chip)

    own_blocks = rows // KB
    chunk_blocks = chunk_rows // KB

    def piece_rows(piece):
        return pl.ds(piece * chunk_rows, chunk_rows)

    def piece_blocks(holder, piece):
        return pl.ds(holder * own_blocks + piece * chunk_blocks, chunk_blocks)

    def goes_up(step):
        return (step <= most_up) & (z - step + 1 >= 0) & (z < end)

    def comes_up(step):
        return (step <= most_up) & (z - step >= 0)

    def comes_down(step):
        return (step <= most_down) & (z + step >= chips)

    def goes_down(step):
        return (step <= most_down) & (z + step > chips)

    def send_up(step, piece):
        block = need.at[piece_blocks(lax.rem(z - step + 1 + chips, chips) * 2 + core, piece)]
        return remote(block, block, send_z.at[0, step, piece], recv_z.at[0, step, piece], kv=up)

    def send_down(step, piece):
        block = need.at[piece_blocks(lax.rem(z + step - 1, chips) * 2 + core, piece)]
        return remote(block, block, send_z.at[1, step, piece], recv_z.at[1, step, piece], kv=down)

    def send_far(piece):
        block = need.at[piece_blocks(mine, piece)]
        step = jnp.minimum(z + 1, most_down)
        return remote(block, block, send_z.at[1, step, piece], recv_z.at[1, step, piece], kv=last)

    def across(direction, step, piece):
        chip = lax.rem(z - step + chips, chips) if direction == 0 else lax.rem(z + step, chips)
        block = need.at[piece_blocks(chip * 2 + core, piece)]
        return remote(
            block, block, send_c.at[direction, step], recv_c.at[direction, step], kv=partner
        )

    def across_whole(direction, step):
        block = need.at[pl.ds(mine * own_blocks, own_blocks)]
        return remote(
            block, block, send_c.at[direction, step], recv_c.at[direction, step], kv=partner
        )

    def project(chunk):
        at = piece_rows(chunk)
        total = jnp.zeros((chunk_rows, weights.shape[1]), jnp.float32)
        squares = jnp.zeros((chunk_rows, 1), jnp.float32)
        for t in range(tp):
            block = slots[t, at, :].astype(jnp.float32)
            squares += jnp.sum(block * block, axis=1, keepdims=True)
            scaled = (block * gain[:, t * width:(t + 1) * width].astype(jnp.float32)).astype(
                jnp.bfloat16
            )
            total += jnp.dot(
                scaled, weights[t * width:(t + 1) * width, :], preferred_element_type=jnp.float32
            )
        total *= lax.rsqrt(squares / (tp * width) + epsilon)
        cosine, sine = cos[at, :], sin[at, :]
        heads = []
        for h in range((q_cols + k_cols) // HD):
            head = total[:, h * HD:(h + 1) * HD]
            heads.append((head * cosine + pltpu.roll(head, HD // 2, 1) * sine).astype(jnp.bfloat16))
        for h in range(q_cols // HD):
            queries[at, h * HD:(h + 1) * HD] = heads[h]
        kept = piece_blocks(mine, chunk)
        values = total[:, q_cols + k_cols:].astype(jnp.bfloat16)
        need[kept, :, 0:k_cols] = heads[-1].reshape(chunk_blocks, KB, k_cols)
        need[kept, :, k_cols:2 * k_cols] = values.reshape(chunk_blocks, KB, k_cols)

        @pl.when(goes_up(1))
        def _():
            send_up(1, chunk).start()

    def hand_up(step, piece):
        @pl.when(comes_up(step))
        def _():
            send_up(step, piece).wait_recv()

            @pl.when(goes_up(step + 1))
            def _():
                send_up(step + 1, piece).start()

            across(0, step, piece).start()

    ring.begin(0)
    ring.begin(1)
    for load in loads:
        load.wait()
    for chunk in range(PIECES):
        if chunk == 0:
            ring.hand_on(0)
            ring.begin(2)
            ring.hand_on(1)
            ring.begin(3)
        elif chunk + 1 < PIECES:
            ring.hand_on(chunk + 1)
        ring.arrived(chunk)
        project(chunk)
        for step in range(1, chunk + 1):
            hand_up(step, chunk - step)
    give = across_whole(0, 0)
    give.start()

    blocks, listed_slots = sel.shape
    wide = listed_slots * KB
    heads_here = q_cols // HD

    def attend(b, key_pos):
        @pl.loop(0, listed_slots, unroll=4)
        def _(s):
            keys[pl.ds(pl.multiple_of(s * KB, KB), KB), :] = need[jnp.maximum(listed[b, s], 0)]

        q_pos = mine * rows + b * QB + lax.broadcasted_iota(jnp.int32, (QB, wide), 0)
        allowed = jnp.broadcast_to(key_pos[b:b + 1, :], (QB, wide)) <= q_pos
        for h in range(heads_here):
            score = lax.dot_general(
                queries[b * QB:(b + 1) * QB, h * HD:(h + 1) * HD], keys[:, 0:HD],
                (((1,), (1,)), ((), ())), preferred_element_type=jnp.float32,
            ) * HD ** (-0.5)
            score = jnp.where(allowed, score, -jnp.inf)
            raised = jnp.exp(score - jnp.max(score, axis=1, keepdims=True))
            parts = (raised / jnp.sum(raised, axis=1, keepdims=True)).astype(jnp.bfloat16)
            attended[b * QB:(b + 1) * QB, h * HD:(h + 1) * HD] = jnp.dot(
                parts, keys[:, HD:2 * HD], preferred_element_type=jnp.float32
            ).astype(jnp.bfloat16)
        mixing[mix_ring.me, b * QB:(b + 1) * QB, :] = attended[b * QB:(b + 1) * QB, :]

    def mix(chunk):
        at = piece_rows(chunk)
        total = jnp.zeros((chunk_rows, out.shape[1]), jnp.float32)
        for t in range(tp):
            total += jnp.dot(
                mixing[t, at, :], w_out[t * q_cols:(t + 1) * q_cols, :],
                preferred_element_type=jnp.float32,
            )
        out[at, :] = total.astype(jnp.bfloat16)

    def finish():
        give.wait()

        @pl.loop(1, jnp.minimum(z, most_up) + 1)
        def _(step):
            across_whole(0, step).wait()

        @pl.loop(jnp.maximum(chips - z, 1), most_down + 1)
        def _(step):
            across_whole(1, step).wait()

        spread = (
            lax.broadcasted_iota(jnp.int32, (listed_slots, wide), 1) // KB
            == lax.broadcasted_iota(jnp.int32, (listed_slots, wide), 0)
        ).astype(jnp.float32)
        ids = sel[...]
        safe = jnp.where(ids < 0, 1 << 20, ids)
        high = (safe // 64).astype(jnp.float32)
        low = lax.rem(safe, 64).astype(jnp.float32)
        found = jnp.dot(high, spread, preferred_element_type=jnp.float32) * 64.0 + jnp.dot(
            low, spread, preferred_element_type=jnp.float32
        )
        key_pos = found.astype(jnp.int32) * KB + lax.rem(
            lax.broadcasted_iota(jnp.int32, (blocks, wide), 1), KB
        )
        for b in range(PIECES):
            attend(b, key_pos)
            mix_ring.begin(b)
            if b:
                mix_ring.hand_on(b - 1)
        for b in range(PIECES):
            if b == 0:
                mix_ring.hand_on(PIECES - 1)
            mix_ring.arrived(b)
            mix(b)

    attend_at = jnp.minimum(z, most_up)

    def go_far():
        pl.semaphore_wait(go, 1)
        for piece in range(PIECES):
            send_far(piece).start()

    @pl.loop(0, most_up + 1)
    def _(step):
        for piece in range(PIECES):
            @pl.when((step > 0) & (step + piece >= PIECES))
            def _():
                hand_up(step, piece)

        down_step = step - DOWN_LAG

        for piece in range(PIECES):
            @pl.when((down_step > 0) & comes_down(down_step))
            def _():
                send_down(down_step, piece).wait_recv()

                @pl.when(goes_down(down_step + 1))
                def _():
                    send_down(down_step + 1, piece).start()

                across(1, down_step, piece).start()

        @pl.when((down_step > 0) & (down_step + IN_FLIGHT <= most_down) & (z == end))
        def _():
            let_go(jnp.minimum(down_step + IN_FLIGHT - 1, most_down - 1))

        @pl.when((step == attend_at) & (z < most_down))
        def _():
            go_far()

        @pl.when(step == attend_at)
        def _():
            finish()

    for chunk in range(PIECES):
        ring.sent(chunk)
        mix_ring.sent(chunk)

    @pl.when(z < most_down)
    def _():
        for piece in range(PIECES):
            send_far(piece).wait_send()

    @pl.loop(1, most_up + 1)
    def _(step):
        for piece in range(PIECES):
            @pl.when(goes_up(step))
            def _():
                send_up(step, piece).wait_send()

            @pl.when(goes_down(step) & (step > 1))
            def _():
                send_down(step, piece).wait_send()


def reach(chips):
    most_up = chips // 2
    return most_up, chips - 1 - most_up


def layer(tokens, gain, w_query, w_key, w_value, w_out, cosine, sine, select):
    rows, width = tokens.shape
    devices = lax.axis_size("kv")
    tp = lax.axis_size("tp")
    q_cols, k_cols = w_query.shape[1], w_key.shape[1]
    most_up, most_down = reach(devices // 2)
    dma = pltpu.SemaphoreType.DMA
    bf16 = jnp.bfloat16
    vmem = pl.BlockSpec(memory_space=pltpu.VMEM)
    hbm = pl.BlockSpec(memory_space=pl.ANY)
    smem = pl.BlockSpec(memory_space=pltpu.SMEM)
    return pl.pallas_call(
        layer_kernel,
        out_shape=jax.ShapeDtypeStruct((rows, w_out.shape[1]), bf16),
        in_specs=[vmem, vmem, hbm, hbm, hbm, vmem, vmem, vmem, smem, vmem],
        out_specs=vmem,
        scratch_shapes=[
            pltpu.VMEM((tp, rows, width), bf16),
            pltpu.VMEM((tp * width, q_cols + 2 * k_cols), bf16),
            pltpu.VMEM((rows, q_cols), bf16),
            pltpu.VMEM((devices * rows // KB, KB, 2 * k_cols), bf16),
            pltpu.VMEM((select.shape[1] * KB, 2 * k_cols), bf16),
            pltpu.VMEM((rows, q_cols), bf16),
            pltpu.VMEM((tp, rows, q_cols), bf16),
            dma((PIECES, 4)),
            dma((PIECES, 4)),
            dma((2, most_up + 1, PIECES)),
            dma((2, most_up + 1, PIECES)),
            dma((2, most_up + 1)),
            dma((2, most_up + 1)),
            dma((PIECES, 4)),
            dma((PIECES, 4)),
            dma((4,)),
            pltpu.SemaphoreType.REGULAR,
        ],
        compiler_params=pltpu.CompilerParams(collective_id=0, has_side_effects=True),
        name="layer",
    )(tokens, gain, w_query, w_key, w_value, w_out, cosine, sine, select, select)


def per_device(tokens, gain, w_query, w_key, w_value, w_out, select):
    rows = tokens.shape[0]
    positions = lax.axis_index("kv") * rows + jnp.arange(rows, dtype=jnp.int32)
    cosine, sine = rotary_tables(positions)
    return layer(
        tokens, gain.reshape(1, -1), w_query, w_key, w_value, w_out, cosine, sine, select
    )


def solution(mesh):
    placed = (
        P(("grp", "kv"), "tp"),
        P(),
        P(None, "tp"),
        P(None, "tp"),
        P(None, "tp"),
        P(None, "tp"),
        P(("grp", "kv"), None),
    )
    return jax.shard_map(
        per_device, mesh=mesh, in_specs=placed, out_specs=P(("grp", "kv"), "tp"), check_vma=False
    )
```

```python
import functools

import jax
import jax.numpy as jnp
from jax import lax
from jax.experimental import pallas as pl
from jax.experimental.pallas import tpu as pltpu
from jax.sharding import PartitionSpec as P

HD = 128
QB = 128
KB = 32
PIECES = 4
DOWN_LAG = 1

epsilon = 1e-06
theta = 10000.0
MESH = pl.DeviceIdType.MESH


def rotary_tables(positions):
    frequency = theta ** (-jnp.arange(0, HD, 2, dtype=jnp.float32) / HD)
    angles = positions.astype(jnp.float32)[:, None] * frequency[None, :]
    cosine, sine = jnp.cos(angles), jnp.sin(angles)
    return jnp.concatenate([cosine, cosine], 1), jnp.concatenate([-sine, sine], 1)


def remote(src, dst, send, recv, **where):
    return pltpu.make_async_remote_copy(
        src_ref=src, dst_ref=dst, send_sem=send, recv_sem=recv, device_id=where, device_id_type=MESH
    )


class TpRing:
    def __init__(self, own, slots, send, recv, rows):
        self.n = lax.axis_size("tp")
        self.me = lax.axis_index("tp")
        self.right = lax.rem(self.me + 1, self.n)
        self.left = lax.rem(self.me + self.n - 1, self.n)
        self.far = lax.rem(self.me + 2, self.n)
        self.own, self.slots, self.send, self.recv, self.rows = own, slots, send, recv, rows

    def copy(self, chunk, kind):
        half = self.rows // 2
        start, size, source, to = {
            0: (0, self.rows, None, self.right),
            1: (0, self.rows, None, self.left),
            2: (0, half, self.left, self.right),
            3: (half, half, self.right, self.left),
        }[kind]
        at = pl.ds(chunk * self.rows + start, size)
        src = self.own.at[at] if source is None else self.slots.at[source, at]
        dst = self.slots.at[self.me if source is None else source, at]
        return remote(src, dst, self.send.at[chunk, kind], self.recv.at[chunk, kind], tp=to)

    def begin(self, chunk):
        self.copy(chunk, 0).start()
        self.copy(chunk, 1).start()

    def hand_on(self, chunk):
        self.copy(chunk, 0).wait_recv()
        self.copy(chunk, 2).start()
        self.copy(chunk, 1).wait_recv()
        self.copy(chunk, 3).start()

    def arrived(self, chunk):
        self.copy(chunk, 2).wait_recv()
        self.copy(chunk, 3).wait_recv()

    def sent(self, chunk):
        for kind in range(4):
            self.copy(chunk, kind).wait_send()


def layer_kernel(
    tok, gain, wq, wk, wv, w_out, cos, sin, listed, sel, out,
    slots, weights, queries, need, keys, attended, mixing,
    send_t, recv_t, send_z, recv_z, send_c, recv_c, send_m, recv_m, local, go,
):
    rows, width = tok.shape
    tp = lax.axis_size("tp")
    chunk_rows = rows // PIECES
    devices = lax.axis_size("kv")
    chips = devices // 2
    most_up, most_down = reach(chips)
    mine = lax.axis_index("kv")
    z, core = mine // 2, lax.rem(mine, 2)
    partner = mine + 1 - 2 * core
    up = lax.rem(mine + 2, devices)
    down = lax.rem(mine + devices - 2, devices)
    q_cols, k_cols = wq.shape[1], wk.shape[1]
    ring = TpRing(tok, slots, send_t, recv_t, chunk_rows)
    mix_ring = TpRing(attended, mixing, send_m, recv_m, chunk_rows)

    loads = [
        pltpu.make_async_copy(wq, weights.at[:, pl.ds(0, q_cols)], local.at[0]),
        pltpu.make_async_copy(wk, weights.at[:, pl.ds(q_cols, k_cols)], local.at[1]),
        pltpu.make_async_copy(wv, weights.at[:, pl.ds(q_cols + k_cols, k_cols)], local.at[2]),
        pltpu.make_async_copy(tok, slots.at[ring.me], local.at[3]),
    ]
    for load in loads:
        load.start()

    barrier = pltpu.get_barrier_semaphore()
    end = chips - 1
    last = end * 2 + core

    def hail(**where):
        pl.semaphore_signal(barrier, inc=1, device_id=where, device_id_type=MESH)

    def let_go(chip):
        pl.semaphore_signal(go, inc=1, device_id={"kv": chip * 2 + core}, device_id_type=MESH)

    hail(tp=ring.right)
    hail(tp=ring.left)
    hail(kv=partner)

    @pl.when(z > 0)
    def _():
        hail(kv=mine - 2)

    @pl.when(z < end)
    def _():
        hail(kv=mine + 2)

    @pl.when(z < most_down)
    def _():
        hail(kv=last)

    @pl.when(z == 0)
    def _():
        pl.semaphore_wait(barrier, 4)

    @pl.when((z > 0) & (z < end))
    def _():
        pl.semaphore_wait(barrier, 5)

    @pl.when(z == end)
    def _():
        pl.semaphore_wait(barrier, 4 + most_down)
        let_go(0)

    own_blocks = rows // KB
    chunk_blocks = chunk_rows // KB

    def piece_rows(piece):
        return pl.ds(piece * chunk_rows, chunk_rows)

    def piece_blocks(holder, piece):
        return pl.ds(holder * own_blocks + piece * chunk_blocks, chunk_blocks)

    def goes_up(step):
        return (step <= most_up) & (z - step + 1 >= 0) & (z < end)

    def comes_up(step):
        return (step <= most_up) & (z - step >= 0)

    def comes_down(step):
        return (step <= most_down) & (z + step >= chips)

    def goes_down(step):
        return (step <= most_down) & (z + step > chips)

    def send_up(step, piece):
        block = need.at[piece_blocks(lax.rem(z - step + 1 + chips, chips) * 2 + core, piece)]
        return remote(block, block, send_z.at[0, step, piece], recv_z.at[0, step, piece], kv=up)

    def send_down(step, piece):
        block = need.at[piece_blocks(lax.rem(z + step - 1, chips) * 2 + core, piece)]
        return remote(block, block, send_z.at[1, step, piece], recv_z.at[1, step, piece], kv=down)

    def send_far(piece):
        block = need.at[piece_blocks(mine, piece)]
        step = jnp.minimum(z + 1, most_down)
        return remote(block, block, send_z.at[1, step, piece], recv_z.at[1, step, piece], kv=last)

    def across(direction, step, piece):
        chip = lax.rem(z - step + chips, chips) if direction == 0 else lax.rem(z + step, chips)
        block = need.at[piece_blocks(chip * 2 + core, piece)]
        return remote(
            block, block, send_c.at[direction, step], recv_c.at[direction, step], kv=partner
        )

    def across_whole(direction, step):
        block = need.at[pl.ds(mine * own_blocks, own_blocks)]
        return remote(
            block, block, send_c.at[direction, step], recv_c.at[direction, step], kv=partner
        )

    def project(chunk):
        at = piece_rows(chunk)
        total = jnp.zeros((chunk_rows, weights.shape[1]), jnp.float32)
        squares = jnp.zeros((chunk_rows, 1), jnp.float32)
        for t in range(tp):
            block = slots[t, at, :].astype(jnp.float32)
            squares += jnp.sum(block * block, axis=1, keepdims=True)
            scaled = (block * gain[:, t * width:(t + 1) * width].astype(jnp.float32)).astype(
                jnp.bfloat16
            )
            total += jnp.dot(
                scaled, weights[t * width:(t + 1) * width, :], preferred_element_type=jnp.float32
            )
        total *= lax.rsqrt(squares / (tp * width) + epsilon)
        cosine, sine = cos[at, :], sin[at, :]
        heads = []
        for h in range((q_cols + k_cols) // HD):
            head = total[:, h * HD:(h + 1) * HD]
            heads.append((head * cosine + pltpu.roll(head, HD // 2, 1) * sine).astype(jnp.bfloat16))
        for h in range(q_cols // HD):
            queries[at, h * HD:(h + 1) * HD] = heads[h]
        kept = piece_blocks(mine, chunk)
        values = total[:, q_cols + k_cols:].astype(jnp.bfloat16)
        need[kept, :, 0:k_cols] = heads[-1].reshape(chunk_blocks, KB, k_cols)
        need[kept, :, k_cols:2 * k_cols] = values.reshape(chunk_blocks, KB, k_cols)

        @pl.when(goes_up(1))
        def _():
            send_up(1, chunk).start()

    def hand_up(step, piece):
        @pl.when(comes_up(step))
        def _():
            send_up(step, piece).wait_recv()

            @pl.when(goes_up(step + 1))
            def _():
                send_up(step + 1, piece).start()

            across(0, step, piece).start()

    ring.begin(0)
    ring.begin(1)
    for load in loads:
        load.wait()
    for chunk in range(PIECES):
        if chunk == 0:
            ring.hand_on(0)
            ring.begin(2)
            ring.hand_on(1)
            ring.begin(3)
        elif chunk + 1 < PIECES:
            ring.hand_on(chunk + 1)
        ring.arrived(chunk)
        project(chunk)
        for step in range(1, chunk + 1):
            hand_up(step, chunk - step)
    give = across_whole(0, 0)
    give.start()

    blocks, listed_slots = sel.shape
    wide = listed_slots * KB
    heads_here = q_cols // HD

    def attend(b, key_pos):
        @pl.loop(0, listed_slots, unroll=4)
        def _(s):
            keys[pl.ds(pl.multiple_of(s * KB, KB), KB), :] = need[jnp.maximum(listed[b, s], 0)]

        q_pos = mine * rows + b * QB + lax.broadcasted_iota(jnp.int32, (QB, wide), 0)
        allowed = jnp.broadcast_to(key_pos[b:b + 1, :], (QB, wide)) <= q_pos
        for h in range(heads_here):
            score = lax.dot_general(
                queries[b * QB:(b + 1) * QB, h * HD:(h + 1) * HD], keys[:, 0:HD],
                (((1,), (1,)), ((), ())), preferred_element_type=jnp.float32,
            ) * HD ** (-0.5)
            score = jnp.where(allowed, score, -jnp.inf)
            raised = jnp.exp(score - jnp.max(score, axis=1, keepdims=True))
            parts = (raised / jnp.sum(raised, axis=1, keepdims=True)).astype(jnp.bfloat16)
            attended[b * QB:(b + 1) * QB, h * HD:(h + 1) * HD] = jnp.dot(
                parts, keys[:, HD:2 * HD], preferred_element_type=jnp.float32
            ).astype(jnp.bfloat16)
        mixing[mix_ring.me, b * QB:(b + 1) * QB, :] = attended[b * QB:(b + 1) * QB, :]

    def mix(chunk):
        at = piece_rows(chunk)
        total = jnp.zeros((chunk_rows, out.shape[1]), jnp.float32)
        for t in range(tp):
            total += jnp.dot(
                mixing[t, at, :], w_out[t * q_cols:(t + 1) * q_cols, :],
                preferred_element_type=jnp.float32,
            )
        out[at, :] = total.astype(jnp.bfloat16)

    def finish():
        give.wait()

        @pl.loop(1, jnp.minimum(z, most_up) + 1)
        def _(step):
            across_whole(0, step).wait()

        @pl.loop(jnp.maximum(chips - z, 1), most_down + 1)
        def _(step):
            across_whole(1, step).wait()

        spread = (
            lax.broadcasted_iota(jnp.int32, (listed_slots, wide), 1) // KB
            == lax.broadcasted_iota(jnp.int32, (listed_slots, wide), 0)
        ).astype(jnp.float32)
        ids = sel[...]
        safe = jnp.where(ids < 0, 1 << 20, ids)
        high = (safe // 64).astype(jnp.float32)
        low = lax.rem(safe, 64).astype(jnp.float32)
        found = jnp.dot(high, spread, preferred_element_type=jnp.float32) * 64.0 + jnp.dot(
            low, spread, preferred_element_type=jnp.float32
        )
        key_pos = found.astype(jnp.int32) * KB + lax.rem(
            lax.broadcasted_iota(jnp.int32, (blocks, wide), 1), KB
        )
        for b in range(PIECES):
            attend(b, key_pos)
            mix_ring.begin(b)
            if b:
                mix_ring.hand_on(b - 1)
        for b in range(PIECES):
            if b == 0:
                mix_ring.hand_on(PIECES - 1)
            mix_ring.arrived(b)
            mix(b)

    attend_at = jnp.minimum(z, most_up)

    def go_far():
        pl.semaphore_wait(go, 1)
        for piece in range(PIECES):
            send_far(piece).start()
        send_far(0).wait_send()

        @pl.when(z < most_down - 1)
        def _():
            let_go(z + 1)

    @pl.loop(0, most_up + 1)
    def _(step):
        for piece in range(PIECES):
            @pl.when((step > 0) & (step + piece >= PIECES))
            def _():
                hand_up(step, piece)

        down_step = step - DOWN_LAG

        for piece in range(PIECES):
            @pl.when((down_step > 0) & comes_down(down_step))
            def _():
                send_down(down_step, piece).wait_recv()

                @pl.when(goes_down(down_step + 1))
                def _():
                    send_down(down_step + 1, piece).start()

                across(1, down_step, piece).start()

        @pl.when((step == attend_at) & (z == 0))
        def _():
            go_far()

        @pl.when(step == attend_at)
        def _():
            finish()

        @pl.when((step == attend_at) & (z > 0) & (z < most_down))
        def _():
            go_far()

    for chunk in range(PIECES):
        ring.sent(chunk)
        mix_ring.sent(chunk)

    @pl.when(z < most_down)
    def _():
        for piece in range(1, PIECES):
            send_far(piece).wait_send()

    @pl.loop(1, most_up + 1)
    def _(step):
        for piece in range(PIECES):
            @pl.when(goes_up(step))
            def _():
                send_up(step, piece).wait_send()

            @pl.when(goes_down(step) & (step > 1))
            def _():
                send_down(step, piece).wait_send()


def reach(chips):
    most_up = chips // 2
    return most_up, chips - 1 - most_up


def layer(tokens, gain, w_query, w_key, w_value, w_out, cosine, sine, select):
    rows, width = tokens.shape
    devices = lax.axis_size("kv")
    tp = lax.axis_size("tp")
    q_cols, k_cols = w_query.shape[1], w_key.shape[1]
    most_up, most_down = reach(devices // 2)
    dma = pltpu.SemaphoreType.DMA
    bf16 = jnp.bfloat16
    vmem = pl.BlockSpec(memory_space=pltpu.VMEM)
    hbm = pl.BlockSpec(memory_space=pl.ANY)
    smem = pl.BlockSpec(memory_space=pltpu.SMEM)
    return pl.pallas_call(
        layer_kernel,
        out_shape=jax.ShapeDtypeStruct((rows, w_out.shape[1]), bf16),
        in_specs=[vmem, vmem, hbm, hbm, hbm, vmem, vmem, vmem, smem, vmem],
        out_specs=vmem,
        scratch_shapes=[
            pltpu.VMEM((tp, rows, width), bf16),
            pltpu.VMEM((tp * width, q_cols + 2 * k_cols), bf16),
            pltpu.VMEM((rows, q_cols), bf16),
            pltpu.VMEM((devices * rows // KB, KB, 2 * k_cols), bf16),
            pltpu.VMEM((select.shape[1] * KB, 2 * k_cols), bf16),
            pltpu.VMEM((rows, q_cols), bf16),
            pltpu.VMEM((tp, rows, q_cols), bf16),
            dma((PIECES, 4)),
            dma((PIECES, 4)),
            dma((2, most_up + 1, PIECES)),
            dma((2, most_up + 1, PIECES)),
            dma((2, most_up + 1)),
            dma((2, most_up + 1)),
            dma((PIECES, 4)),
            dma((PIECES, 4)),
            dma((4,)),
            pltpu.SemaphoreType.REGULAR,
        ],
        compiler_params=pltpu.CompilerParams(collective_id=0, has_side_effects=True),
        name="layer",
    )(tokens, gain, w_query, w_key, w_value, w_out, cosine, sine, select, select)


def per_device(tokens, gain, w_query, w_key, w_value, w_out, select):
    rows = tokens.shape[0]
    positions = lax.axis_index("kv") * rows + jnp.arange(rows, dtype=jnp.int32)
    cosine, sine = rotary_tables(positions)
    return layer(
        tokens, gain.reshape(1, -1), w_query, w_key, w_value, w_out, cosine, sine, select
    )


def solution(mesh):
    placed = (
        P(("grp", "kv"), "tp"),
        P(),
        P(None, "tp"),
        P(None, "tp"),
        P(None, "tp"),
        P(None, "tp"),
        P(("grp", "kv"), None),
    )
    return jax.shard_map(
        per_device, mesh=mesh, in_specs=placed, out_specs=P(("grp", "kv"), "tp"), check_vma=False
    )
```

```python
import functools

import jax
import jax.numpy as jnp
from jax import lax
from jax.experimental import pallas as pl
from jax.experimental.pallas import tpu as pltpu
from jax.sharding import PartitionSpec as P

HD = 128
QB = 128
KB = 32
PIECES = 4
MOST_LAG = 4

epsilon = 1e-06
theta = 10000.0
MESH = pl.DeviceIdType.MESH


def rotary_tables(positions):
    frequency = theta ** (-jnp.arange(0, HD, 2, dtype=jnp.float32) / HD)
    angles = positions.astype(jnp.float32)[:, None] * frequency[None, :]
    cosine, sine = jnp.cos(angles), jnp.sin(angles)
    return jnp.concatenate([cosine, cosine], 1), jnp.concatenate([-sine, sine], 1)


def remote(src, dst, send, recv, **where):
    return pltpu.make_async_remote_copy(
        src_ref=src, dst_ref=dst, send_sem=send, recv_sem=recv, device_id=where, device_id_type=MESH
    )


class TpRing:
    def __init__(self, own, slots, send, recv, rows):
        self.n = lax.axis_size("tp")
        self.me = lax.axis_index("tp")
        self.right = lax.rem(self.me + 1, self.n)
        self.left = lax.rem(self.me + self.n - 1, self.n)
        self.far = lax.rem(self.me + 2, self.n)
        self.own, self.slots, self.send, self.recv, self.rows = own, slots, send, recv, rows

    def copy(self, chunk, kind):
        half = self.rows // 2
        start, size, source, to = {
            0: (0, self.rows, None, self.right),
            1: (0, self.rows, None, self.left),
            2: (0, half, self.left, self.right),
            3: (half, half, self.right, self.left),
        }[kind]
        at = pl.ds(chunk * self.rows + start, size)
        src = self.own.at[at] if source is None else self.slots.at[source, at]
        dst = self.slots.at[self.me if source is None else source, at]
        return remote(src, dst, self.send.at[chunk, kind], self.recv.at[chunk, kind], tp=to)

    def begin(self, chunk):
        self.copy(chunk, 0).start()
        self.copy(chunk, 1).start()

    def hand_on(self, chunk):
        self.copy(chunk, 0).wait_recv()
        self.copy(chunk, 2).start()
        self.copy(chunk, 1).wait_recv()
        self.copy(chunk, 3).start()

    def arrived(self, chunk):
        self.copy(chunk, 2).wait_recv()
        self.copy(chunk, 3).wait_recv()

    def sent(self, chunk):
        for kind in range(4):
            self.copy(chunk, kind).wait_send()


def layer_kernel(
    tok, gain, wq, wk, wv, w_out, cos, sin, listed, sel, out,
    slots, weights, queries, need, keys, attended, mixing,
    send_t, recv_t, send_z, recv_z, send_c, recv_c, send_m, recv_m, local, go,
):
    rows, width = tok.shape
    tp = lax.axis_size("tp")
    chunk_rows = rows // PIECES
    devices = lax.axis_size("kv")
    chips = devices // 2
    most_up, most_down = reach(chips)
    mine = lax.axis_index("kv")
    z, core = mine // 2, lax.rem(mine, 2)
    partner = mine + 1 - 2 * core
    up = lax.rem(mine + 2, devices)
    down = lax.rem(mine + devices - 2, devices)
    q_cols, k_cols = wq.shape[1], wk.shape[1]
    ring = TpRing(tok, slots, send_t, recv_t, chunk_rows)
    mix_ring = TpRing(attended, mixing, send_m, recv_m, chunk_rows)

    loads = [
        pltpu.make_async_copy(wq, weights.at[:, pl.ds(0, q_cols)], local.at[0]),
        pltpu.make_async_copy(wk, weights.at[:, pl.ds(q_cols, k_cols)], local.at[1]),
        pltpu.make_async_copy(wv, weights.at[:, pl.ds(q_cols + k_cols, k_cols)], local.at[2]),
        pltpu.make_async_copy(tok, slots.at[ring.me], local.at[3]),
    ]
    for load in loads:
        load.start()

    barrier = pltpu.get_barrier_semaphore()
    end = chips - 1
    last = end * 2 + core

    def hail(**where):
        pl.semaphore_signal(barrier, inc=1, device_id=where, device_id_type=MESH)

    def let_go(chip):
        pl.semaphore_signal(go, inc=1, device_id={"kv": chip * 2 + core}, device_id_type=MESH)

    hail(tp=ring.right)
    hail(tp=ring.left)
    hail(kv=partner)

    @pl.when(z > 0)
    def _():
        hail(kv=mine - 2)

    @pl.when(z < end)
    def _():
        hail(kv=mine + 2)

    @pl.when(z < most_down)
    def _():
        hail(kv=last)

    @pl.when(z == 0)
    def _():
        pl.semaphore_wait(barrier, 4)

    @pl.when((z > 0) & (z < end))
    def _():
        pl.semaphore_wait(barrier, 5)

    @pl.when(z == end)
    def _():
        pl.semaphore_wait(barrier, 4 + most_down)
        for chip in range(most_down):
            let_go(chip)

    own_blocks = rows // KB
    chunk_blocks = chunk_rows // KB

    def piece_rows(piece):
        return pl.ds(piece * chunk_rows, chunk_rows)

    def piece_blocks(holder, piece):
        return pl.ds(holder * own_blocks + piece * chunk_blocks, chunk_blocks)

    def goes_up(step):
        return (step <= most_up) & (z - step + 1 >= 0) & (z < end)

    def comes_up(step):
        return (step <= most_up) & (z - step >= 0)

    def comes_down(step):
        return (step <= most_down) & (z + step >= chips)

    def goes_down(step):
        return (step <= most_down) & (z + step > chips)

    def send_up(step, piece):
        block = need.at[piece_blocks(lax.rem(z - step + 1 + chips, chips) * 2 + core, piece)]
        return remote(block, block, send_z.at[0, step, piece], recv_z.at[0, step, piece], kv=up)

    def send_down(step, piece):
        block = need.at[piece_blocks(lax.rem(z + step - 1, chips) * 2 + core, piece)]
        return remote(block, block, send_z.at[1, step, piece], recv_z.at[1, step, piece], kv=down)

    def send_far(piece):
        block = need.at[piece_blocks(mine, piece)]
        step = jnp.minimum(z + 1, most_down)
        return remote(block, block, send_z.at[1, step, piece], recv_z.at[1, step, piece], kv=last)

    def across(direction, step, piece):
        chip = lax.rem(z - step + chips, chips) if direction == 0 else lax.rem(z + step, chips)
        block = need.at[piece_blocks(chip * 2 + core, piece)]
        return remote(
            block, block, send_c.at[direction, step], recv_c.at[direction, step], kv=partner
        )

    def across_whole(direction, step):
        block = need.at[pl.ds(mine * own_blocks, own_blocks)]
        return remote(
            block, block, send_c.at[direction, step], recv_c.at[direction, step], kv=partner
        )

    def project(chunk):
        at = piece_rows(chunk)
        total = jnp.zeros((chunk_rows, weights.shape[1]), jnp.float32)
        squares = jnp.zeros((chunk_rows, 1), jnp.float32)
        for t in range(tp):
            block = slots[t, at, :].astype(jnp.float32)
            squares += jnp.sum(block * block, axis=1, keepdims=True)
            scaled = (block * gain[:, t * width:(t + 1) * width].astype(jnp.float32)).astype(
                jnp.bfloat16
            )
            total += jnp.dot(
                scaled, weights[t * width:(t + 1) * width, :], preferred_element_type=jnp.float32
            )
        total *= lax.rsqrt(squares / (tp * width) + epsilon)
        cosine, sine = cos[at, :], sin[at, :]
        heads = []
        for h in range((q_cols + k_cols) // HD):
            head = total[:, h * HD:(h + 1) * HD]
            heads.append((head * cosine + pltpu.roll(head, HD // 2, 1) * sine).astype(jnp.bfloat16))
        for h in range(q_cols // HD):
            queries[at, h * HD:(h + 1) * HD] = heads[h]
        kept = piece_blocks(mine, chunk)
        values = total[:, q_cols + k_cols:].astype(jnp.bfloat16)
        need[kept, :, 0:k_cols] = heads[-1].reshape(chunk_blocks, KB, k_cols)
        need[kept, :, k_cols:2 * k_cols] = values.reshape(chunk_blocks, KB, k_cols)

        @pl.when(goes_up(1))
        def _():
            send_up(1, chunk).start()

    def hand_up(step, piece):
        @pl.when(comes_up(step))
        def _():
            send_up(step, piece).wait_recv()

            @pl.when(goes_up(step + 1))
            def _():
                send_up(step + 1, piece).start()

            across(0, step, piece).start()

    ring.begin(0)
    ring.begin(1)
    for load in loads:
        load.wait()
    for chunk in range(PIECES):
        if chunk == 0:
            ring.hand_on(0)
            ring.begin(2)
            ring.hand_on(1)
            ring.begin(3)
        elif chunk + 1 < PIECES:
            ring.hand_on(chunk + 1)
        ring.arrived(chunk)
        project(chunk)
        for step in range(1, chunk + 1):
            hand_up(step, chunk - step)
    give = across_whole(0, 0)
    give.start()

    blocks, listed_slots = sel.shape
    wide = listed_slots * KB
    heads_here = q_cols // HD

    def attend(b, key_pos):
        @pl.loop(0, listed_slots, unroll=4)
        def _(s):
            keys[pl.ds(pl.multiple_of(s * KB, KB), KB), :] = need[jnp.maximum(listed[b, s], 0)]

        q_pos = mine * rows + b * QB + lax.broadcasted_iota(jnp.int32, (QB, wide), 0)
        allowed = jnp.broadcast_to(key_pos[b:b + 1, :], (QB, wide)) <= q_pos
        for h in range(heads_here):
            score = lax.dot_general(
                queries[b * QB:(b + 1) * QB, h * HD:(h + 1) * HD], keys[:, 0:HD],
                (((1,), (1,)), ((), ())), preferred_element_type=jnp.float32,
            ) * HD ** (-0.5)
            score = jnp.where(allowed, score, -jnp.inf)
            raised = jnp.exp(score - jnp.max(score, axis=1, keepdims=True))
            parts = (raised / jnp.sum(raised, axis=1, keepdims=True)).astype(jnp.bfloat16)
            attended[b * QB:(b + 1) * QB, h * HD:(h + 1) * HD] = jnp.dot(
                parts, keys[:, HD:2 * HD], preferred_element_type=jnp.float32
            ).astype(jnp.bfloat16)
        mixing[mix_ring.me, b * QB:(b + 1) * QB, :] = attended[b * QB:(b + 1) * QB, :]

    def mix(chunk):
        at = piece_rows(chunk)
        total = jnp.zeros((chunk_rows, out.shape[1]), jnp.float32)
        for t in range(tp):
            total += jnp.dot(
                mixing[t, at, :], w_out[t * q_cols:(t + 1) * q_cols, :],
                preferred_element_type=jnp.float32,
            )
        out[at, :] = total.astype(jnp.bfloat16)

    def finish():
        give.wait()

        @pl.loop(1, jnp.minimum(z, most_up) + 1)
        def _(step):
            across_whole(0, step).wait()

        @pl.loop(jnp.maximum(chips - z, 1), most_down + 1)
        def _(step):
            across_whole(1, step).wait()

        spread = (
            lax.broadcasted_iota(jnp.int32, (listed_slots, wide), 1) // KB
            == lax.broadcasted_iota(jnp.int32, (listed_slots, wide), 0)
        ).astype(jnp.float32)
        ids = sel[...]
        safe = jnp.where(ids < 0, 1 << 20, ids)
        high = (safe // 64).astype(jnp.float32)
        low = lax.rem(safe, 64).astype(jnp.float32)
        found = jnp.dot(high, spread, preferred_element_type=jnp.float32) * 64.0 + jnp.dot(
            low, spread, preferred_element_type=jnp.float32
        )
        key_pos = found.astype(jnp.int32) * KB + lax.rem(
            lax.broadcasted_iota(jnp.int32, (blocks, wide), 1), KB
        )
        for b in range(PIECES):
            attend(b, key_pos)
            mix_ring.begin(b)
            if b:
                mix_ring.hand_on(b - 1)
        for b in range(PIECES):
            if b == 0:
                mix_ring.hand_on(PIECES - 1)
            mix_ring.arrived(b)
            mix(b)

    first = most_up + 1
    lag = (jnp.maximum(z - first, 0) * MOST_LAG) // (end - first)
    attend_at = jnp.where(z < first, z, jnp.maximum(most_up, most_down + lag))

    def go_far():
        pl.semaphore_wait(go, 1)
        for piece in range(PIECES):
            send_far(piece).start()

    @pl.loop(0, most_down + MOST_LAG + 1)
    def _(step):
        for piece in range(PIECES):
            @pl.when((step > 0) & (step + piece >= PIECES))
            def _():
                hand_up(step, piece)

        down_step = step - lag

        for piece in range(PIECES):
            @pl.when((down_step > 0) & comes_down(down_step))
            def _():
                send_down(down_step, piece).wait_recv()

                @pl.when(goes_down(down_step + 1))
                def _():
                    send_down(down_step + 1, piece).start()

                across(1, down_step, piece).start()

        @pl.when((step == attend_at) & (z < most_down))
        def _():
            go_far()

        @pl.when(step == attend_at)
        def _():
            finish()

    for chunk in range(PIECES):
        ring.sent(chunk)
        mix_ring.sent(chunk)

    @pl.when(z < most_down)
    def _():
        for piece in range(PIECES):
            send_far(piece).wait_send()

    @pl.loop(1, most_up + 1)
    def _(step):
        for piece in range(PIECES):
            @pl.when(goes_up(step))
            def _():
                send_up(step, piece).wait_send()

            @pl.when(goes_down(step) & (step > 1))
            def _():
                send_down(step, piece).wait_send()


def reach(chips):
    most_up = chips // 2
    return most_up, chips - 1 - most_up


def layer(tokens, gain, w_query, w_key, w_value, w_out, cosine, sine, select):
    rows, width = tokens.shape
    devices = lax.axis_size("kv")
    tp = lax.axis_size("tp")
    q_cols, k_cols = w_query.shape[1], w_key.shape[1]
    most_up, most_down = reach(devices // 2)
    dma = pltpu.SemaphoreType.DMA
    bf16 = jnp.bfloat16
    vmem = pl.BlockSpec(memory_space=pltpu.VMEM)
    hbm = pl.BlockSpec(memory_space=pl.ANY)
    smem = pl.BlockSpec(memory_space=pltpu.SMEM)
    return pl.pallas_call(
        layer_kernel,
        out_shape=jax.ShapeDtypeStruct((rows, w_out.shape[1]), bf16),
        in_specs=[vmem, vmem, hbm, hbm, hbm, vmem, vmem, vmem, smem, vmem],
        out_specs=vmem,
        scratch_shapes=[
            pltpu.VMEM((tp, rows, width), bf16),
            pltpu.VMEM((tp * width, q_cols + 2 * k_cols), bf16),
            pltpu.VMEM((rows, q_cols), bf16),
            pltpu.VMEM((devices * rows // KB, KB, 2 * k_cols), bf16),
            pltpu.VMEM((select.shape[1] * KB, 2 * k_cols), bf16),
            pltpu.VMEM((rows, q_cols), bf16),
            pltpu.VMEM((tp, rows, q_cols), bf16),
            dma((PIECES, 4)),
            dma((PIECES, 4)),
            dma((2, most_up + 1, PIECES)),
            dma((2, most_up + 1, PIECES)),
            dma((2, most_up + 1)),
            dma((2, most_up + 1)),
            dma((PIECES, 4)),
            dma((PIECES, 4)),
            dma((4,)),
            pltpu.SemaphoreType.REGULAR,
        ],
        compiler_params=pltpu.CompilerParams(collective_id=0, has_side_effects=True),
        name="layer",
    )(tokens, gain, w_query, w_key, w_value, w_out, cosine, sine, select, select)


def per_device(tokens, gain, w_query, w_key, w_value, w_out, select):
    rows = tokens.shape[0]
    positions = lax.axis_index("kv") * rows + jnp.arange(rows, dtype=jnp.int32)
    cosine, sine = rotary_tables(positions)
    return layer(
        tokens, gain.reshape(1, -1), w_query, w_key, w_value, w_out, cosine, sine, select
    )


def solution(mesh):
    placed = (
        P(("grp", "kv"), "tp"),
        P(),
        P(None, "tp"),
        P(None, "tp"),
        P(None, "tp"),
        P(None, "tp"),
        P(("grp", "kv"), None),
    )
    return jax.shard_map(
        per_device, mesh=mesh, in_specs=placed, out_specs=P(("grp", "kv"), "tp"), check_vma=False
    )
```

```python
import functools

import jax
import jax.numpy as jnp
from jax import lax
from jax.experimental import pallas as pl
from jax.experimental.pallas import tpu as pltpu
from jax.sharding import PartitionSpec as P

HD = 128
QB = 128
KB = 32
PIECES = 4
FAR_FIRST = 9

epsilon = 1e-06
theta = 10000.0
MESH = pl.DeviceIdType.MESH


def rotary_tables(positions):
    frequency = theta ** (-jnp.arange(0, HD, 2, dtype=jnp.float32) / HD)
    angles = positions.astype(jnp.float32)[:, None] * frequency[None, :]
    cosine, sine = jnp.cos(angles), jnp.sin(angles)
    return jnp.concatenate([cosine, cosine], 1), jnp.concatenate([-sine, sine], 1)


def remote(src, dst, send, recv, **where):
    return pltpu.make_async_remote_copy(
        src_ref=src, dst_ref=dst, send_sem=send, recv_sem=recv, device_id=where, device_id_type=MESH
    )


class TpRing:
    def __init__(self, own, slots, send, recv, rows):
        self.n = lax.axis_size("tp")
        self.me = lax.axis_index("tp")
        self.right = lax.rem(self.me + 1, self.n)
        self.left = lax.rem(self.me + self.n - 1, self.n)
        self.far = lax.rem(self.me + 2, self.n)
        self.own, self.slots, self.send, self.recv, self.rows = own, slots, send, recv, rows

    def copy(self, chunk, kind):
        half = self.rows // 2
        start, size, source, to = {
            0: (0, self.rows, None, self.right),
            1: (0, self.rows, None, self.left),
            2: (0, half, self.left, self.right),
            3: (half, half, self.right, self.left),
        }[kind]
        at = pl.ds(chunk * self.rows + start, size)
        src = self.own.at[at] if source is None else self.slots.at[source, at]
        dst = self.slots.at[self.me if source is None else source, at]
        return remote(src, dst, self.send.at[chunk, kind], self.recv.at[chunk, kind], tp=to)

    def begin(self, chunk):
        self.copy(chunk, 0).start()
        self.copy(chunk, 1).start()

    def hand_on(self, chunk):
        self.copy(chunk, 0).wait_recv()
        self.copy(chunk, 2).start()
        self.copy(chunk, 1).wait_recv()
        self.copy(chunk, 3).start()

    def arrived(self, chunk):
        self.copy(chunk, 2).wait_recv()
        self.copy(chunk, 3).wait_recv()

    def sent(self, chunk):
        for kind in range(4):
            self.copy(chunk, kind).wait_send()


def layer_kernel(
    tok, gain, wq, wk, wv, w_out, cos, sin, listed, sel, out,
    slots, weights, queries, need, keys, attended, mixing,
    send_t, recv_t, send_z, recv_z, send_c, recv_c, send_m, recv_m, local, go,
):
    rows, width = tok.shape
    tp = lax.axis_size("tp")
    chunk_rows = rows // PIECES
    devices = lax.axis_size("kv")
    chips = devices // 2
    most_up, most_down = reach(chips)
    mine = lax.axis_index("kv")
    z, core = mine // 2, lax.rem(mine, 2)
    partner = mine + 1 - 2 * core
    up = lax.rem(mine + 2, devices)
    down = lax.rem(mine + devices - 2, devices)
    q_cols, k_cols = wq.shape[1], wk.shape[1]
    ring = TpRing(tok, slots, send_t, recv_t, chunk_rows)
    mix_ring = TpRing(attended, mixing, send_m, recv_m, chunk_rows)

    loads = [
        pltpu.make_async_copy(wq, weights.at[:, pl.ds(0, q_cols)], local.at[0]),
        pltpu.make_async_copy(wk, weights.at[:, pl.ds(q_cols, k_cols)], local.at[1]),
        pltpu.make_async_copy(wv, weights.at[:, pl.ds(q_cols + k_cols, k_cols)], local.at[2]),
        pltpu.make_async_copy(tok, slots.at[ring.me], local.at[3]),
    ]
    for load in loads:
        load.start()

    barrier = pltpu.get_barrier_semaphore()
    end = chips - 1
    last = end * 2 + core

    def hail(**where):
        pl.semaphore_signal(barrier, inc=1, device_id=where, device_id_type=MESH)

    def let_go(chip):
        pl.semaphore_signal(go, inc=1, device_id={"kv": chip * 2 + core}, device_id_type=MESH)

    hail(tp=ring.right)
    hail(tp=ring.left)
    hail(kv=partner)

    @pl.when(z > 0)
    def _():
        hail(kv=mine - 2)

    @pl.when(z < end)
    def _():
        hail(kv=mine + 2)

    @pl.when(z < most_down)
    def _():
        hail(kv=last)

    @pl.when(z == 0)
    def _():
        pl.semaphore_wait(barrier, 4)

    @pl.when((z > 0) & (z < end))
    def _():
        pl.semaphore_wait(barrier, 5)

    @pl.when(z == end)
    def _():
        pl.semaphore_wait(barrier, 4 + most_down)
        let_go(0)

    own_blocks = rows // KB
    chunk_blocks = chunk_rows // KB

    def piece_rows(piece):
        return pl.ds(piece * chunk_rows, chunk_rows)

    def piece_blocks(holder, piece):
        return pl.ds(holder * own_blocks + piece * chunk_blocks, chunk_blocks)

    def goes_up(step):
        return (step <= most_up) & (z - step + 1 >= 0) & (z < end)

    def comes_up(step):
        return (step <= most_up) & (z - step >= 0)

    def comes_down(step):
        return (step <= most_down) & (z + step >= chips)

    def goes_down(step):
        return (step <= most_down) & (z + step > chips)

    def send_up(step, piece):
        block = need.at[piece_blocks(lax.rem(z - step + 1 + chips, chips) * 2 + core, piece)]
        return remote(block, block, send_z.at[0, step, piece], recv_z.at[0, step, piece], kv=up)

    def send_down(step, piece):
        block = need.at[piece_blocks(lax.rem(z + step - 1, chips) * 2 + core, piece)]
        return remote(block, block, send_z.at[1, step, piece], recv_z.at[1, step, piece], kv=down)

    def send_far(piece):
        block = need.at[piece_blocks(mine, piece)]
        step = jnp.minimum(z + 1, most_down)
        return remote(block, block, send_z.at[1, step, piece], recv_z.at[1, step, piece], kv=last)

    def across(direction, step, piece):
        chip = lax.rem(z - step + chips, chips) if direction == 0 else lax.rem(z + step, chips)
        block = need.at[piece_blocks(chip * 2 + core, piece)]
        return remote(
            block, block, send_c.at[direction, step], recv_c.at[direction, step], kv=partner
        )

    def across_whole(direction, step):
        block = need.at[pl.ds(mine * own_blocks, own_blocks)]
        return remote(
            block, block, send_c.at[direction, step], recv_c.at[direction, step], kv=partner
        )

    def project(chunk):
        at = piece_rows(chunk)
        total = jnp.zeros((chunk_rows, weights.shape[1]), jnp.float32)
        squares = jnp.zeros((chunk_rows, 1), jnp.float32)
        for t in range(tp):
            block = slots[t, at, :].astype(jnp.float32)
            squares += jnp.sum(block * block, axis=1, keepdims=True)
            scaled = (block * gain[:, t * width:(t + 1) * width].astype(jnp.float32)).astype(
                jnp.bfloat16
            )
            total += jnp.dot(
                scaled, weights[t * width:(t + 1) * width, :], preferred_element_type=jnp.float32
            )
        total *= lax.rsqrt(squares / (tp * width) + epsilon)
        cosine, sine = cos[at, :], sin[at, :]
        heads = []
        for h in range((q_cols + k_cols) // HD):
            head = total[:, h * HD:(h + 1) * HD]
            heads.append((head * cosine + pltpu.roll(head, HD // 2, 1) * sine).astype(jnp.bfloat16))
        for h in range(q_cols // HD):
            queries[at, h * HD:(h + 1) * HD] = heads[h]
        kept = piece_blocks(mine, chunk)
        values = total[:, q_cols + k_cols:].astype(jnp.bfloat16)
        need[kept, :, 0:k_cols] = heads[-1].reshape(chunk_blocks, KB, k_cols)
        need[kept, :, k_cols:2 * k_cols] = values.reshape(chunk_blocks, KB, k_cols)

        @pl.when(goes_up(1))
        def _():
            send_up(1, chunk).start()

    def hand_up(step, piece):
        @pl.when(comes_up(step))
        def _():
            send_up(step, piece).wait_recv()

            @pl.when(goes_up(step + 1))
            def _():
                send_up(step + 1, piece).start()

            across(0, step, piece).start()

    ring.begin(0)
    ring.begin(1)
    for load in loads:
        load.wait()
    for chunk in range(PIECES):
        if chunk == 0:
            ring.hand_on(0)
            ring.begin(2)
            ring.hand_on(1)
            ring.begin(3)
        elif chunk + 1 < PIECES:
            ring.hand_on(chunk + 1)
        ring.arrived(chunk)
        project(chunk)
        for step in range(1, chunk + 1):
            hand_up(step, chunk - step)
    give = across_whole(0, 0)
    give.start()

    blocks, listed_slots = sel.shape
    wide = listed_slots * KB
    heads_here = q_cols // HD

    def attend(b, key_pos):
        @pl.loop(0, listed_slots, unroll=4)
        def _(s):
            keys[pl.ds(pl.multiple_of(s * KB, KB), KB), :] = need[jnp.maximum(listed[b, s], 0)]

        q_pos = mine * rows + b * QB + lax.broadcasted_iota(jnp.int32, (QB, wide), 0)
        allowed = jnp.broadcast_to(key_pos[b:b + 1, :], (QB, wide)) <= q_pos
        for h in range(heads_here):
            score = lax.dot_general(
                queries[b * QB:(b + 1) * QB, h * HD:(h + 1) * HD], keys[:, 0:HD],
                (((1,), (1,)), ((), ())), preferred_element_type=jnp.float32,
            ) * HD ** (-0.5)
            score = jnp.where(allowed, score, -jnp.inf)
            raised = jnp.exp(score - jnp.max(score, axis=1, keepdims=True))
            parts = (raised / jnp.sum(raised, axis=1, keepdims=True)).astype(jnp.bfloat16)
            attended[b * QB:(b + 1) * QB, h * HD:(h + 1) * HD] = jnp.dot(
                parts, keys[:, HD:2 * HD], preferred_element_type=jnp.float32
            ).astype(jnp.bfloat16)
        mixing[mix_ring.me, b * QB:(b + 1) * QB, :] = attended[b * QB:(b + 1) * QB, :]

    def mix(chunk):
        at = piece_rows(chunk)
        total = jnp.zeros((chunk_rows, out.shape[1]), jnp.float32)
        for t in range(tp):
            total += jnp.dot(
                mixing[t, at, :], w_out[t * q_cols:(t + 1) * q_cols, :],
                preferred_element_type=jnp.float32,
            )
        out[at, :] = total.astype(jnp.bfloat16)

    def finish():
        give.wait()

        @pl.loop(1, jnp.minimum(z, most_up) + 1)
        def _(step):
            across_whole(0, step).wait()

        @pl.loop(jnp.maximum(chips - z, 1), most_down + 1)
        def _(step):
            across_whole(1, step).wait()

        spread = (
            lax.broadcasted_iota(jnp.int32, (listed_slots, wide), 1) // KB
            == lax.broadcasted_iota(jnp.int32, (listed_slots, wide), 0)
        ).astype(jnp.float32)
        ids = sel[...]
        safe = jnp.where(ids < 0, 1 << 20, ids)
        high = (safe // 64).astype(jnp.float32)
        low = lax.rem(safe, 64).astype(jnp.float32)
        found = jnp.dot(high, spread, preferred_element_type=jnp.float32) * 64.0 + jnp.dot(
            low, spread, preferred_element_type=jnp.float32
        )
        key_pos = found.astype(jnp.int32) * KB + lax.rem(
            lax.broadcasted_iota(jnp.int32, (blocks, wide), 1), KB
        )
        for b in range(PIECES):
            attend(b, key_pos)
            mix_ring.begin(b)
            if b:
                mix_ring.hand_on(b - 1)
        for b in range(PIECES):
            if b == 0:
                mix_ring.hand_on(PIECES - 1)
            mix_ring.arrived(b)
            mix(b)

    first = most_up + 1
    lag = 1 + (jnp.maximum(z - first, 0) * 2) // (end - first)
    attend_at = jnp.where(z < first, z, jnp.maximum(most_up, most_down + lag))

    def go_far():
        pl.semaphore_wait(go, 1)
        for piece in range(PIECES):
            send_far(piece).start()
        send_far(0).wait_send()

        @pl.when(z < most_down - 1)
        def _():
            let_go(z + 1)

    @pl.loop(0, most_down + 4)
    def _(step):
        for piece in range(PIECES):
            @pl.when((step > 0) & (step + piece >= PIECES))
            def _():
                hand_up(step, piece)

        down_step = step - lag

        for piece in range(PIECES):
            @pl.when((down_step > 0) & comes_down(down_step))
            def _():
                send_down(down_step, piece).wait_recv()

                @pl.when(goes_down(down_step + 1))
                def _():
                    send_down(down_step + 1, piece).start()

                across(1, down_step, piece).start()

        @pl.when((step == attend_at) & (z < FAR_FIRST))
        def _():
            go_far()

        @pl.when(step == attend_at)
        def _():
            finish()

        @pl.when((step == attend_at) & (z >= FAR_FIRST) & (z < most_down))
        def _():
            go_far()

    for chunk in range(PIECES):
        ring.sent(chunk)
        mix_ring.sent(chunk)

    @pl.when(z < most_down)
    def _():
        for piece in range(1, PIECES):
            send_far(piece).wait_send()

    @pl.loop(1, most_up + 1)
    def _(step):
        for piece in range(PIECES):
            @pl.when(goes_up(step))
            def _():
                send_up(step, piece).wait_send()

            @pl.when(goes_down(step) & (step > 1))
            def _():
                send_down(step, piece).wait_send()


def reach(chips):
    most_up = chips // 2
    return most_up, chips - 1 - most_up


def layer(tokens, gain, w_query, w_key, w_value, w_out, cosine, sine, select):
    rows, width = tokens.shape
    devices = lax.axis_size("kv")
    tp = lax.axis_size("tp")
    q_cols, k_cols = w_query.shape[1], w_key.shape[1]
    most_up, most_down = reach(devices // 2)
    dma = pltpu.SemaphoreType.DMA
    bf16 = jnp.bfloat16
    vmem = pl.BlockSpec(memory_space=pltpu.VMEM)
    hbm = pl.BlockSpec(memory_space=pl.ANY)
    smem = pl.BlockSpec(memory_space=pltpu.SMEM)
    return pl.pallas_call(
        layer_kernel,
        out_shape=jax.ShapeDtypeStruct((rows, w_out.shape[1]), bf16),
        in_specs=[vmem, vmem, hbm, hbm, hbm, vmem, vmem, vmem, smem, vmem],
        out_specs=vmem,
        scratch_shapes=[
            pltpu.VMEM((tp, rows, width), bf16),
            pltpu.VMEM((tp * width, q_cols + 2 * k_cols), bf16),
            pltpu.VMEM((rows, q_cols), bf16),
            pltpu.VMEM((devices * rows // KB, KB, 2 * k_cols), bf16),
            pltpu.VMEM((select.shape[1] * KB, 2 * k_cols), bf16),
            pltpu.VMEM((rows, q_cols), bf16),
            pltpu.VMEM((tp, rows, q_cols), bf16),
            dma((PIECES, 4)),
            dma((PIECES, 4)),
            dma((2, most_up + 1, PIECES)),
            dma((2, most_up + 1, PIECES)),
            dma((2, most_up + 1)),
            dma((2, most_up + 1)),
            dma((PIECES, 4)),
            dma((PIECES, 4)),
            dma((4,)),
            pltpu.SemaphoreType.REGULAR,
        ],
        compiler_params=pltpu.CompilerParams(collective_id=0, has_side_effects=True),
        name="layer",
    )(tokens, gain, w_query, w_key, w_value, w_out, cosine, sine, select, select)


def per_device(tokens, gain, w_query, w_key, w_value, w_out, select):
    rows = tokens.shape[0]
    positions = lax.axis_index("kv") * rows + jnp.arange(rows, dtype=jnp.int32)
    cosine, sine = rotary_tables(positions)
    return layer(
        tokens, gain.reshape(1, -1), w_query, w_key, w_value, w_out, cosine, sine, select
    )


def solution(mesh):
    placed = (
        P(("grp", "kv"), "tp"),
        P(),
        P(None, "tp"),
        P(None, "tp"),
        P(None, "tp"),
        P(None, "tp"),
        P(("grp", "kv"), None),
    )
    return jax.shard_map(
        per_device, mesh=mesh, in_specs=placed, out_specs=P(("grp", "kv"), "tp"), check_vma=False
    )
```

```python
import functools

import jax
import jax.numpy as jnp
from jax import lax
from jax.experimental import pallas as pl
from jax.experimental.pallas import tpu as pltpu
from jax.sharding import PartitionSpec as P

HD = 128
QB = 128
KB = 32
PIECES = 4

epsilon = 1e-06
theta = 10000.0
MESH = pl.DeviceIdType.MESH


def rotary_tables(positions):
    frequency = theta ** (-jnp.arange(0, HD, 2, dtype=jnp.float32) / HD)
    angles = positions.astype(jnp.float32)[:, None] * frequency[None, :]
    cosine, sine = jnp.cos(angles), jnp.sin(angles)
    return jnp.concatenate([cosine, cosine], 1), jnp.concatenate([-sine, sine], 1)


def remote(src, dst, send, recv, **where):
    return pltpu.make_async_remote_copy(
        src_ref=src, dst_ref=dst, send_sem=send, recv_sem=recv, device_id=where, device_id_type=MESH
    )


class TpRing:
    def __init__(self, own, slots, send, recv, rows):
        self.n = lax.axis_size("tp")
        self.me = lax.axis_index("tp")
        self.right = lax.rem(self.me + 1, self.n)
        self.left = lax.rem(self.me + self.n - 1, self.n)
        self.far = lax.rem(self.me + 2, self.n)
        self.own, self.slots, self.send, self.recv, self.rows = own, slots, send, recv, rows

    def copy(self, chunk, kind):
        half = self.rows // 2
        start, size, source, to = {
            0: (0, self.rows, None, self.right),
            1: (0, self.rows, None, self.left),
            2: (0, half, self.left, self.right),
            3: (half, half, self.right, self.left),
        }[kind]
        at = pl.ds(chunk * self.rows + start, size)
        src = self.own.at[at] if source is None else self.slots.at[source, at]
        dst = self.slots.at[self.me if source is None else source, at]
        return remote(src, dst, self.send.at[chunk, kind], self.recv.at[chunk, kind], tp=to)

    def begin(self, chunk):
        self.copy(chunk, 0).start()
        self.copy(chunk, 1).start()

    def hand_on(self, chunk):
        self.copy(chunk, 0).wait_recv()
        self.copy(chunk, 2).start()
        self.copy(chunk, 1).wait_recv()
        self.copy(chunk, 3).start()

    def arrived(self, chunk):
        self.copy(chunk, 2).wait_recv()
        self.copy(chunk, 3).wait_recv()

    def sent(self, chunk):
        for kind in range(4):
            self.copy(chunk, kind).wait_send()


def layer_kernel(
    tok, gain, wq, wk, wv, w_out, cos, sin, listed, sel, out,
    slots, weights, queries, need, transit, keys, attended, mixing,
    send_t, recv_t, send_z, recv_z, send_c, recv_c, send_m, recv_m, local, go,
):
    rows, width = tok.shape
    tp = lax.axis_size("tp")
    chunk_rows = rows // PIECES
    devices = lax.axis_size("kv")
    chips = devices // 2
    most_up, most_down = reach(chips)
    mine = lax.axis_index("kv")
    z, core = mine // 2, lax.rem(mine, 2)
    partner = mine + 1 - 2 * core
    up = lax.rem(mine + 2, devices)
    down = lax.rem(mine + devices - 2, devices)
    q_cols, k_cols = wq.shape[1], wk.shape[1]
    ring = TpRing(tok, slots, send_t, recv_t, chunk_rows)
    mix_ring = TpRing(attended, mixing, send_m, recv_m, chunk_rows)

    loads = [
        pltpu.make_async_copy(wq, weights.at[:, pl.ds(0, q_cols)], local.at[0]),
        pltpu.make_async_copy(wk, weights.at[:, pl.ds(q_cols, k_cols)], local.at[1]),
        pltpu.make_async_copy(wv, weights.at[:, pl.ds(q_cols + k_cols, k_cols)], local.at[2]),
        pltpu.make_async_copy(tok, slots.at[ring.me], local.at[3]),
    ]
    for load in loads:
        load.start()

    barrier = pltpu.get_barrier_semaphore()

    def hail(**where):
        pl.semaphore_signal(barrier, inc=1, device_id=where, device_id_type=MESH)

    hail(tp=ring.right)
    hail(tp=ring.left)
    hail(kv=partner)
    hail(kv=down)

    @pl.when(z < chips - 1)
    def _():
        hail(kv=up)

    @pl.when(z == 0)
    def _():
        pl.semaphore_wait(barrier, 4)

    @pl.when(z > 0)
    def _():
        pl.semaphore_wait(barrier, 5)

    @pl.when(z == chips - 1)
    def _():
        pl.semaphore_signal(go, inc=1, device_id={"kv": up}, device_id_type=MESH)

    own_blocks = rows // KB
    chunk_blocks = chunk_rows // KB

    def piece_rows(piece):
        return pl.ds(piece * chunk_rows, chunk_rows)

    def piece_blocks(holder, piece):
        return pl.ds(holder * own_blocks + piece * chunk_blocks, chunk_blocks)

    def goes_up(step):
        return (step <= most_up) & (z - step + 1 >= 0) & (z < chips - 1)

    def comes_up(step):
        return (step <= most_up) & (z - step >= 0)

    def goes_down(step):
        return (step <= most_down) & (lax.rem(z + step - 1, chips) < most_down)

    def comes_down(step):
        return (step <= most_down) & (lax.rem(z + step, chips) < most_down)

    def send_up(step, piece):
        block = need.at[piece_blocks(lax.rem(z - step + 1 + chips, chips) * 2 + core, piece)]
        return remote(block, block, send_z.at[0, step, piece], recv_z.at[0, step, piece], kv=up)

    def send_down(step, piece, from_transit, to_transit):
        chip = lax.rem(z + step - 1, chips)
        kept = need.at[piece_blocks(chip * 2 + core, piece)]
        passing = transit.at[piece_blocks(lax.rem(chip, most_down), piece)]
        return remote(
            passing if from_transit else kept, passing if to_transit else kept,
            send_z.at[1, step, piece], recv_z.at[1, step, piece], kv=down,
        )

    def across(direction, step, piece):
        chip = lax.rem(z - step + chips, chips) if direction == 0 else lax.rem(z + step, chips)
        block = need.at[piece_blocks(chip * 2 + core, piece)]
        return remote(
            block, block, send_c.at[direction, step], recv_c.at[direction, step], kv=partner
        )

    def across_whole(direction, step):
        block = need.at[pl.ds(mine * own_blocks, own_blocks)]
        return remote(
            block, block, send_c.at[direction, step], recv_c.at[direction, step], kv=partner
        )

    def project(chunk):
        at = piece_rows(chunk)
        total = jnp.zeros((chunk_rows, weights.shape[1]), jnp.float32)
        squares = jnp.zeros((chunk_rows, 1), jnp.float32)
        for t in range(tp):
            block = slots[t, at, :].astype(jnp.float32)
            squares += jnp.sum(block * block, axis=1, keepdims=True)
            scaled = (block * gain[:, t * width:(t + 1) * width].astype(jnp.float32)).astype(
                jnp.bfloat16
            )
            total += jnp.dot(
                scaled, weights[t * width:(t + 1) * width, :], preferred_element_type=jnp.float32
            )
        total *= lax.rsqrt(squares / (tp * width) + epsilon)
        cosine, sine = cos[at, :], sin[at, :]
        heads = []
        for h in range((q_cols + k_cols) // HD):
            head = total[:, h * HD:(h + 1) * HD]
            heads.append((head * cosine + pltpu.roll(head, HD // 2, 1) * sine).astype(jnp.bfloat16))
        for h in range(q_cols // HD):
            queries[at, h * HD:(h + 1) * HD] = heads[h]
        kept = piece_blocks(mine, chunk)
        values = total[:, q_cols + k_cols:].astype(jnp.bfloat16)
        need[kept, :, 0:k_cols] = heads[-1].reshape(chunk_blocks, KB, k_cols)
        need[kept, :, k_cols:2 * k_cols] = values.reshape(chunk_blocks, KB, k_cols)

        @pl.when(goes_up(1))
        def _():
            send_up(1, chunk).start()

        @pl.when(goes_down(1) & (z > 0))
        def _():
            send_down(1, chunk, False, True).start()

    def hand_up(step, piece):
        @pl.when(comes_up(step))
        def _():
            send_up(step, piece).wait_recv()

            @pl.when(goes_up(step + 1))
            def _():
                send_up(step + 1, piece).start()

            across(0, step, piece).start()

    ring.begin(0)
    ring.begin(1)
    for load in loads:
        load.wait()
    for chunk in range(PIECES):
        if chunk == 0:
            ring.hand_on(0)
            ring.begin(2)
            ring.hand_on(1)
            ring.begin(3)
        elif chunk + 1 < PIECES:
            ring.hand_on(chunk + 1)
        ring.arrived(chunk)
        project(chunk)
        for step in range(1, chunk + 1):
            hand_up(step, chunk - step)
    give = across_whole(0, 0)
    give.start()

    blocks, listed_slots = sel.shape
    wide = listed_slots * KB
    heads_here = q_cols // HD

    def attend(b, key_pos):
        @pl.loop(0, listed_slots, unroll=4)
        def _(s):
            keys[pl.ds(pl.multiple_of(s * KB, KB), KB), :] = need[jnp.maximum(listed[b, s], 0)]

        q_pos = mine * rows + b * QB + lax.broadcasted_iota(jnp.int32, (QB, wide), 0)
        allowed = jnp.broadcast_to(key_pos[b:b + 1, :], (QB, wide)) <= q_pos
        for h in range(heads_here):
            score = lax.dot_general(
                queries[b * QB:(b + 1) * QB, h * HD:(h + 1) * HD], keys[:, 0:HD],
                (((1,), (1,)), ((), ())), preferred_element_type=jnp.float32,
            ) * HD ** (-0.5)
            score = jnp.where(allowed, score, -jnp.inf)
            raised = jnp.exp(score - jnp.max(score, axis=1, keepdims=True))
            parts = (raised / jnp.sum(raised, axis=1, keepdims=True)).astype(jnp.bfloat16)
            attended[b * QB:(b + 1) * QB, h * HD:(h + 1) * HD] = jnp.dot(
                parts, keys[:, HD:2 * HD], preferred_element_type=jnp.float32
            ).astype(jnp.bfloat16)
        mixing[mix_ring.me, b * QB:(b + 1) * QB, :] = attended[b * QB:(b + 1) * QB, :]

    def mix(chunk):
        at = piece_rows(chunk)
        total = jnp.zeros((chunk_rows, out.shape[1]), jnp.float32)
        for t in range(tp):
            total += jnp.dot(
                mixing[t, at, :], w_out[t * q_cols:(t + 1) * q_cols, :],
                preferred_element_type=jnp.float32,
            )
        out[at, :] = total.astype(jnp.bfloat16)

    def all_here():
        give.wait()

        @pl.loop(1, jnp.minimum(z, most_up) + 1)
        def _(step):
            across_whole(0, step).wait()

        @pl.loop(jnp.maximum(chips - z, 1), most_down + 1)
        def _(step):
            across_whole(1, step).wait()

    def key_positions():
        spread = (
            lax.broadcasted_iota(jnp.int32, (listed_slots, wide), 1) // KB
            == lax.broadcasted_iota(jnp.int32, (listed_slots, wide), 0)
        ).astype(jnp.float32)
        ids = sel[...]
        safe = jnp.where(ids < 0, 1 << 20, ids)
        high = (safe // 64).astype(jnp.float32)
        low = lax.rem(safe, 64).astype(jnp.float32)
        found = jnp.dot(high, spread, preferred_element_type=jnp.float32) * 64.0 + jnp.dot(
            low, spread, preferred_element_type=jnp.float32
        )
        key_pos = found.astype(jnp.int32) * KB + lax.rem(
            lax.broadcasted_iota(jnp.int32, (blocks, wide), 1), KB
        )
        return key_pos

    def stage(which):
        if which == 0:
            all_here()
        if which < PIECES:
            attend(which, key_positions())
            mix_ring.begin(which)
            if which:
                mix_ring.hand_on(which - 1)
        else:
            if which == PIECES:
                mix_ring.hand_on(PIECES - 1)
            mix_ring.arrived(which - PIECES)
            mix(which - PIECES)

    attend_at = jnp.minimum(z, most_up)

    @pl.loop(0, most_up + 2 * PIECES)
    def _(step):
        for piece in range(PIECES):
            @pl.when((step > 0) & (step + piece >= PIECES))
            def _():
                hand_up(step, piece)

            @pl.when((step > 0) & comes_down(step))
            def _():
                send_down(step, piece, False, False).wait_recv()
                wrapped = z + step >= chips
                onward = step < most_down

                @pl.when(onward & wrapped)
                def _():
                    send_down(step + 1, piece, False, False).start()

                @pl.when(onward & jnp.logical_not(wrapped) & (z > 0))
                def _():
                    send_down(step + 1, piece, True, True).start()

                @pl.when(onward & (z == 0))
                def _():
                    send_down(step + 1, piece, True, False).start()

                @pl.when(wrapped)
                def _():
                    across(1, step, piece).start()

        @pl.when((step == 0) & (z == 0))
        def _():
            pl.semaphore_wait(go, 1)
            for piece in range(PIECES):
                send_down(1, piece, False, False).start()

        for which in range(2 * PIECES):
            @pl.when(step == attend_at + which)
            def _():
                stage(which)

    for chunk in range(PIECES):
        ring.sent(chunk)
        mix_ring.sent(chunk)

    @pl.loop(1, most_up + 1)
    def _(step):
        for piece in range(PIECES):
            @pl.when(goes_up(step))
            def _():
                send_up(step, piece).wait_send()

            @pl.when(goes_down(step))
            def _():
                send_down(step, piece, False, False).wait_send()


def reach(chips):
    most_up = chips // 2 + 1
    return most_up, chips - 1 - most_up


def layer(tokens, gain, w_query, w_key, w_value, w_out, cosine, sine, select):
    rows, width = tokens.shape
    devices = lax.axis_size("kv")
    tp = lax.axis_size("tp")
    q_cols, k_cols = w_query.shape[1], w_key.shape[1]
    most_up, most_down = reach(devices // 2)
    dma = pltpu.SemaphoreType.DMA
    bf16 = jnp.bfloat16
    vmem = pl.BlockSpec(memory_space=pltpu.VMEM)
    hbm = pl.BlockSpec(memory_space=pl.ANY)
    smem = pl.BlockSpec(memory_space=pltpu.SMEM)
    return pl.pallas_call(
        layer_kernel,
        out_shape=jax.ShapeDtypeStruct((rows, w_out.shape[1]), bf16),
        in_specs=[vmem, vmem, hbm, hbm, hbm, vmem, vmem, vmem, smem, vmem],
        out_specs=vmem,
        scratch_shapes=[
            pltpu.VMEM((tp, rows, width), bf16),
            pltpu.VMEM((tp * width, q_cols + 2 * k_cols), bf16),
            pltpu.VMEM((rows, q_cols), bf16),
            pltpu.VMEM((devices * rows // KB, KB, 2 * k_cols), bf16),
            pltpu.VMEM((most_down * rows // KB, KB, 2 * k_cols), bf16),
            pltpu.VMEM((select.shape[1] * KB, 2 * k_cols), bf16),
            pltpu.VMEM((rows, q_cols), bf16),
            pltpu.VMEM((tp, rows, q_cols), bf16),
            dma((PIECES, 4)),
            dma((PIECES, 4)),
            dma((2, most_up + 1, PIECES)),
            dma((2, most_up + 1, PIECES)),
            dma((2, most_up + 1)),
            dma((2, most_up + 1)),
            dma((PIECES, 4)),
            dma((PIECES, 4)),
            dma((4,)),
            pltpu.SemaphoreType.REGULAR,
        ],
        compiler_params=pltpu.CompilerParams(collective_id=0, has_side_effects=True),
        name="layer",
    )(tokens, gain, w_query, w_key, w_value, w_out, cosine, sine, select, select)


def per_device(tokens, gain, w_query, w_key, w_value, w_out, select):
    rows = tokens.shape[0]
    positions = lax.axis_index("kv") * rows + jnp.arange(rows, dtype=jnp.int32)
    cosine, sine = rotary_tables(positions)
    return layer(
        tokens, gain.reshape(1, -1), w_query, w_key, w_value, w_out, cosine, sine, select
    )


def solution(mesh):
    placed = (
        P(("grp", "kv"), "tp"),
        P(),
        P(None, "tp"),
        P(None, "tp"),
        P(None, "tp"),
        P(None, "tp"),
        P(("grp", "kv"), None),
    )
    return jax.shard_map(
        per_device, mesh=mesh, in_specs=placed, out_specs=P(("grp", "kv"), "tp"), check_vma=False
    )
```

```python
import functools

import jax
import jax.numpy as jnp
from jax import lax
from jax.experimental import pallas as pl
from jax.experimental.pallas import tpu as pltpu
from jax.sharding import PartitionSpec as P

HD = 128
QB = 128
KB = 32
PIECES = 4

epsilon = 1e-06
theta = 10000.0
MESH = pl.DeviceIdType.MESH


def rotary_table(positions):
    half = HD // 2
    column = jnp.arange(HD, dtype=jnp.int32)
    frequency = theta ** (-(2 * (column % half)).astype(jnp.float32) / HD)
    angles = positions.astype(jnp.float32)[:, None] * frequency[None, :]
    return jnp.where((column < half)[None, :], jnp.cos(angles), jnp.sin(angles))


def remote(src, dst, send, recv, **where):
    return pltpu.make_async_remote_copy(
        src_ref=src, dst_ref=dst, send_sem=send, recv_sem=recv, device_id=where, device_id_type=MESH
    )


class TpRing:
    def __init__(self, own, slots, send, recv, rows):
        self.n = lax.axis_size("tp")
        self.me = lax.axis_index("tp")
        self.right = lax.rem(self.me + 1, self.n)
        self.left = lax.rem(self.me + self.n - 1, self.n)
        self.far = lax.rem(self.me + 2, self.n)
        self.own, self.slots, self.send, self.recv, self.rows = own, slots, send, recv, rows

    def copy(self, chunk, kind):
        half = self.rows // 2
        start, size, source, to = {
            0: (0, self.rows, None, self.right),
            1: (0, self.rows, None, self.left),
            2: (0, half, self.left, self.right),
            3: (half, half, self.right, self.left),
        }[kind]
        at = pl.ds(chunk * self.rows + start, size)
        src = self.own.at[at] if source is None else self.slots.at[source, at]
        dst = self.slots.at[self.me if source is None else source, at]
        return remote(src, dst, self.send.at[chunk, kind], self.recv.at[chunk, kind], tp=to)

    def begin(self, chunk):
        self.copy(chunk, 0).start()
        self.copy(chunk, 1).start()

    def hand_on(self, chunk):
        self.copy(chunk, 0).wait_recv()
        self.copy(chunk, 2).start()
        self.copy(chunk, 1).wait_recv()
        self.copy(chunk, 3).start()

    def arrived(self, chunk):
        self.copy(chunk, 2).wait_recv()
        self.copy(chunk, 3).wait_recv()

    def sent(self, chunk):
        for kind in range(4):
            self.copy(chunk, kind).wait_send()


def layer_kernel(
    tok, gain, wq, wk, wv, w_out, table, listed, sel, out,
    slots, weights, queries, need, transit, keys, attended, mixing,
    send_t, recv_t, send_z, recv_z, send_c, recv_c, send_m, recv_m, local, go,
):
    rows, width = tok.shape
    tp = lax.axis_size("tp")
    chunk_rows = rows // PIECES
    devices = lax.axis_size("kv")
    chips = devices // 2
    most_up, most_down = reach(chips, 0)[0], reach(chips, PIECES - 1)[1]
    mine = lax.axis_index("kv")
    z, core = mine // 2, lax.rem(mine, 2)
    partner = mine + 1 - 2 * core
    up = lax.rem(mine + 2, devices)
    down = lax.rem(mine + devices - 2, devices)
    q_cols, k_cols = wq.shape[1], wk.shape[1]
    ring = TpRing(tok, slots, send_t, recv_t, chunk_rows)
    mix_ring = TpRing(attended, mixing, send_m, recv_m, chunk_rows)

    loads = [
        pltpu.make_async_copy(wq, weights.at[:, pl.ds(0, q_cols)], local.at[0]),
        pltpu.make_async_copy(wk, weights.at[:, pl.ds(q_cols, k_cols)], local.at[1]),
        pltpu.make_async_copy(wv, weights.at[:, pl.ds(q_cols + k_cols, k_cols)], local.at[2]),
        pltpu.make_async_copy(tok, slots.at[ring.me], local.at[3]),
    ]
    for load in loads:
        load.start()

    barrier = pltpu.get_barrier_semaphore()

    def hail(**where):
        pl.semaphore_signal(barrier, inc=1, device_id=where, device_id_type=MESH)

    hail(tp=ring.right)
    hail(tp=ring.left)
    hail(kv=partner)
    hail(kv=down)

    @pl.when(z < chips - 1)
    def _():
        hail(kv=up)

    @pl.when(z == 0)
    def _():
        pl.semaphore_wait(barrier, 4)

    @pl.when(z > 0)
    def _():
        pl.semaphore_wait(barrier, 5)

    @pl.when(z == chips - 1)
    def _():
        pl.semaphore_signal(go, inc=1, device_id={"kv": up}, device_id_type=MESH)

    own_blocks = rows // KB
    chunk_blocks = chunk_rows // KB

    def piece_rows(piece):
        return pl.ds(piece * chunk_rows, chunk_rows)

    def piece_blocks(holder, piece):
        return pl.ds(holder * own_blocks + piece * chunk_blocks, chunk_blocks)

    def goes_up(step, piece):
        return (step <= reach(chips, piece)[0]) & (z - step + 1 >= 0) & (z < chips - 1)

    def comes_up(step, piece):
        return (step <= reach(chips, piece)[0]) & (z - step >= 0)

    def goes_down(step, piece):
        far = reach(chips, piece)[1]
        return (step <= far) & (lax.rem(z + step - 1, chips) < far)

    def comes_down(step, piece):
        far = reach(chips, piece)[1]
        return (step <= far) & (lax.rem(z + step, chips) < far)

    def send_up(step, piece):
        block = need.at[piece_blocks(lax.rem(z - step + 1 + chips, chips) * 2 + core, piece)]
        return remote(block, block, send_z.at[0, step, piece], recv_z.at[0, step, piece], kv=up)

    def send_down(step, piece, from_transit, to_transit):
        chip = lax.rem(z + step - 1, chips)
        kept = need.at[piece_blocks(chip * 2 + core, piece)]
        passing = transit.at[piece_blocks(lax.rem(chip, most_down), piece)]
        return remote(
            passing if from_transit else kept, passing if to_transit else kept,
            send_z.at[1, step, piece], recv_z.at[1, step, piece], kv=down,
        )

    def across(direction, step, piece):
        chip = lax.rem(z - step + chips, chips) if direction == 0 else lax.rem(z + step, chips)
        block = need.at[piece_blocks(chip * 2 + core, piece)]
        return remote(
            block, block, send_c.at[direction, step], recv_c.at[direction, step], kv=partner
        )

    def across_whole(direction, step, share=1):
        block = need.at[pl.ds(mine * own_blocks, own_blocks // share)]
        return remote(
            block, block, send_c.at[direction, step], recv_c.at[direction, step], kv=partner
        )

    gain_row = gain[...].astype(jnp.float32).reshape(1, -1)

    def project(chunk):
        at = piece_rows(chunk)
        total = jnp.zeros((chunk_rows, weights.shape[1]), jnp.float32)
        squares = jnp.zeros((chunk_rows, 1), jnp.float32)
        for t in range(tp):
            block = slots[t, at, :].astype(jnp.float32)
            squares += jnp.sum(block * block, axis=1, keepdims=True)
            scaled = (block * gain_row[:, t * width:(t + 1) * width]).astype(
                jnp.bfloat16
            )
            total += jnp.dot(
                scaled, weights[t * width:(t + 1) * width, :], preferred_element_type=jnp.float32
            )
        total *= lax.rsqrt(squares / (tp * width) + epsilon)
        turns = table[at, :]
        swapped = pltpu.roll(turns, HD // 2, 1)
        front = lax.broadcasted_iota(jnp.int32, turns.shape, 1) < HD // 2
        cosine, sine = jnp.where(front, turns, swapped), jnp.where(front, -swapped, turns)
        heads = []
        for h in range((q_cols + k_cols) // HD):
            head = total[:, h * HD:(h + 1) * HD]
            heads.append((head * cosine + pltpu.roll(head, HD // 2, 1) * sine).astype(jnp.bfloat16))
        for h in range(q_cols // HD):
            queries[at, h * HD:(h + 1) * HD] = heads[h]
        kept = piece_blocks(mine, chunk)
        values = total[:, q_cols + k_cols:].astype(jnp.bfloat16)
        need[kept, :, 0:k_cols] = heads[-1].reshape(chunk_blocks, KB, k_cols)
        need[kept, :, k_cols:2 * k_cols] = values.reshape(chunk_blocks, KB, k_cols)

        @pl.when(goes_up(1, chunk))
        def _():
            send_up(1, chunk).start()

        @pl.when(goes_down(1, chunk) & (z > 0))
        def _():
            send_down(1, chunk, False, True).start()

    def hand_up(step, piece):
        @pl.when(comes_up(step, piece))
        def _():
            send_up(step, piece).wait_recv()

            @pl.when(goes_up(step + 1, piece))
            def _():
                send_up(step + 1, piece).start()

            across(0, step, piece).start()

    ring.begin(0)
    ring.begin(1)
    for load in loads:
        load.wait()
    for chunk in range(PIECES):
        if chunk == 0:
            ring.hand_on(0)
            ring.begin(2)
            ring.hand_on(1)
            ring.begin(3)
        elif chunk + 1 < PIECES:
            ring.hand_on(chunk + 1)
        ring.arrived(chunk)
        project(chunk)
        for step in range(1, chunk + 1):
            hand_up(step, chunk - step)
    give = across_whole(0, 0)
    give.start()

    blocks, listed_slots = sel.shape
    wide = listed_slots * KB
    heads_here = q_cols // HD

    def attend(b, key_pos):
        @pl.loop(0, listed_slots, unroll=4)
        def _(s):
            keys[pl.ds(pl.multiple_of(s * KB, KB), KB), :] = need[jnp.maximum(listed[b, s], 0)]

        q_pos = mine * rows + b * QB + lax.broadcasted_iota(jnp.int32, (QB, wide), 0)
        allowed = jnp.broadcast_to(key_pos[b:b + 1, :], (QB, wide)) <= q_pos
        for h in range(heads_here):
            score = lax.dot_general(
                queries[b * QB:(b + 1) * QB, h * HD:(h + 1) * HD], keys[:, 0:HD],
                (((1,), (1,)), ((), ())), preferred_element_type=jnp.float32,
            ) * HD ** (-0.5)
            score = jnp.where(allowed, score, -jnp.inf)
            raised = jnp.exp(score - jnp.max(score, axis=1, keepdims=True))
            parts = (raised / jnp.sum(raised, axis=1, keepdims=True)).astype(jnp.bfloat16)
            attended[b * QB:(b + 1) * QB, h * HD:(h + 1) * HD] = jnp.dot(
                parts, keys[:, HD:2 * HD], preferred_element_type=jnp.float32
            ).astype(jnp.bfloat16)
        mixing[mix_ring.me, b * QB:(b + 1) * QB, :] = attended[b * QB:(b + 1) * QB, :]

    def mix(chunk):
        at = piece_rows(chunk)
        total = jnp.zeros((chunk_rows, out.shape[1]), jnp.float32)
        for t in range(tp):
            total += jnp.dot(
                mixing[t, at, :], w_out[t * q_cols:(t + 1) * q_cols, :],
                preferred_element_type=jnp.float32,
            )
        out[at, :] = total.astype(jnp.bfloat16)

    def all_here():
        give.wait()

        @pl.loop(1, jnp.minimum(z, most_up - 1) + 1)
        def _(step):
            across_whole(0, step).wait()

        @pl.loop(jnp.maximum(chips - z, 1), most_down)
        def _(step):
            across_whole(1, step).wait()

        @pl.when(z >= most_up)
        def _():
            across_whole(0, most_up, 2).wait()
            across_whole(1, most_down, 2).wait()

    def key_positions():
        spread = (
            lax.broadcasted_iota(jnp.int32, (listed_slots, wide), 1) // KB
            == lax.broadcasted_iota(jnp.int32, (listed_slots, wide), 0)
        ).astype(jnp.float32)
        ids = sel[...]
        safe = jnp.where(ids < 0, 1 << 20, ids)
        high = (safe // 64).astype(jnp.float32)
        low = lax.rem(safe, 64).astype(jnp.float32)
        found = jnp.dot(high, spread, preferred_element_type=jnp.float32) * 64.0 + jnp.dot(
            low, spread, preferred_element_type=jnp.float32
        )
        key_pos = found.astype(jnp.int32) * KB + lax.rem(
            lax.broadcasted_iota(jnp.int32, (blocks, wide), 1), KB
        )
        return key_pos

    def stage(which):
        if which == 0:
            all_here()
        if which < PIECES:
            attend(which, key_positions())
            mix_ring.begin(which)
            if which:
                mix_ring.hand_on(which - 1)
        else:
            if which == PIECES:
                mix_ring.hand_on(PIECES - 1)
            mix_ring.arrived(which - PIECES)
            mix(which - PIECES)

    attend_at = jnp.minimum(z, most_up)

    @pl.loop(0, most_up + 2 * PIECES)
    def _(step):
        for piece in range(PIECES):
            @pl.when((step > 0) & (step + piece >= PIECES))
            def _():
                hand_up(step, piece)

            @pl.when((step > 0) & comes_down(step, piece))
            def _():
                send_down(step, piece, False, False).wait_recv()
                wrapped = z + step >= chips
                onward = step < reach(chips, piece)[1]

                @pl.when(onward & wrapped)
                def _():
                    send_down(step + 1, piece, False, False).start()

                @pl.when(onward & jnp.logical_not(wrapped) & (z > 0))
                def _():
                    send_down(step + 1, piece, True, True).start()

                @pl.when(onward & (z == 0))
                def _():
                    send_down(step + 1, piece, True, False).start()

                @pl.when(wrapped)
                def _():
                    across(1, step, piece).start()

        @pl.when((step == 0) & (z == 0))
        def _():
            pl.semaphore_wait(go, 1)
            for piece in range(PIECES):
                send_down(1, piece, False, False).start()

        for which in range(2 * PIECES):
            @pl.when(step == attend_at + which)
            def _():
                stage(which)

    for chunk in range(PIECES):
        ring.sent(chunk)
        mix_ring.sent(chunk)

    @pl.loop(1, most_up + 1)
    def _(step):
        for piece in range(PIECES):
            @pl.when(goes_up(step, piece))
            def _():
                send_up(step, piece).wait_send()

            @pl.when(goes_down(step, piece))
            def _():
                send_down(step, piece, False, False).wait_send()


def reach(chips, piece):
    most_up = chips // 2 + 1 + (piece < PIECES // 2)
    return most_up, chips - 1 - most_up


def layer(tokens, gain, w_query, w_key, w_value, w_out, table, select):
    rows, width = tokens.shape
    devices = lax.axis_size("kv")
    tp = lax.axis_size("tp")
    q_cols, k_cols = w_query.shape[1], w_key.shape[1]
    chips = devices // 2
    most_up, most_down = reach(chips, 0)[0], reach(chips, PIECES - 1)[1]
    dma = pltpu.SemaphoreType.DMA
    bf16 = jnp.bfloat16
    vmem = pl.BlockSpec(memory_space=pltpu.VMEM)
    hbm = pl.BlockSpec(memory_space=pl.ANY)
    smem = pl.BlockSpec(memory_space=pltpu.SMEM)
    return pl.pallas_call(
        layer_kernel,
        out_shape=jax.ShapeDtypeStruct((rows, w_out.shape[1]), bf16),
        in_specs=[vmem, vmem, hbm, hbm, hbm, vmem, vmem, smem, vmem],
        out_specs=vmem,
        scratch_shapes=[
            pltpu.VMEM((tp, rows, width), bf16),
            pltpu.VMEM((tp * width, q_cols + 2 * k_cols), bf16),
            pltpu.VMEM((rows, q_cols), bf16),
            pltpu.VMEM((devices * rows // KB, KB, 2 * k_cols), bf16),
            pltpu.VMEM((most_down * rows // KB, KB, 2 * k_cols), bf16),
            pltpu.VMEM((select.shape[1] * KB, 2 * k_cols), bf16),
            pltpu.VMEM((rows, q_cols), bf16),
            pltpu.VMEM((tp, rows, q_cols), bf16),
            dma((PIECES, 4)),
            dma((PIECES, 4)),
            dma((2, most_up + 1, PIECES)),
            dma((2, most_up + 1, PIECES)),
            dma((2, most_up + 1)),
            dma((2, most_up + 1)),
            dma((PIECES, 4)),
            dma((PIECES, 4)),
            dma((4,)),
            pltpu.SemaphoreType.REGULAR,
        ],
        compiler_params=pltpu.CompilerParams(collective_id=0, has_side_effects=True),
        name="layer",
    )(tokens, gain, w_query, w_key, w_value, w_out, table, select, select)


def per_device(tokens, gain, w_query, w_key, w_value, w_out, select):
    rows = tokens.shape[0]
    positions = lax.axis_index("kv") * rows + jnp.arange(rows, dtype=jnp.int32)
    table = rotary_table(positions)
    return layer(
        tokens, gain, w_query, w_key, w_value, w_out, table, select
    )


def solution(mesh):
    placed = (
        P(("grp", "kv"), "tp"),
        P(),
        P(None, "tp"),
        P(None, "tp"),
        P(None, "tp"),
        P(None, "tp"),
        P(("grp", "kv"), None),
    )
    return jax.shard_map(
        per_device, mesh=mesh, in_specs=placed, out_specs=P(("grp", "kv"), "tp"), check_vma=False
    )
```

```python
import functools

import jax
import jax.numpy as jnp
from jax import lax
from jax.experimental import pallas as pl
from jax.experimental.pallas import tpu as pltpu
from jax.sharding import PartitionSpec as P

HD = 128
QB = 128
KB = 32
PIECES = 4
DIRECT = 2

epsilon = 1e-06
theta = 10000.0
MESH = pl.DeviceIdType.MESH


def rotary_tables(positions):
    frequency = theta ** (-jnp.arange(0, HD, 2, dtype=jnp.float32) / HD)
    angles = positions.astype(jnp.float32)[:, None] * frequency[None, :]
    return jnp.cos(angles), jnp.sin(angles)


def remote(src, dst, send, recv, **where):
    return pltpu.make_async_remote_copy(
        src_ref=src, dst_ref=dst, send_sem=send, recv_sem=recv, device_id=where, device_id_type=MESH
    )


class TpRing:
    def __init__(self, own, slots, send, recv, rows):
        self.n = lax.axis_size("tp")
        self.me = lax.axis_index("tp")
        self.right = lax.rem(self.me + 1, self.n)
        self.left = lax.rem(self.me + self.n - 1, self.n)
        self.far = lax.rem(self.me + 2, self.n)
        self.own, self.slots, self.send, self.recv, self.rows = own, slots, send, recv, rows

    def copy(self, chunk, kind):
        half = self.rows // 2
        start, size, source, to = {
            0: (0, self.rows, None, self.right),
            1: (0, self.rows, None, self.left),
            2: (0, half, self.left, self.right),
            3: (half, half, self.right, self.left),
        }[kind]
        at = pl.ds(chunk * self.rows + start, size)
        src = self.own.at[at] if source is None else self.slots.at[source, at]
        dst = self.slots.at[self.me if source is None else source, at]
        return remote(src, dst, self.send.at[chunk, kind], self.recv.at[chunk, kind], tp=to)

    def begin(self, chunk):
        self.copy(chunk, 0).start()
        self.copy(chunk, 1).start()

    def hand_on(self, chunk):
        self.copy(chunk, 0).wait_recv()
        self.copy(chunk, 2).start()
        self.copy(chunk, 1).wait_recv()
        self.copy(chunk, 3).start()

    def arrived(self, chunk):
        self.copy(chunk, 2).wait_recv()
        self.copy(chunk, 3).wait_recv()

    def sent(self, chunk):
        for kind in range(4):
            self.copy(chunk, kind).wait_send()


def layer_kernel(
    tok, gain, wq, wk, wv, w_out, cos, sin, listed, sel, out,
    slots, weights, queries, need, transit, keys, attended, mixing,
    send_t, recv_t, send_z, recv_z, send_c, recv_c, send_m, recv_m, send_d, local, go,
):
    rows, width = tok.shape
    tp = lax.axis_size("tp")
    chunk_rows = rows // PIECES
    devices = lax.axis_size("kv")
    chips = devices // 2
    most_up, most_down = reach(chips)
    mine = lax.axis_index("kv")
    z, core = mine // 2, lax.rem(mine, 2)
    partner = mine + 1 - 2 * core
    up = lax.rem(mine + 2, devices)
    down = lax.rem(mine + devices - 2, devices)
    q_cols, k_cols = wq.shape[1], wk.shape[1]
    ring = TpRing(tok, slots, send_t, recv_t, chunk_rows)
    mix_ring = TpRing(attended, mixing, send_m, recv_m, chunk_rows)

    loads = [
        pltpu.make_async_copy(wq, weights.at[:, pl.ds(0, q_cols)], local.at[0]),
        pltpu.make_async_copy(wk, weights.at[:, pl.ds(q_cols, k_cols)], local.at[1]),
        pltpu.make_async_copy(wv, weights.at[:, pl.ds(q_cols + k_cols, k_cols)], local.at[2]),
        pltpu.make_async_copy(tok, slots.at[ring.me], local.at[3]),
    ]
    for load in loads:
        load.start()

    barrier = pltpu.get_barrier_semaphore()

    def hail(**where):
        pl.semaphore_signal(barrier, inc=1, device_id=where, device_id_type=MESH)

    hail(tp=ring.right)
    hail(tp=ring.left)
    hail(kv=partner)
    hail(kv=down)

    @pl.when(z < chips - 1)
    def _():
        hail(kv=up)

    last = (chips - 1) * 2 + core

    @pl.when((z > 0) & (z <= DIRECT))
    def _():
        hail(kv=last)

    @pl.when(z == 0)
    def _():
        pl.semaphore_wait(barrier, 4)

    @pl.when((z > 0) & (z < chips - 1))
    def _():
        pl.semaphore_wait(barrier, 5)

    @pl.when(z == chips - 1)
    def _():
        pl.semaphore_wait(barrier, 5 + DIRECT)
        for chip in range(DIRECT + 1):
            pl.semaphore_signal(
                go, inc=1, device_id={"kv": chip * 2 + core}, device_id_type=MESH
            )

    own_blocks = rows // KB
    chunk_blocks = chunk_rows // KB

    def piece_rows(piece):
        return pl.ds(piece * chunk_rows, chunk_rows)

    def piece_blocks(holder, piece):
        return pl.ds(holder * own_blocks + piece * chunk_blocks, chunk_blocks)

    def by_relay(at):
        return (at == 0) | (at > DIRECT)

    def goes_up(step):
        return (step <= reach(chips)[0]) & (z - step + 1 >= 0) & (z < chips - 1)

    def comes_up(step):
        return (step <= reach(chips)[0]) & (z - step >= 0)

    def goes_down(step):
        far = reach(chips)[1]
        return (step <= far) & (lax.rem(z + step - 1, chips) < far) & by_relay(z + step - 1)

    def comes_down(step):
        far = reach(chips)[1]
        return (step <= far) & (lax.rem(z + step, chips) < far) & by_relay(z + step)

    def send_up(step, piece):
        block = need.at[piece_blocks(lax.rem(z - step + 1 + chips, chips) * 2 + core, piece)]
        return remote(block, block, send_z.at[0, step, piece], recv_z.at[0, step, piece], kv=up)

    def send_down(step, piece, from_transit, to_transit):
        chip = lax.rem(z + step - 1, chips)
        kept = need.at[piece_blocks(chip * 2 + core, piece)]
        passing = transit.at[piece_blocks(lax.rem(chip, most_down), piece)]
        return remote(
            passing if from_transit else kept, passing if to_transit else kept,
            send_z.at[1, step, piece], recv_z.at[1, step, piece], kv=down,
        )

    def send_direct(piece):
        block = need.at[piece_blocks(mine, piece)]
        step = lax.rem(z, DIRECT + 1) + 1
        return remote(block, block, send_d.at[piece], recv_z.at[1, step, piece], kv=last)

    def across(direction, step, piece):
        chip = lax.rem(z - step + chips, chips) if direction == 0 else lax.rem(z + step, chips)
        block = need.at[piece_blocks(chip * 2 + core, piece)]
        return remote(
            block, block, send_c.at[direction, step], recv_c.at[direction, step], kv=partner
        )

    def across_whole(direction, step):
        block = need.at[pl.ds(mine * own_blocks, own_blocks)]
        return remote(
            block, block, send_c.at[direction, step], recv_c.at[direction, step], kv=partner
        )

    gain_row = gain[...].astype(jnp.float32).reshape(1, -1)

    def project(chunk):
        at = piece_rows(chunk)
        total = jnp.zeros((chunk_rows, weights.shape[1]), jnp.float32)
        squares = jnp.zeros((chunk_rows, 1), jnp.float32)
        for t in range(tp):
            block = slots[t, at, :].astype(jnp.float32)
            squares += jnp.sum(block * block, axis=1, keepdims=True)
            scaled = (block * gain_row[:, t * width:(t + 1) * width]).astype(
                jnp.bfloat16
            )
            total += jnp.dot(
                scaled, weights[t * width:(t + 1) * width, :], preferred_element_type=jnp.float32
            )
        total *= lax.rsqrt(squares / (tp * width) + epsilon)
        c, n = cos[at, :], sin[at, :]
        cosine, sine = jnp.concatenate([c, c], 1), jnp.concatenate([-n, n], 1)
        heads = []
        for h in range((q_cols + k_cols) // HD):
            head = total[:, h * HD:(h + 1) * HD]
            heads.append((head * cosine + pltpu.roll(head, HD // 2, 1) * sine).astype(jnp.bfloat16))
        for h in range(q_cols // HD):
            queries[at, h * HD:(h + 1) * HD] = heads[h]
        kept = piece_blocks(mine, chunk)
        values = total[:, q_cols + k_cols:].astype(jnp.bfloat16)
        need[kept, :, 0:k_cols] = heads[-1].reshape(chunk_blocks, KB, k_cols)
        need[kept, :, k_cols:2 * k_cols] = values.reshape(chunk_blocks, KB, k_cols)

        @pl.when(goes_up(1))
        def _():
            send_up(1, chunk).start()

        @pl.when(goes_down(1) & (z > 0))
        def _():
            send_down(1, chunk, False, True).start()

    def hand_up(step, piece):
        @pl.when(comes_up(step))
        def _():
            send_up(step, piece).wait_recv()

            @pl.when(goes_up(step + 1))
            def _():
                send_up(step + 1, piece).start()

            across(0, step, piece).start()

    ring.begin(0)
    ring.begin(1)
    for load in loads:
        load.wait()
    for chunk in range(PIECES):
        if chunk == 0:
            ring.hand_on(0)
            ring.begin(2)
            ring.hand_on(1)
            ring.begin(3)
        elif chunk + 1 < PIECES:
            ring.hand_on(chunk + 1)
        ring.arrived(chunk)
        project(chunk)

        @pl.when(z >= PIECES)
        def _():
            for step in range(1, chunk + 1):
                hand_up(step, chunk - step)

    give = across_whole(0, 0)
    give.start()

    blocks, listed_slots = sel.shape
    wide = listed_slots * KB
    heads_here = q_cols // HD

    def attend(b, key_pos):
        @pl.loop(0, listed_slots, unroll=4)
        def _(s):
            keys[pl.ds(pl.multiple_of(s * KB, KB), KB), :] = need[jnp.maximum(listed[b, s], 0)]

        q_pos = mine * rows + b * QB + lax.broadcasted_iota(jnp.int32, (QB, wide), 0)
        allowed = jnp.broadcast_to(key_pos[b:b + 1, :], (QB, wide)) <= q_pos
        for h in range(heads_here):
            score = lax.dot_general(
                queries[b * QB:(b + 1) * QB, h * HD:(h + 1) * HD], keys[:, 0:HD],
                (((1,), (1,)), ((), ())), preferred_element_type=jnp.float32,
            ) * HD ** (-0.5)
            score = jnp.where(allowed, score, -jnp.inf)
            raised = jnp.exp(score - jnp.max(score, axis=1, keepdims=True))
            parts = (raised / jnp.sum(raised, axis=1, keepdims=True)).astype(jnp.bfloat16)
            attended[b * QB:(b + 1) * QB, h * HD:(h + 1) * HD] = jnp.dot(
                parts, keys[:, HD:2 * HD], preferred_element_type=jnp.float32
            ).astype(jnp.bfloat16)
        mixing[mix_ring.me, b * QB:(b + 1) * QB, :] = attended[b * QB:(b + 1) * QB, :]

    def mix(chunk):
        at = piece_rows(chunk)
        total = jnp.zeros((chunk_rows, out.shape[1]), jnp.float32)
        for t in range(tp):
            total += jnp.dot(
                mixing[t, at, :], w_out[t * q_cols:(t + 1) * q_cols, :],
                preferred_element_type=jnp.float32,
            )
        out[at, :] = total.astype(jnp.bfloat16)

    def all_here():
        give.wait()

        @pl.loop(1, jnp.minimum(z, most_up) + 1)
        def _(step):
            across_whole(0, step).wait()

        @pl.loop(jnp.maximum(chips - z, 1), most_down + 1)
        def _(step):
            across_whole(1, step).wait()

    def key_positions():
        spread = (
            lax.broadcasted_iota(jnp.int32, (listed_slots, wide), 1) // KB
            == lax.broadcasted_iota(jnp.int32, (listed_slots, wide), 0)
        ).astype(jnp.float32)
        ids = sel[...]
        safe = jnp.where(ids < 0, 1 << 20, ids)
        high = (safe // 64).astype(jnp.float32)
        low = lax.rem(safe, 64).astype(jnp.float32)
        found = jnp.dot(high, spread, preferred_element_type=jnp.float32) * 64.0 + jnp.dot(
            low, spread, preferred_element_type=jnp.float32
        )
        key_pos = found.astype(jnp.int32) * KB + lax.rem(
            lax.broadcasted_iota(jnp.int32, (blocks, wide), 1), KB
        )
        return key_pos

    def stage(which):
        if which == 0:
            all_here()
        if which < PIECES:
            attend(which, key_positions())
            mix_ring.begin(which)
            if which:
                mix_ring.hand_on(which - 1)
        else:
            if which == PIECES:
                mix_ring.hand_on(PIECES - 1)
            mix_ring.arrived(which - PIECES)
            mix(which - PIECES)

    attend_at = jnp.minimum(z, most_up)

    @pl.loop(0, most_up + 2 * PIECES)
    def _(step):
        for piece in range(PIECES):
            @pl.when((step > 0) & ((step + piece >= PIECES) | (z < PIECES)))
            def _():
                hand_up(step, piece)

            @pl.when((step > 0) & comes_down(step))
            def _():
                send_down(step, piece, False, False).wait_recv()
                wrapped = z + step >= chips
                onward = step < reach(chips)[1]

                @pl.when(onward & wrapped)
                def _():
                    send_down(step + 1, piece, False, False).start()

                @pl.when(onward & jnp.logical_not(wrapped) & (z > 0))
                def _():
                    send_down(step + 1, piece, True, True).start()

                @pl.when(onward & (z == 0))
                def _():
                    send_down(step + 1, piece, True, False).start()

                @pl.when(wrapped)
                def _():
                    across(1, step, piece).start()

        @pl.when((step == 0) & (z == 0))
        def _():
            pl.semaphore_wait(go, 1)
            for piece in range(PIECES):
                send_down(1, piece, False, False).start()

        @pl.when((step == 0) & (z > 0) & (z <= DIRECT))
        def _():
            pl.semaphore_wait(go, 1)
            for piece in range(PIECES):
                send_direct(piece).start()

        for which in range(2 * PIECES):
            @pl.when(step == attend_at + which)
            def _():
                stage(which)

    for chunk in range(PIECES):
        ring.sent(chunk)
        mix_ring.sent(chunk)

    @pl.when((z > 0) & (z <= DIRECT))
    def _():
        for piece in range(PIECES):
            send_direct(piece).wait_send()

    @pl.loop(1, most_up + 1)
    def _(step):
        for piece in range(PIECES):
            @pl.when(goes_up(step))
            def _():
                send_up(step, piece).wait_send()

            @pl.when(goes_down(step))
            def _():
                send_down(step, piece, False, False).wait_send()


def reach(chips):
    most_up = chips // 2 + 1
    return most_up, chips - 1 - most_up


def layer(tokens, gain, w_query, w_key, w_value, w_out, tables, select):
    rows, width = tokens.shape
    devices = lax.axis_size("kv")
    tp = lax.axis_size("tp")
    q_cols, k_cols = w_query.shape[1], w_key.shape[1]
    chips = devices // 2
    most_up, most_down = reach(chips)
    dma = pltpu.SemaphoreType.DMA
    bf16 = jnp.bfloat16
    vmem = pl.BlockSpec(memory_space=pltpu.VMEM)
    hbm = pl.BlockSpec(memory_space=pl.ANY)
    smem = pl.BlockSpec(memory_space=pltpu.SMEM)
    return pl.pallas_call(
        layer_kernel,
        out_shape=jax.ShapeDtypeStruct((rows, w_out.shape[1]), bf16),
        in_specs=[vmem, vmem, hbm, hbm, hbm, vmem, vmem, vmem, smem, vmem],
        out_specs=vmem,
        scratch_shapes=[
            pltpu.VMEM((tp, rows, width), bf16),
            pltpu.VMEM((tp * width, q_cols + 2 * k_cols), bf16),
            pltpu.VMEM((rows, q_cols), bf16),
            pltpu.VMEM((devices * rows // KB, KB, 2 * k_cols), bf16),
            pltpu.VMEM((most_down * rows // KB, KB, 2 * k_cols), bf16),
            pltpu.VMEM((select.shape[1] * KB, 2 * k_cols), bf16),
            pltpu.VMEM((rows, q_cols), bf16),
            pltpu.VMEM((tp, rows, q_cols), bf16),
            dma((PIECES, 4)),
            dma((PIECES, 4)),
            dma((2, most_up + 1, PIECES)),
            dma((2, most_up + 1, PIECES)),
            dma((2, most_up + 1)),
            dma((2, most_up + 1)),
            dma((PIECES, 4)),
            dma((PIECES, 4)),
            dma((PIECES,)),
            dma((4,)),
            pltpu.SemaphoreType.REGULAR,
        ],
        compiler_params=pltpu.CompilerParams(collective_id=0, has_side_effects=True),
        name="layer",
    )(tokens, gain, w_query, w_key, w_value, w_out, *tables, select, select)


def per_device(tokens, gain, w_query, w_key, w_value, w_out, select):
    rows = tokens.shape[0]
    positions = lax.axis_index("kv") * rows + jnp.arange(rows, dtype=jnp.int32)
    tables = rotary_tables(positions)
    return layer(
        tokens, gain, w_query, w_key, w_value, w_out, tables, select
    )


def solution(mesh):
    placed = (
        P(("grp", "kv"), "tp"),
        P(),
        P(None, "tp"),
        P(None, "tp"),
        P(None, "tp"),
        P(None, "tp"),
        P(("grp", "kv"), None),
    )
    return jax.shard_map(
        per_device, mesh=mesh, in_specs=placed, out_specs=P(("grp", "kv"), "tp"), check_vma=False
    )
```

```python
import functools

import jax
import jax.numpy as jnp
from jax import lax
from jax.experimental import pallas as pl
from jax.experimental.pallas import tpu as pltpu
from jax.sharding import PartitionSpec as P

HD = 128
QB = 128
KB = 32
PIECES = 4
DIRECT = 3

epsilon = 1e-06
theta = 10000.0
MESH = pl.DeviceIdType.MESH


def rotary_tables(positions):
    frequency = theta ** (-jnp.arange(0, HD, 2, dtype=jnp.float32) / HD)
    angles = positions.astype(jnp.float32)[:, None] * frequency[None, :]
    return jnp.cos(angles), jnp.sin(angles)


def remote(src, dst, send, recv, **where):
    return pltpu.make_async_remote_copy(
        src_ref=src, dst_ref=dst, send_sem=send, recv_sem=recv, device_id=where, device_id_type=MESH
    )


class TpRing:
    def __init__(self, own, slots, send, recv, rows):
        self.n = lax.axis_size("tp")
        self.me = lax.axis_index("tp")
        self.right = lax.rem(self.me + 1, self.n)
        self.left = lax.rem(self.me + self.n - 1, self.n)
        self.far = lax.rem(self.me + 2, self.n)
        self.own, self.slots, self.send, self.recv, self.rows = own, slots, send, recv, rows

    def copy(self, chunk, kind):
        half = self.rows // 2
        start, size, source, to = {
            0: (0, self.rows, None, self.right),
            1: (0, self.rows, None, self.left),
            2: (0, half, self.left, self.right),
            3: (half, half, self.right, self.left),
        }[kind]
        at = pl.ds(chunk * self.rows + start, size)
        src = self.own.at[at] if source is None else self.slots.at[source, at]
        dst = self.slots.at[self.me if source is None else source, at]
        return remote(src, dst, self.send.at[chunk, kind], self.recv.at[chunk, kind], tp=to)

    def begin(self, chunk):
        self.copy(chunk, 0).start()
        self.copy(chunk, 1).start()

    def hand_on(self, chunk):
        self.copy(chunk, 0).wait_recv()
        self.copy(chunk, 2).start()
        self.copy(chunk, 1).wait_recv()
        self.copy(chunk, 3).start()

    def arrived(self, chunk):
        self.copy(chunk, 2).wait_recv()
        self.copy(chunk, 3).wait_recv()

    def sent(self, chunk):
        for kind in range(4):
            self.copy(chunk, kind).wait_send()


def layer_kernel(
    tok, gain, wq, wk, wv, w_out, cos, sin, listed, sel, out,
    slots, weights, queries, need, transit, keys, attended, mixing,
    send_t, recv_t, send_z, recv_z, send_c, recv_c, send_m, recv_m, send_d, local, go,
):
    rows, width = tok.shape
    tp = lax.axis_size("tp")
    chunk_rows = rows // PIECES
    devices = lax.axis_size("kv")
    chips = devices // 2
    most_up, most_down = reach(chips)
    mine = lax.axis_index("kv")
    z, core = mine // 2, lax.rem(mine, 2)
    partner = mine + 1 - 2 * core
    up = lax.rem(mine + 2, devices)
    down = lax.rem(mine + devices - 2, devices)
    q_cols, k_cols = wq.shape[1], wk.shape[1]
    ring = TpRing(tok, slots, send_t, recv_t, chunk_rows)
    mix_ring = TpRing(attended, mixing, send_m, recv_m, chunk_rows)

    loads = [
        pltpu.make_async_copy(wq, weights.at[:, pl.ds(0, q_cols)], local.at[0]),
        pltpu.make_async_copy(wk, weights.at[:, pl.ds(q_cols, k_cols)], local.at[1]),
        pltpu.make_async_copy(wv, weights.at[:, pl.ds(q_cols + k_cols, k_cols)], local.at[2]),
        pltpu.make_async_copy(tok, slots.at[ring.me], local.at[3]),
    ]
    for load in loads:
        load.start()

    barrier = pltpu.get_barrier_semaphore()

    def hail(**where):
        pl.semaphore_signal(barrier, inc=1, device_id=where, device_id_type=MESH)

    hail(tp=ring.right)
    hail(tp=ring.left)
    hail(kv=partner)
    hail(kv=down)

    @pl.when(z < chips - 1)
    def _():
        hail(kv=up)

    last = (chips - 1) * 2 + core

    @pl.when((z > 0) & (z <= DIRECT))
    def _():
        hail(kv=last)

    @pl.when(z == 0)
    def _():
        pl.semaphore_wait(barrier, 4)

    @pl.when((z > 0) & (z < chips - 1))
    def _():
        pl.semaphore_wait(barrier, 5)

    @pl.when(z == chips - 1)
    def _():
        pl.semaphore_wait(barrier, 5 + DIRECT)
        for chip in range(DIRECT + 1):
            pl.semaphore_signal(
                go, inc=1, device_id={"kv": chip * 2 + core}, device_id_type=MESH
            )

    own_blocks = rows // KB
    chunk_blocks = chunk_rows // KB

    def piece_rows(piece):
        return pl.ds(piece * chunk_rows, chunk_rows)

    def piece_blocks(holder, piece):
        return pl.ds(holder * own_blocks + piece * chunk_blocks, chunk_blocks)

    def by_relay(at):
        return (at == 0) | (at > DIRECT)

    def goes_up(step):
        return (step <= reach(chips)[0]) & (z - step + 1 >= 0) & (z < chips - 1)

    def comes_up(step):
        return (step <= reach(chips)[0]) & (z - step >= 0)

    def goes_down(step):
        far = reach(chips)[1]
        return (step <= far) & (lax.rem(z + step - 1, chips) < far) & by_relay(z + step - 1)

    def comes_down(step):
        far = reach(chips)[1]
        return (step <= far) & (lax.rem(z + step, chips) < far) & by_relay(z + step)

    def send_up(step, piece):
        block = need.at[piece_blocks(lax.rem(z - step + 1 + chips, chips) * 2 + core, piece)]
        return remote(block, block, send_z.at[0, step, piece], recv_z.at[0, step, piece], kv=up)

    def send_down(step, piece, from_transit, to_transit):
        chip = lax.rem(z + step - 1, chips)
        kept = need.at[piece_blocks(chip * 2 + core, piece)]
        passing = transit.at[piece_blocks(lax.rem(chip, most_down), piece)]
        return remote(
            passing if from_transit else kept, passing if to_transit else kept,
            send_z.at[1, step, piece], recv_z.at[1, step, piece], kv=down,
        )

    def send_direct(piece):
        block = need.at[piece_blocks(mine, piece)]
        step = lax.rem(z, DIRECT + 1) + 1
        return remote(block, block, send_d.at[piece], recv_z.at[1, step, piece], kv=last)

    def across(direction, step, piece):
        chip = lax.rem(z - step + chips, chips) if direction == 0 else lax.rem(z + step, chips)
        block = need.at[piece_blocks(chip * 2 + core, piece)]
        return remote(
            block, block, send_c.at[direction, step], recv_c.at[direction, step], kv=partner
        )

    def across_whole(direction, step):
        block = need.at[pl.ds(mine * own_blocks, own_blocks)]
        return remote(
            block, block, send_c.at[direction, step], recv_c.at[direction, step], kv=partner
        )

    gain_row = gain[...].astype(jnp.float32).reshape(1, -1)

    def project(chunk):
        at = piece_rows(chunk)
        total = jnp.zeros((chunk_rows, weights.shape[1]), jnp.float32)
        squares = jnp.zeros((chunk_rows, 1), jnp.float32)
        for t in range(tp):
            block = slots[t, at, :].astype(jnp.float32)
            squares += jnp.sum(block * block, axis=1, keepdims=True)
            scaled = (block * gain_row[:, t * width:(t + 1) * width]).astype(
                jnp.bfloat16
            )
            total += jnp.dot(
                scaled, weights[t * width:(t + 1) * width, :], preferred_element_type=jnp.float32
            )
        total *= lax.rsqrt(squares / (tp * width) + epsilon)
        c, n = cos[at, :], sin[at, :]
        cosine, sine = jnp.concatenate([c, c], 1), jnp.concatenate([-n, n], 1)
        heads = []
        for h in range((q_cols + k_cols) // HD):
            head = total[:, h * HD:(h + 1) * HD]
            heads.append((head * cosine + pltpu.roll(head, HD // 2, 1) * sine).astype(jnp.bfloat16))
        for h in range(q_cols // HD):
            queries[at, h * HD:(h + 1) * HD] = heads[h]
        kept = piece_blocks(mine, chunk)
        values = total[:, q_cols + k_cols:].astype(jnp.bfloat16)
        need[kept, :, 0:k_cols] = heads[-1].reshape(chunk_blocks, KB, k_cols)
        need[kept, :, k_cols:2 * k_cols] = values.reshape(chunk_blocks, KB, k_cols)

        @pl.when(goes_up(1))
        def _():
            send_up(1, chunk).start()

        @pl.when(goes_down(1) & (z > 0))
        def _():
            send_down(1, chunk, False, True).start()

    def hand_up(step, piece):
        @pl.when(comes_up(step))
        def _():
            send_up(step, piece).wait_recv()

            @pl.when(goes_up(step + 1))
            def _():
                send_up(step + 1, piece).start()

            across(0, step, piece).start()

    ring.begin(0)
    ring.begin(1)
    for load in loads:
        load.wait()
    for chunk in range(PIECES):
        if chunk == 0:
            ring.hand_on(0)
            ring.begin(2)
            ring.hand_on(1)
            ring.begin(3)
        elif chunk + 1 < PIECES:
            ring.hand_on(chunk + 1)
        ring.arrived(chunk)
        project(chunk)

        @pl.when(z >= PIECES)
        def _():
            for step in range(1, chunk + 1):
                hand_up(step, chunk - step)

    give = across_whole(0, 0)
    give.start()

    blocks, listed_slots = sel.shape
    wide = listed_slots * KB
    heads_here = q_cols // HD

    def attend(b, key_pos):
        @pl.loop(0, listed_slots, unroll=4)
        def _(s):
            keys[pl.ds(pl.multiple_of(s * KB, KB), KB), :] = need[jnp.maximum(listed[b, s], 0)]

        q_pos = mine * rows + b * QB + lax.broadcasted_iota(jnp.int32, (QB, wide), 0)
        allowed = jnp.broadcast_to(key_pos[b:b + 1, :], (QB, wide)) <= q_pos
        for h in range(heads_here):
            score = lax.dot_general(
                queries[b * QB:(b + 1) * QB, h * HD:(h + 1) * HD], keys[:, 0:HD],
                (((1,), (1,)), ((), ())), preferred_element_type=jnp.float32,
            ) * HD ** (-0.5)
            score = jnp.where(allowed, score, -jnp.inf)
            raised = jnp.exp(score - jnp.max(score, axis=1, keepdims=True))
            parts = (raised / jnp.sum(raised, axis=1, keepdims=True)).astype(jnp.bfloat16)
            attended[b * QB:(b + 1) * QB, h * HD:(h + 1) * HD] = jnp.dot(
                parts, keys[:, HD:2 * HD], preferred_element_type=jnp.float32
            ).astype(jnp.bfloat16)
        mixing[mix_ring.me, b * QB:(b + 1) * QB, :] = attended[b * QB:(b + 1) * QB, :]

    def mix(chunk):
        at = piece_rows(chunk)
        total = jnp.zeros((chunk_rows, out.shape[1]), jnp.float32)
        for t in range(tp):
            total += jnp.dot(
                mixing[t, at, :], w_out[t * q_cols:(t + 1) * q_cols, :],
                preferred_element_type=jnp.float32,
            )
        out[at, :] = total.astype(jnp.bfloat16)

    def all_here():
        give.wait()

        @pl.loop(1, jnp.minimum(z, most_up) + 1)
        def _(step):
            across_whole(0, step).wait()

        @pl.loop(jnp.maximum(chips - z, 1), most_down + 1)
        def _(step):
            across_whole(1, step).wait()

    def key_positions():
        spread = (
            lax.broadcasted_iota(jnp.int32, (listed_slots, wide), 1) // KB
            == lax.broadcasted_iota(jnp.int32, (listed_slots, wide), 0)
        ).astype(jnp.float32)
        ids = sel[...]
        safe = jnp.where(ids < 0, 1 << 20, ids)
        high = (safe // 64).astype(jnp.float32)
        low = lax.rem(safe, 64).astype(jnp.float32)
        found = jnp.dot(high, spread, preferred_element_type=jnp.float32) * 64.0 + jnp.dot(
            low, spread, preferred_element_type=jnp.float32
        )
        key_pos = found.astype(jnp.int32) * KB + lax.rem(
            lax.broadcasted_iota(jnp.int32, (blocks, wide), 1), KB
        )
        return key_pos

    def stage(which):
        if which == 0:
            all_here()
        if which < PIECES:
            attend(which, key_positions())
            mix_ring.begin(which)
            if which:
                mix_ring.hand_on(which - 1)
        else:
            if which == PIECES:
                mix_ring.hand_on(PIECES - 1)
            mix_ring.arrived(which - PIECES)
            mix(which - PIECES)

    attend_at = jnp.minimum(z, most_up)

    @pl.loop(0, most_up + 2 * PIECES)
    def _(step):
        for piece in range(PIECES):
            @pl.when((step > 0) & ((step + piece >= PIECES) | (z < PIECES)))
            def _():
                hand_up(step, piece)

        down_step = step - jnp.where(z > most_up, 1, 0)

        for piece in range(PIECES):
            @pl.when((down_step > 0) & comes_down(down_step))
            def _():
                send_down(down_step, piece, False, False).wait_recv()
                wrapped = z + down_step >= chips
                onward = down_step < reach(chips)[1]

                @pl.when(onward & wrapped)
                def _():
                    send_down(down_step + 1, piece, False, False).start()

                @pl.when(onward & jnp.logical_not(wrapped) & (z > 0))
                def _():
                    send_down(down_step + 1, piece, True, True).start()

                @pl.when(onward & (z == 0))
                def _():
                    send_down(down_step + 1, piece, True, False).start()

                @pl.when(wrapped)
                def _():
                    across(1, down_step, piece).start()

        @pl.when((step == 0) & (z == 0))
        def _():
            pl.semaphore_wait(go, 1)
            for piece in range(PIECES):
                send_down(1, piece, False, False).start()

        @pl.when((step == 0) & (z > 0) & (z <= DIRECT))
        def _():
            pl.semaphore_wait(go, 1)
            for piece in range(PIECES):
                send_direct(piece).start()

        for which in range(2 * PIECES):
            @pl.when(step == attend_at + which)
            def _():
                stage(which)

    for chunk in range(PIECES):
        ring.sent(chunk)
        mix_ring.sent(chunk)

    @pl.when((z > 0) & (z <= DIRECT))
    def _():
        for piece in range(PIECES):
            send_direct(piece).wait_send()

    @pl.loop(1, most_up + 1)
    def _(step):
        for piece in range(PIECES):
            @pl.when(goes_up(step))
            def _():
                send_up(step, piece).wait_send()

            @pl.when(goes_down(step))
            def _():
                send_down(step, piece, False, False).wait_send()


def reach(chips):
    most_up = chips // 2 + 1
    return most_up, chips - 1 - most_up


def layer(tokens, gain, w_query, w_key, w_value, w_out, tables, select):
    rows, width = tokens.shape
    devices = lax.axis_size("kv")
    tp = lax.axis_size("tp")
    q_cols, k_cols = w_query.shape[1], w_key.shape[1]
    chips = devices // 2
    most_up, most_down = reach(chips)
    dma = pltpu.SemaphoreType.DMA
    bf16 = jnp.bfloat16
    vmem = pl.BlockSpec(memory_space=pltpu.VMEM)
    hbm = pl.BlockSpec(memory_space=pl.ANY)
    smem = pl.BlockSpec(memory_space=pltpu.SMEM)
    return pl.pallas_call(
        layer_kernel,
        out_shape=jax.ShapeDtypeStruct((rows, w_out.shape[1]), bf16),
        in_specs=[vmem, vmem, hbm, hbm, hbm, vmem, vmem, vmem, smem, vmem],
        out_specs=vmem,
        scratch_shapes=[
            pltpu.VMEM((tp, rows, width), bf16),
            pltpu.VMEM((tp * width, q_cols + 2 * k_cols), bf16),
            pltpu.VMEM((rows, q_cols), bf16),
            pltpu.VMEM((devices * rows // KB, KB, 2 * k_cols), bf16),
            pltpu.VMEM((most_down * rows // KB, KB, 2 * k_cols), bf16),
            pltpu.VMEM((select.shape[1] * KB, 2 * k_cols), bf16),
            pltpu.VMEM((rows, q_cols), bf16),
            pltpu.VMEM((tp, rows, q_cols), bf16),
            dma((PIECES, 4)),
            dma((PIECES, 4)),
            dma((2, most_up + 1, PIECES)),
            dma((2, most_up + 1, PIECES)),
            dma((2, most_up + 1)),
            dma((2, most_up + 1)),
            dma((PIECES, 4)),
            dma((PIECES, 4)),
            dma((PIECES,)),
            dma((4,)),
            pltpu.SemaphoreType.REGULAR,
        ],
        compiler_params=pltpu.CompilerParams(collective_id=0, has_side_effects=True),
        name="layer",
    )(tokens, gain, w_query, w_key, w_value, w_out, *tables, select, select)


def per_device(tokens, gain, w_query, w_key, w_value, w_out, select):
    rows = tokens.shape[0]
    positions = lax.axis_index("kv") * rows + jnp.arange(rows, dtype=jnp.int32)
    tables = rotary_tables(positions)
    return layer(
        tokens, gain, w_query, w_key, w_value, w_out, tables, select
    )


def solution(mesh):
    placed = (
        P(("grp", "kv"), "tp"),
        P(),
        P(None, "tp"),
        P(None, "tp"),
        P(None, "tp"),
        P(None, "tp"),
        P(("grp", "kv"), None),
    )
    return jax.shard_map(
        per_device, mesh=mesh, in_specs=placed, out_specs=P(("grp", "kv"), "tp"), check_vma=False
    )
```

```python
import functools

import jax
import jax.numpy as jnp
from jax import lax
from jax.experimental import pallas as pl
from jax.experimental.pallas import tpu as pltpu
from jax.sharding import PartitionSpec as P

HD = 128
QB = 128
KB = 32
PIECES = 4
DIRECT = 3

epsilon = 1e-06
theta = 10000.0
MESH = pl.DeviceIdType.MESH


def rotary_tables(positions):
    frequency = theta ** (-jnp.arange(0, HD, 2, dtype=jnp.float32) / HD)
    angles = positions.astype(jnp.float32)[:, None] * frequency[None, :]
    return jnp.cos(angles), jnp.sin(angles)


def remote(src, dst, send, recv, **where):
    return pltpu.make_async_remote_copy(
        src_ref=src, dst_ref=dst, send_sem=send, recv_sem=recv, device_id=where, device_id_type=MESH
    )


class TpRing:
    def __init__(self, own, slots, send, recv, rows):
        self.n = lax.axis_size("tp")
        self.me = lax.axis_index("tp")
        self.right = lax.rem(self.me + 1, self.n)
        self.left = lax.rem(self.me + self.n - 1, self.n)
        self.far = lax.rem(self.me + 2, self.n)
        self.own, self.slots, self.send, self.recv, self.rows = own, slots, send, recv, rows

    def copy(self, chunk, kind):
        half = self.rows // 2
        start, size, source, to = {
            0: (0, self.rows, None, self.right),
            1: (0, self.rows, None, self.left),
            2: (0, half, self.left, self.right),
            3: (half, half, self.right, self.left),
        }[kind]
        at = pl.ds(chunk * self.rows + start, size)
        src = self.own.at[at] if source is None else self.slots.at[source, at]
        dst = self.slots.at[self.me if source is None else source, at]
        return remote(src, dst, self.send.at[chunk, kind], self.recv.at[chunk, kind], tp=to)

    def begin(self, chunk):
        self.copy(chunk, 0).start()
        self.copy(chunk, 1).start()

    def hand_on(self, chunk):
        self.copy(chunk, 0).wait_recv()
        self.copy(chunk, 2).start()
        self.copy(chunk, 1).wait_recv()
        self.copy(chunk, 3).start()

    def arrived(self, chunk):
        self.copy(chunk, 2).wait_recv()
        self.copy(chunk, 3).wait_recv()

    def sent(self, chunk):
        for kind in range(4):
            self.copy(chunk, kind).wait_send()


def layer_kernel(
    tok, gain, wq, wk, wv, w_out, cos, sin, listed, sel, out,
    slots, weights, queries, need, transit, keys, places, attended, mixing,
    send_t, recv_t, send_z, recv_z, send_c, recv_c, send_m, recv_m, send_d, local, go,
):
    rows, width = tok.shape
    tp = lax.axis_size("tp")
    chunk_rows = rows // PIECES
    devices = lax.axis_size("kv")
    chips = devices // 2
    most_up, most_down = reach(chips)
    mine = lax.axis_index("kv")
    z, core = mine // 2, lax.rem(mine, 2)
    partner = mine + 1 - 2 * core
    up = lax.rem(mine + 2, devices)
    down = lax.rem(mine + devices - 2, devices)
    q_cols, k_cols = wq.shape[1], wk.shape[1]
    ring = TpRing(tok, slots, send_t, recv_t, chunk_rows)
    mix_ring = TpRing(attended, mixing, send_m, recv_m, chunk_rows)

    loads = [
        pltpu.make_async_copy(wq, weights.at[:, pl.ds(0, q_cols)], local.at[0]),
        pltpu.make_async_copy(wk, weights.at[:, pl.ds(q_cols, k_cols)], local.at[1]),
        pltpu.make_async_copy(wv, weights.at[:, pl.ds(q_cols + k_cols, k_cols)], local.at[2]),
        pltpu.make_async_copy(tok, slots.at[ring.me], local.at[3]),
    ]
    for load in loads:
        load.start()

    barrier = pltpu.get_barrier_semaphore()

    def hail(**where):
        pl.semaphore_signal(barrier, inc=1, device_id=where, device_id_type=MESH)

    hail(tp=ring.right)
    hail(tp=ring.left)
    hail(kv=partner)
    hail(kv=down)

    @pl.when(z < chips - 1)
    def _():
        hail(kv=up)

    last = (chips - 1) * 2 + core

    @pl.when((z > 0) & (z <= DIRECT))
    def _():
        hail(kv=last)

    @pl.when(z == 0)
    def _():
        pl.semaphore_wait(barrier, 4)

    @pl.when((z > 0) & (z < chips - 1))
    def _():
        pl.semaphore_wait(barrier, 5)

    @pl.when(z == chips - 1)
    def _():
        pl.semaphore_wait(barrier, 5 + DIRECT)
        for chip in range(DIRECT + 1):
            pl.semaphore_signal(
                go, inc=1, device_id={"kv": chip * 2 + core}, device_id_type=MESH
            )

    own_blocks = rows // KB
    chunk_blocks = chunk_rows // KB

    def piece_rows(piece):
        return pl.ds(piece * chunk_rows, chunk_rows)

    def piece_blocks(holder, piece):
        return pl.ds(holder * own_blocks + piece * chunk_blocks, chunk_blocks)

    def by_relay(at):
        return (at == 0) | (at > DIRECT)

    def goes_up(step):
        return (step <= reach(chips)[0]) & (z - step + 1 >= 0) & (z < chips - 1)

    def comes_up(step):
        return (step <= reach(chips)[0]) & (z - step >= 0)

    def goes_down(step):
        far = reach(chips)[1]
        return (step <= far) & (lax.rem(z + step - 1, chips) < far) & by_relay(z + step - 1)

    def comes_down(step):
        far = reach(chips)[1]
        return (step <= far) & (lax.rem(z + step, chips) < far) & by_relay(z + step)

    def send_up(step, piece):
        block = need.at[piece_blocks(lax.rem(z - step + 1 + chips, chips) * 2 + core, piece)]
        return remote(block, block, send_z.at[0, step, piece], recv_z.at[0, step, piece], kv=up)

    def send_down(step, piece, from_transit, to_transit):
        chip = lax.rem(z + step - 1, chips)
        kept = need.at[piece_blocks(chip * 2 + core, piece)]
        passing = transit.at[piece_blocks(lax.rem(chip, most_down), piece)]
        return remote(
            passing if from_transit else kept, passing if to_transit else kept,
            send_z.at[1, step, piece], recv_z.at[1, step, piece], kv=down,
        )

    def send_direct(piece):
        block = need.at[piece_blocks(mine, piece)]
        step = lax.rem(z, DIRECT + 1) + 1
        return remote(block, block, send_d.at[piece], recv_z.at[1, step, piece], kv=last)

    def across(direction, step, piece):
        chip = lax.rem(z - step + chips, chips) if direction == 0 else lax.rem(z + step, chips)
        block = need.at[piece_blocks(chip * 2 + core, piece)]
        return remote(
            block, block, send_c.at[direction, step], recv_c.at[direction, step], kv=partner
        )

    def across_whole(direction, step):
        block = need.at[pl.ds(mine * own_blocks, own_blocks)]
        return remote(
            block, block, send_c.at[direction, step], recv_c.at[direction, step], kv=partner
        )

    gain_row = gain[...].astype(jnp.float32).reshape(1, -1)

    def project(chunk):
        at = piece_rows(chunk)
        total = jnp.zeros((chunk_rows, weights.shape[1]), jnp.float32)
        squares = jnp.zeros((chunk_rows, 1), jnp.float32)
        for t in range(tp):
            block = slots[t, at, :].astype(jnp.float32)
            squares += jnp.sum(block * block, axis=1, keepdims=True)
            scaled = (block * gain_row[:, t * width:(t + 1) * width]).astype(
                jnp.bfloat16
            )
            total += jnp.dot(
                scaled, weights[t * width:(t + 1) * width, :], preferred_element_type=jnp.float32
            )
        total *= lax.rsqrt(squares / (tp * width) + epsilon)
        c, n = cos[at, :], sin[at, :]
        cosine, sine = jnp.concatenate([c, c], 1), jnp.concatenate([-n, n], 1)
        heads = []
        for h in range((q_cols + k_cols) // HD):
            head = total[:, h * HD:(h + 1) * HD]
            heads.append((head * cosine + pltpu.roll(head, HD // 2, 1) * sine).astype(jnp.bfloat16))
        for h in range(q_cols // HD):
            queries[at, h * HD:(h + 1) * HD] = heads[h]
        kept = piece_blocks(mine, chunk)
        values = total[:, q_cols + k_cols:].astype(jnp.bfloat16)
        need[kept, :, 0:k_cols] = heads[-1].reshape(chunk_blocks, KB, k_cols)
        need[kept, :, k_cols:2 * k_cols] = values.reshape(chunk_blocks, KB, k_cols)

        @pl.when(goes_up(1))
        def _():
            send_up(1, chunk).start()

        @pl.when(goes_down(1) & (z > 0))
        def _():
            send_down(1, chunk, False, True).start()

    def hand_up(step, piece):
        @pl.when(comes_up(step))
        def _():
            send_up(step, piece).wait_recv()

            @pl.when(goes_up(step + 1))
            def _():
                send_up(step + 1, piece).start()

            across(0, step, piece).start()

    blocks, listed_slots = sel.shape
    wide = listed_slots * KB
    heads_here = q_cols // HD

    def key_positions():
        spread = (
            lax.broadcasted_iota(jnp.int32, (listed_slots, wide), 1) // KB
            == lax.broadcasted_iota(jnp.int32, (listed_slots, wide), 0)
        ).astype(jnp.float32)
        ids = sel[...]
        safe = jnp.where(ids < 0, 1 << 20, ids)
        high = (safe // 64).astype(jnp.float32)
        low = lax.rem(safe, 64).astype(jnp.float32)
        found = jnp.dot(high, spread, preferred_element_type=jnp.float32) * 64.0 + jnp.dot(
            low, spread, preferred_element_type=jnp.float32
        )
        key_pos = found.astype(jnp.int32) * KB + lax.rem(
            lax.broadcasted_iota(jnp.int32, (blocks, wide), 1), KB
        )
        return key_pos

    ring.begin(0)
    ring.begin(1)
    places[...] = key_positions()
    for load in loads:
        load.wait()
    for chunk in range(PIECES):
        if chunk == 0:
            ring.hand_on(0)
            ring.begin(2)
            ring.hand_on(1)
            ring.begin(3)
        elif chunk + 1 < PIECES:
            ring.hand_on(chunk + 1)
        ring.arrived(chunk)
        project(chunk)

        @pl.when(z >= PIECES)
        def _():
            for step in range(1, chunk + 1):
                hand_up(step, chunk - step)

    give = across_whole(0, 0)
    give.start()


    def attend(b, key_pos):
        @pl.loop(0, listed_slots, unroll=4)
        def _(s):
            keys[pl.ds(pl.multiple_of(s * KB, KB), KB), :] = need[jnp.maximum(listed[b, s], 0)]

        q_pos = mine * rows + b * QB + lax.broadcasted_iota(jnp.int32, (QB, wide), 0)
        allowed = jnp.broadcast_to(key_pos[b:b + 1, :], (QB, wide)) <= q_pos
        for h in range(heads_here):
            score = lax.dot_general(
                queries[b * QB:(b + 1) * QB, h * HD:(h + 1) * HD], keys[:, 0:HD],
                (((1,), (1,)), ((), ())), preferred_element_type=jnp.float32,
            ) * HD ** (-0.5)
            score = jnp.where(allowed, score, -jnp.inf)
            raised = jnp.exp(score - jnp.max(score, axis=1, keepdims=True))
            parts = (raised * (1.0 / jnp.sum(raised, axis=1, keepdims=True))).astype(jnp.bfloat16)
            attended[b * QB:(b + 1) * QB, h * HD:(h + 1) * HD] = jnp.dot(
                parts, keys[:, HD:2 * HD], preferred_element_type=jnp.float32
            ).astype(jnp.bfloat16)
        mixing[mix_ring.me, b * QB:(b + 1) * QB, :] = attended[b * QB:(b + 1) * QB, :]

    def mix(chunk):
        at = piece_rows(chunk)
        total = jnp.zeros((chunk_rows, out.shape[1]), jnp.float32)
        for t in range(tp):
            total += jnp.dot(
                mixing[t, at, :], w_out[t * q_cols:(t + 1) * q_cols, :],
                preferred_element_type=jnp.float32,
            )
        out[at, :] = total.astype(jnp.bfloat16)

    def all_here():
        give.wait()

        @pl.loop(1, jnp.minimum(z, most_up) + 1)
        def _(step):
            across_whole(0, step).wait()

        @pl.loop(jnp.maximum(chips - z, 1), most_down + 1)
        def _(step):
            across_whole(1, step).wait()

    def stage(which):
        if which == 0:
            all_here()
        if which < PIECES:
            attend(which, places[...])
            mix_ring.begin(which)
            if which:
                mix_ring.hand_on(which - 1)
        else:
            if which == PIECES:
                mix_ring.hand_on(PIECES - 1)
            mix_ring.arrived(which - PIECES)
            mix(which - PIECES)

    attend_at = jnp.minimum(z, most_up)

    @pl.loop(0, most_up + 2 * PIECES)
    def _(step):
        for piece in range(PIECES):
            @pl.when((step > 0) & ((step + piece >= PIECES) | (z < PIECES)))
            def _():
                hand_up(step, piece)

        down_step = step - jnp.where(z > most_up, 1, 0)

        for piece in range(PIECES):
            @pl.when((down_step > 0) & comes_down(down_step))
            def _():
                send_down(down_step, piece, False, False).wait_recv()
                wrapped = z + down_step >= chips
                onward = down_step < reach(chips)[1]

                @pl.when(onward & wrapped)
                def _():
                    send_down(down_step + 1, piece, False, False).start()

                @pl.when(onward & jnp.logical_not(wrapped) & (z > 0))
                def _():
                    send_down(down_step + 1, piece, True, True).start()

                @pl.when(onward & (z == 0))
                def _():
                    send_down(down_step + 1, piece, True, False).start()

                @pl.when(wrapped)
                def _():
                    across(1, down_step, piece).start()

        @pl.when((step == 0) & (z == 0))
        def _():
            pl.semaphore_wait(go, 1)
            for piece in range(PIECES):
                send_down(1, piece, False, False).start()

        @pl.when((step == 0) & (z > 0) & (z <= DIRECT))
        def _():
            pl.semaphore_wait(go, 1)
            for piece in range(PIECES):
                send_direct(piece).start()

        for which in range(2 * PIECES):
            @pl.when(step == attend_at + which)
            def _():
                stage(which)

    for chunk in range(PIECES):
        ring.sent(chunk)
        mix_ring.sent(chunk)

    @pl.when((z > 0) & (z <= DIRECT))
    def _():
        for piece in range(PIECES):
            send_direct(piece).wait_send()

    @pl.loop(1, most_up + 1)
    def _(step):
        for piece in range(PIECES):
            @pl.when(goes_up(step))
            def _():
                send_up(step, piece).wait_send()

            @pl.when(goes_down(step))
            def _():
                send_down(step, piece, False, False).wait_send()


def reach(chips):
    most_up = chips // 2 + 1
    return most_up, chips - 1 - most_up


def layer(tokens, gain, w_query, w_key, w_value, w_out, tables, select):
    rows, width = tokens.shape
    devices = lax.axis_size("kv")
    tp = lax.axis_size("tp")
    q_cols, k_cols = w_query.shape[1], w_key.shape[1]
    chips = devices // 2
    most_up, most_down = reach(chips)
    dma = pltpu.SemaphoreType.DMA
    bf16 = jnp.bfloat16
    vmem = pl.BlockSpec(memory_space=pltpu.VMEM)
    hbm = pl.BlockSpec(memory_space=pl.ANY)
    smem = pl.BlockSpec(memory_space=pltpu.SMEM)
    return pl.pallas_call(
        layer_kernel,
        out_shape=jax.ShapeDtypeStruct((rows, w_out.shape[1]), bf16),
        in_specs=[vmem, vmem, hbm, hbm, hbm, vmem, vmem, vmem, smem, vmem],
        out_specs=vmem,
        scratch_shapes=[
            pltpu.VMEM((tp, rows, width), bf16),
            pltpu.VMEM((tp * width, q_cols + 2 * k_cols), bf16),
            pltpu.VMEM((rows, q_cols), bf16),
            pltpu.VMEM((devices * rows // KB, KB, 2 * k_cols), bf16),
            pltpu.VMEM((most_down * rows // KB, KB, 2 * k_cols), bf16),
            pltpu.VMEM((select.shape[1] * KB, 2 * k_cols), bf16),
            pltpu.VMEM((select.shape[0], select.shape[1] * KB), jnp.int32),
            pltpu.VMEM((rows, q_cols), bf16),
            pltpu.VMEM((tp, rows, q_cols), bf16),
            dma((PIECES, 4)),
            dma((PIECES, 4)),
            dma((2, most_up + 1, PIECES)),
            dma((2, most_up + 1, PIECES)),
            dma((2, most_up + 1)),
            dma((2, most_up + 1)),
            dma((PIECES, 4)),
            dma((PIECES, 4)),
            dma((PIECES,)),
            dma((4,)),
            pltpu.SemaphoreType.REGULAR,
        ],
        compiler_params=pltpu.CompilerParams(collective_id=0, has_side_effects=True),
        name="layer",
    )(tokens, gain, w_query, w_key, w_value, w_out, *tables, select, select)


def per_device(tokens, gain, w_query, w_key, w_value, w_out, select):
    rows = tokens.shape[0]
    positions = lax.axis_index("kv") * rows + jnp.arange(rows, dtype=jnp.int32)
    tables = rotary_tables(positions)
    return layer(
        tokens, gain, w_query, w_key, w_value, w_out, tables, select
    )


def solution(mesh):
    placed = (
        P(("grp", "kv"), "tp"),
        P(),
        P(None, "tp"),
        P(None, "tp"),
        P(None, "tp"),
        P(None, "tp"),
        P(("grp", "kv"), None),
    )
    return jax.shard_map(
        per_device, mesh=mesh, in_specs=placed, out_specs=P(("grp", "kv"), "tp"), check_vma=False
    )
```

```python
import functools

import jax
import jax.numpy as jnp
from jax import lax
from jax.experimental import pallas as pl
from jax.experimental.pallas import tpu as pltpu
from jax.sharding import PartitionSpec as P

HD = 128
QB = 128
KB = 32
PIECES = 4
DIRECT = 3

epsilon = 1e-06
theta = 10000.0
MESH = pl.DeviceIdType.MESH


def rotary_tables(positions):
    frequency = theta ** (-jnp.arange(0, HD, 2, dtype=jnp.float32) / HD)
    angles = positions.astype(jnp.float32)[:, None] * frequency[None, :]
    return jnp.cos(angles), jnp.sin(angles)


def remote(src, dst, send, recv, **where):
    return pltpu.make_async_remote_copy(
        src_ref=src, dst_ref=dst, send_sem=send, recv_sem=recv, device_id=where, device_id_type=MESH
    )


class TpRing:
    def __init__(self, own, slots, send, recv, rows):
        self.n = lax.axis_size("tp")
        self.me = lax.axis_index("tp")
        self.right = lax.rem(self.me + 1, self.n)
        self.left = lax.rem(self.me + self.n - 1, self.n)
        self.far = lax.rem(self.me + 2, self.n)
        self.own, self.slots, self.send, self.recv, self.rows = own, slots, send, recv, rows

    def copy(self, chunk, kind):
        half = self.rows // 2
        start, size, source, to = {
            0: (0, self.rows, None, self.right),
            1: (0, self.rows, None, self.left),
            2: (0, half, self.left, self.right),
            3: (half, half, self.right, self.left),
        }[kind]
        at = pl.ds(chunk * self.rows + start, size)
        src = self.own.at[at] if source is None else self.slots.at[source, at]
        dst = self.slots.at[self.me if source is None else source, at]
        return remote(src, dst, self.send.at[chunk, kind], self.recv.at[chunk, kind], tp=to)

    def begin(self, chunk):
        self.copy(chunk, 0).start()
        self.copy(chunk, 1).start()

    def hand_on(self, chunk):
        self.copy(chunk, 0).wait_recv()
        self.copy(chunk, 2).start()
        self.copy(chunk, 1).wait_recv()
        self.copy(chunk, 3).start()

    def arrived(self, chunk):
        self.copy(chunk, 2).wait_recv()
        self.copy(chunk, 3).wait_recv()

    def sent(self, chunk):
        for kind in range(4):
            self.copy(chunk, kind).wait_send()


def layer_kernel(
    tok, gain, wq, wk, wv, w_out, cos, sin, listed, sel, out,
    slots, weights, queries, need, transit, keys, places, attended, mixing,
    send_t, recv_t, send_z, recv_z, send_c, recv_c, send_m, recv_m, send_d, local, go,
):
    rows, width = tok.shape
    tp = lax.axis_size("tp")
    chunk_rows = rows // PIECES
    devices = lax.axis_size("kv")
    chips = devices // 2
    most_up, most_down = reach(chips)
    mine = lax.axis_index("kv")
    z, core = mine // 2, lax.rem(mine, 2)
    partner = mine + 1 - 2 * core
    up = lax.rem(mine + 2, devices)
    down = lax.rem(mine + devices - 2, devices)
    q_cols, k_cols = wq.shape[1], wk.shape[1]
    ring = TpRing(tok, slots, send_t, recv_t, chunk_rows)
    mix_ring = TpRing(attended, mixing, send_m, recv_m, chunk_rows)

    loads = [
        pltpu.make_async_copy(wq, weights.at[:, pl.ds(0, q_cols)], local.at[0]),
        pltpu.make_async_copy(wk, weights.at[:, pl.ds(q_cols, k_cols)], local.at[1]),
        pltpu.make_async_copy(wv, weights.at[:, pl.ds(q_cols + k_cols, k_cols)], local.at[2]),
        pltpu.make_async_copy(tok, slots.at[ring.me], local.at[3]),
    ]
    for load in loads:
        load.start()

    barrier = pltpu.get_barrier_semaphore()

    def hail(**where):
        pl.semaphore_signal(barrier, inc=1, device_id=where, device_id_type=MESH)

    hail(tp=ring.right)
    hail(tp=ring.left)
    hail(kv=partner)
    hail(kv=down)

    @pl.when(z < chips - 1)
    def _():
        hail(kv=up)

    last = (chips - 1) * 2 + core

    @pl.when((z > 0) & (z <= DIRECT))
    def _():
        hail(kv=last)

    @pl.when(z == 0)
    def _():
        pl.semaphore_wait(barrier, 4)

    @pl.when((z > 0) & (z < chips - 1))
    def _():
        pl.semaphore_wait(barrier, 5)

    @pl.when(z == chips - 1)
    def _():
        pl.semaphore_wait(barrier, 5 + DIRECT)
        for chip in range(DIRECT + 1):
            pl.semaphore_signal(
                go, inc=1, device_id={"kv": chip * 2 + core}, device_id_type=MESH
            )

    own_blocks = rows // KB
    chunk_blocks = chunk_rows // KB

    def piece_rows(piece):
        return pl.ds(piece * chunk_rows, chunk_rows)

    def piece_blocks(holder, piece):
        return pl.ds(holder * own_blocks + piece * chunk_blocks, chunk_blocks)

    def by_relay(at):
        return (at == 0) | (at > DIRECT)

    def goes_up(step):
        return (step <= reach(chips)[0]) & (z - step + 1 >= 0) & (z < chips - 1)

    def comes_up(step):
        return (step <= reach(chips)[0]) & (z - step >= 0)

    def goes_down(step):
        far = reach(chips)[1]
        return (step <= far) & (lax.rem(z + step - 1, chips) < far) & by_relay(z + step - 1)

    def comes_down(step):
        far = reach(chips)[1]
        return (step <= far) & (lax.rem(z + step, chips) < far) & by_relay(z + step)

    def send_up(step, piece):
        block = need.at[piece_blocks(lax.rem(z - step + 1 + chips, chips) * 2 + core, piece)]
        return remote(block, block, send_z.at[0, step, piece], recv_z.at[0, step, piece], kv=up)

    def send_down(step, piece, from_transit, to_transit):
        chip = lax.rem(z + step - 1, chips)
        kept = need.at[piece_blocks(chip * 2 + core, piece)]
        passing = transit.at[piece_blocks(lax.rem(chip, most_down), piece)]
        return remote(
            passing if from_transit else kept, passing if to_transit else kept,
            send_z.at[1, step, piece], recv_z.at[1, step, piece], kv=down,
        )

    def send_direct(piece):
        block = need.at[piece_blocks(mine, piece)]
        step = lax.rem(z, DIRECT + 1) + 1
        return remote(block, block, send_d.at[piece], recv_z.at[1, step, piece], kv=last)

    def across(direction, step, piece):
        chip = lax.rem(z - step + chips, chips) if direction == 0 else lax.rem(z + step, chips)
        block = need.at[piece_blocks(chip * 2 + core, piece)]
        return remote(
            block, block, send_c.at[direction, step], recv_c.at[direction, step], kv=partner
        )

    def across_whole(direction, step):
        block = need.at[pl.ds(mine * own_blocks, own_blocks)]
        return remote(
            block, block, send_c.at[direction, step], recv_c.at[direction, step], kv=partner
        )

    gain_row = gain[...].astype(jnp.float32).reshape(1, -1)

    def project(chunk):
        at = piece_rows(chunk)
        total = jnp.zeros((chunk_rows, weights.shape[1]), jnp.float32)
        squares = jnp.zeros((chunk_rows, 1), jnp.float32)
        for t in range(tp):
            block = slots[t, at, :].astype(jnp.float32)
            squares += jnp.sum(block * block, axis=1, keepdims=True)
            scaled = (block * gain_row[:, t * width:(t + 1) * width]).astype(
                jnp.bfloat16
            )
            total += jnp.dot(
                scaled, weights[t * width:(t + 1) * width, :], preferred_element_type=jnp.float32
            )
        total *= lax.rsqrt(squares / (tp * width) + epsilon)
        c, n = cos[at, :], sin[at, :]
        cosine, sine = jnp.concatenate([c, c], 1), jnp.concatenate([-n, n], 1)
        heads = []
        for h in range((q_cols + k_cols) // HD):
            head = total[:, h * HD:(h + 1) * HD]
            heads.append((head * cosine + pltpu.roll(head, HD // 2, 1) * sine).astype(jnp.bfloat16))
        for h in range(q_cols // HD):
            queries[at, h * HD:(h + 1) * HD] = heads[h]
        kept = piece_blocks(mine, chunk)
        values = total[:, q_cols + k_cols:].astype(jnp.bfloat16)
        need[kept, :, 0:k_cols] = heads[-1].reshape(chunk_blocks, KB, k_cols)
        need[kept, :, k_cols:2 * k_cols] = values.reshape(chunk_blocks, KB, k_cols)

        @pl.when(goes_up(1))
        def _():
            send_up(1, chunk).start()

        @pl.when(goes_down(1) & (z > 0))
        def _():
            send_down(1, chunk, False, True).start()

    def hand_up(step, piece):
        @pl.when(comes_up(step))
        def _():
            send_up(step, piece).wait_recv()

            @pl.when(goes_up(step + 1))
            def _():
                send_up(step + 1, piece).start()

            across(0, step, piece).start()

    blocks, listed_slots = sel.shape
    wide = listed_slots * KB
    heads_here = q_cols // HD

    def key_positions():
        spread = (
            lax.broadcasted_iota(jnp.int32, (listed_slots, wide), 1) // KB
            == lax.broadcasted_iota(jnp.int32, (listed_slots, wide), 0)
        ).astype(jnp.float32)
        ids = sel[...]
        safe = jnp.where(ids < 0, 1 << 20, ids)
        high = (safe // 64).astype(jnp.float32)
        low = lax.rem(safe, 64).astype(jnp.float32)
        found = jnp.dot(high, spread, preferred_element_type=jnp.float32) * 64.0 + jnp.dot(
            low, spread, preferred_element_type=jnp.float32
        )
        key_pos = found.astype(jnp.int32) * KB + lax.rem(
            lax.broadcasted_iota(jnp.int32, (blocks, wide), 1), KB
        )
        return key_pos

    ring.begin(0)
    ring.begin(1)
    places[...] = key_positions()
    for load in loads:
        load.wait()
    for chunk in range(PIECES):
        if chunk == 0:
            ring.hand_on(0)
            ring.begin(2)
            ring.hand_on(1)
            ring.begin(3)
        elif chunk + 1 < PIECES:
            ring.hand_on(chunk + 1)
        ring.arrived(chunk)
        project(chunk)

        @pl.when(z >= PIECES)
        def _():
            for step in range(1, chunk + 1):
                hand_up(step, chunk - step)

    give = across_whole(0, 0)
    give.start()


    def attend(b, key_pos):
        @pl.loop(0, listed_slots, unroll=4)
        def _(s):
            keys[pl.ds(pl.multiple_of(s * KB, KB), KB), :] = need[jnp.maximum(listed[b, s], 0)]

        q_pos = mine * rows + b * QB + lax.broadcasted_iota(jnp.int32, (QB, wide), 0)
        allowed = jnp.broadcast_to(key_pos[b:b + 1, :], (QB, wide)) <= q_pos
        for h in range(heads_here):
            score = lax.dot_general(
                queries[b * QB:(b + 1) * QB, h * HD:(h + 1) * HD], keys[:, 0:HD],
                (((1,), (1,)), ((), ())), preferred_element_type=jnp.float32,
            ) * HD ** (-0.5)
            score = jnp.where(allowed, score, -jnp.inf)
            raised = jnp.exp(score - jnp.max(score, axis=1, keepdims=True))
            parts = (raised * (1.0 / jnp.sum(raised, axis=1, keepdims=True))).astype(jnp.bfloat16)
            attended[b * QB:(b + 1) * QB, h * HD:(h + 1) * HD] = jnp.dot(
                parts, keys[:, HD:2 * HD], preferred_element_type=jnp.float32
            ).astype(jnp.bfloat16)
        mixing[mix_ring.me, b * QB:(b + 1) * QB, :] = attended[b * QB:(b + 1) * QB, :]

    def mix(chunk):
        at = piece_rows(chunk)
        total = jnp.zeros((chunk_rows, out.shape[1]), jnp.float32)
        for t in range(tp):
            total += jnp.dot(
                mixing[t, at, :], w_out[t * q_cols:(t + 1) * q_cols, :],
                preferred_element_type=jnp.float32,
            )
        out[at, :] = total.astype(jnp.bfloat16)

    def all_here():
        give.wait()

        @pl.loop(1, jnp.minimum(z, most_up) + 1)
        def _(step):
            across_whole(0, step).wait()

        @pl.loop(jnp.maximum(chips - z, 1), most_down + 1)
        def _(step):
            across_whole(1, step).wait()

    def stage(which):
        if which == 0:
            all_here()
        if which < PIECES:
            attend(which, places[...])
            mix_ring.begin(which)
            if which > 1:
                mix_ring.hand_on(which - 2)
        else:
            if which == PIECES:
                mix_ring.hand_on(PIECES - 2)
            if which == PIECES + 1:
                mix_ring.hand_on(PIECES - 1)
            mix_ring.arrived(which - PIECES)
            mix(which - PIECES)

    attend_at = jnp.minimum(z, most_up)

    @pl.loop(0, most_up + 2 * PIECES)
    def _(step):
        for piece in range(PIECES):
            @pl.when((step > 0) & ((step + piece >= PIECES) | (z < PIECES)))
            def _():
                hand_up(step, piece)

        down_step = step - jnp.where(z > most_up, 1, 0)

        for piece in range(PIECES):
            @pl.when((down_step > 0) & comes_down(down_step))
            def _():
                send_down(down_step, piece, False, False).wait_recv()
                wrapped = z + down_step >= chips
                onward = down_step < reach(chips)[1]

                @pl.when(onward & wrapped)
                def _():
                    send_down(down_step + 1, piece, False, False).start()

                @pl.when(onward & jnp.logical_not(wrapped) & (z > 0))
                def _():
                    send_down(down_step + 1, piece, True, True).start()

                @pl.when(onward & (z == 0))
                def _():
                    send_down(down_step + 1, piece, True, False).start()

                @pl.when(wrapped)
                def _():
                    across(1, down_step, piece).start()

        @pl.when((step == 0) & (z == 0))
        def _():
            pl.semaphore_wait(go, 1)
            for piece in range(PIECES):
                send_down(1, piece, False, False).start()

        @pl.when((step == 0) & (z > 0) & (z <= DIRECT))
        def _():
            pl.semaphore_wait(go, 1)
            for piece in range(PIECES):
                send_direct(piece).start()

        for which in range(2 * PIECES):
            @pl.when(step == attend_at + which)
            def _():
                stage(which)

    for chunk in range(PIECES):
        ring.sent(chunk)
        mix_ring.sent(chunk)

    @pl.when((z > 0) & (z <= DIRECT))
    def _():
        for piece in range(PIECES):
            send_direct(piece).wait_send()

    @pl.loop(1, most_up + 1)
    def _(step):
        for piece in range(PIECES):
            @pl.when(goes_up(step))
            def _():
                send_up(step, piece).wait_send()

            @pl.when(goes_down(step))
            def _():
                send_down(step, piece, False, False).wait_send()


def reach(chips):
    most_up = chips // 2 + 1
    return most_up, chips - 1 - most_up


def layer(tokens, gain, w_query, w_key, w_value, w_out, tables, select):
    rows, width = tokens.shape
    devices = lax.axis_size("kv")
    tp = lax.axis_size("tp")
    q_cols, k_cols = w_query.shape[1], w_key.shape[1]
    chips = devices // 2
    most_up, most_down = reach(chips)
    dma = pltpu.SemaphoreType.DMA
    bf16 = jnp.bfloat16
    vmem = pl.BlockSpec(memory_space=pltpu.VMEM)
    hbm = pl.BlockSpec(memory_space=pl.ANY)
    smem = pl.BlockSpec(memory_space=pltpu.SMEM)
    return pl.pallas_call(
        layer_kernel,
        out_shape=jax.ShapeDtypeStruct((rows, w_out.shape[1]), bf16),
        in_specs=[vmem, vmem, hbm, hbm, hbm, vmem, vmem, vmem, smem, vmem],
        out_specs=vmem,
        scratch_shapes=[
            pltpu.VMEM((tp, rows, width), bf16),
            pltpu.VMEM((tp * width, q_cols + 2 * k_cols), bf16),
            pltpu.VMEM((rows, q_cols), bf16),
            pltpu.VMEM((devices * rows // KB, KB, 2 * k_cols), bf16),
            pltpu.VMEM((most_down * rows // KB, KB, 2 * k_cols), bf16),
            pltpu.VMEM((select.shape[1] * KB, 2 * k_cols), bf16),
            pltpu.VMEM((select.shape[0], select.shape[1] * KB), jnp.int32),
            pltpu.VMEM((rows, q_cols), bf16),
            pltpu.VMEM((tp, rows, q_cols), bf16),
            dma((PIECES, 4)),
            dma((PIECES, 4)),
            dma((2, most_up + 1, PIECES)),
            dma((2, most_up + 1, PIECES)),
            dma((2, most_up + 1)),
            dma((2, most_up + 1)),
            dma((PIECES, 4)),
            dma((PIECES, 4)),
            dma((PIECES,)),
            dma((4,)),
            pltpu.SemaphoreType.REGULAR,
        ],
        compiler_params=pltpu.CompilerParams(collective_id=0, has_side_effects=True),
        name="layer",
    )(tokens, gain, w_query, w_key, w_value, w_out, *tables, select, select)


def per_device(tokens, gain, w_query, w_key, w_value, w_out, select):
    rows = tokens.shape[0]
    positions = lax.axis_index("kv") * rows + jnp.arange(rows, dtype=jnp.int32)
    tables = rotary_tables(positions)
    return layer(
        tokens, gain, w_query, w_key, w_value, w_out, tables, select
    )


def solution(mesh):
    placed = (
        P(("grp", "kv"), "tp"),
        P(),
        P(None, "tp"),
        P(None, "tp"),
        P(None, "tp"),
        P(None, "tp"),
        P(("grp", "kv"), None),
    )
    return jax.shard_map(
        per_device, mesh=mesh, in_specs=placed, out_specs=P(("grp", "kv"), "tp"), check_vma=False
    )
```
